256 devices in a mesh: sp: 64 (over z, x, core), tp: 4 (over y).
Axes of the slice: x: 4, y: 4, z: 8, core: 2. Of those that a mesh axis runs over, the one named last changes fastest.
Arguments:
- tokens: bfloat16 [24576, 2048], P(('sp', 'tp')), may hold values from -6 to 6
- norm_gain: float32 [2048], replicated, may hold values from 0.1 to 1.9
- w_recept: bfloat16 [2048, 1024], P(None, 'tp'), may hold values from -0.125 to 0.125
- w_key: bfloat16 [2048, 1024], P(None, 'tp'), may hold values from -0.125 to 0.125
- w_value: bfloat16 [2048, 1024], P(None, 'tp'), may hold values from -0.125 to 0.125
- w_decay: bfloat16 [2048, 1024], P(None, 'tp'), may hold values from -0.125 to 0.125
- w_rate: bfloat16 [2048, 1024], P(None, 'tp'), may hold values from -0.125 to 0.125
- w_gate: bfloat16 [2048, 1024], P(None, 'tp'), may hold values from -0.125 to 0.125
- shift_mix: float32 [3, 1024], P(None, 'tp'), may hold values from 0 to 1
- decay_base: float32 [1024], P('tp'), may hold values from -16 to -2
- rate_base: float32 [1024], P('tp'), may hold values from -10 to 1
- decay_drift: float32 [24576], P('sp'), may hold values from -2 to 2, as said below
- group_gain: float32 [1024], P('tp'), may hold values from 0.1 to 1.9
- initial_state: float32 [16, 64, 64], P('tp'), may hold values from -240 to 240
- w_out: bfloat16 [1024, 2048], replicated, may hold values from -0.1875 to 0.1875
Outputs:
- out: bfloat16 [24576, 2048], P(('sp', 'tp'))
The draws below stay inside these ranges and needn't reach their ends.
Inputs may be any that keep to these rules, and one draw needn't show every extreme that they name: `decay_drift`: constant over aligned runs of 64 positions.
All inputs are finite; a program needn't handle non-finite values.
Results may differ from the reference program's by a relative error of at most 0.0083.
Values may be sent and summed in bfloat16 or wider, within the bound.
A program may use at most 128 MiB of HBM per device.

```python
import math
import jax
import jax.numpy as jnp
from jax import lax

D = 2048
HEADS = 16
HEAD = 64
BLOCK = 64
INNER = 1024
TOKENS = 24576


def head_kinds(key):
    picks = jax.random.randint(jax.random.fold_in(key, 11), (HEADS,), 0, 8)
    return picks < 4


def draw_decay_base(key, part):
    slow = head_kinds(key)
    jitter = jax.random.uniform(jax.random.fold_in(key, 12), (HEADS, HEAD), jnp.float32, -0.5, 0.5)
    long_level = -math.log(TOKENS) - 1.0
    value = jnp.where(slow[:, None], long_level, -3.0) + jitter
    return value.reshape(HEADS * HEAD).astype(jnp.float32)


def draw_rate_base(key, part):
    slow = head_kinds(key)
    jitter = jax.random.uniform(jax.random.fold_in(key, 13), (HEADS, HEAD), jnp.float32, -1.0, 1.0)
    long_level = math.log(HEAD / TOKENS) - 1.0
    value = jnp.where(slow[:, None], long_level + 0.5 * jitter, jitter)
    return value.reshape(HEADS * HEAD).astype(jnp.float32)


def draw_decay_drift(key, part):
    count = TOKENS // BLOCK
    levels = jax.random.uniform(jax.random.fold_in(key, 14), (count,), jnp.float32, -1.5, 1.5)
    return jnp.repeat(levels, BLOCK).astype(jnp.float32)


def level_of(own_key, dims, cuts, low, high):
    gain, own = 1.0, jax.random.fold_in(own_key, 6)
    for position, shards_of in cuts:
        draws = jnp.exp(jax.random.uniform(jax.random.fold_in(own, position), (shards_of,), jnp.float32, low / len(cuts), high / len(cuts)))
        gain = gain * jnp.repeat(draws, dims[position] // shards_of).reshape([-1 if axis == position else 1 for axis in range(len(dims))])
    return gain


def gaussian(rng, extent, width, limit, cuts=(), held_as=jnp.bfloat16):
    drawn = jax.random.normal(rng, extent, jnp.float32) * width
    if len(cuts) > 0:
        drawn = level_of(rng, extent, cuts, -0.22, 0.18) * drawn
    return jnp.clip(drawn, min=-limit, max=limit).astype(held_as)


def setup_inputs(seed: int = 0) -> dict:
    arg_keys = jax.random.split(jax.random.key(seed), 16)
    return {
        "tokens": gaussian(arg_keys[0], (TOKENS, D), 1.0, 6.0, ((0, 256),)),
        "norm_gain": jnp.clip(1.0 + 0.18 * jax.random.normal(arg_keys[1], (D,), jnp.float32), 0.1, 1.9),
        "w_recept": gaussian(arg_keys[2], (D, INNER), D ** -0.5, 0.125, ((1, 4),)),
        "w_key": gaussian(arg_keys[3], (D, INNER), D ** -0.5, 0.125, ((1, 4),)),
        "w_value": gaussian(arg_keys[4], (D, INNER), D ** -0.5, 0.125, ((1, 4),)),
        "w_decay": gaussian(arg_keys[5], (D, INNER), D ** -0.5, 0.125, ((1, 4),)),
        "w_rate": gaussian(arg_keys[6], (D, INNER), D ** -0.5, 0.125, ((1, 4),)),
        "w_gate": gaussian(arg_keys[7], (D, INNER), D ** -0.5, 0.125, ((1, 4),)),
        "shift_mix": jnp.clip(1.0 * jax.random.uniform(arg_keys[8], (3, INNER), jnp.float32) ** level_of(arg_keys[8], (3, INNER), ((1, 4),), -0.2, 0.2), 0.0, 1.0),
        "decay_base": draw_decay_base(jax.random.fold_in(arg_keys[15], 71), 0),
        "rate_base": draw_rate_base(jax.random.fold_in(arg_keys[15], 71), 0),
        "decay_drift": draw_decay_drift(jax.random.fold_in(arg_keys[15], 71), 0),
        "group_gain": jnp.clip(1.0 + 0.18 * jax.random.normal(arg_keys[12], (INNER,), jnp.float32), 0.1, 1.9),
        "initial_state": gaussian(arg_keys[13], (HEADS, HEAD, HEAD), 40.0, 240.0, ((0, 4),), jnp.float32),
        "w_out": gaussian(arg_keys[14], (INNER, D), INNER ** -0.5, 0.1875),
    }


norm_floor = 0.5
group_floor = 1.0
highest = lax.Precision.HIGHEST

def reference(tokens, norm_gain, w_recept, w_key, w_value, w_decay, w_rate, w_gate, shift_mix, decay_base, rate_base, decay_drift, group_gain, initial_state, w_out):
    tok_float = tokens.astype(jnp.float32)
    normed = (tok_float * lax.rsqrt(lax.optimization_barrier(jnp.mean(tok_float * tok_float, axis=-1, keepdims=True)) + norm_floor) * norm_gain).astype(jnp.bfloat16)

    def project(weight):
        return jnp.dot(normed, weight, preferred_element_type=jnp.float32).astype(jnp.bfloat16)

    def shifted(raw_proj, mix_row):
        current = raw_proj.astype(jnp.float32)
        earlier = jnp.concatenate([jnp.zeros((1, current.shape[1]), jnp.float32), current[:-1]], axis=0)
        return current + (earlier - current) * mix_row
    recept = shifted(project(w_recept), shift_mix[0])
    key = shifted(project(w_key), shift_mix[1])
    value = shifted(project(w_value), shift_mix[2])
    level = decay_base + project(w_decay).astype(jnp.float32) + decay_drift[:, None]
    decay = jnp.exp(-jnp.exp(-jax.nn.softplus(-level) - 0.5))
    rate = jax.nn.sigmoid(rate_base + project(w_rate).astype(jnp.float32))
    gate = jax.nn.sigmoid(project(w_gate).astype(jnp.float32))

    def heads(array):
        return array.reshape(TOKENS, HEADS, HEAD)
    key_heads = heads(key)
    unit = key_heads * lax.rsqrt(lax.optimization_barrier(jnp.sum(key_heads * key_heads, axis=-1, keepdims=True)) + 1.0)

    def advance(state, inputs):
        recept_now, decay_now, key_now, value_now, unit_now, rate_now = inputs
        removed = jnp.einsum('hvk,hk->hv', state, unit_now, precision=highest)
        state = state * decay_now[:, None, :] - removed[:, :, None] * (unit_now * rate_now)[:, None, :] + value_now[:, :, None] * key_now[:, None, :]
        return (state, jnp.einsum('hvk,hk->hv', state, recept_now, precision=highest))
    _, mixed = lax.scan(advance, initial_state, (heads(recept), heads(decay), key_heads, heads(value), unit, heads(rate)))
    center = mixed - lax.optimization_barrier(jnp.mean(mixed, axis=-1, keepdims=True))
    spread = lax.optimization_barrier(jnp.mean(center * center, axis=-1, keepdims=True))
    scaled = center * lax.rsqrt(spread + group_floor) * group_gain.reshape(HEADS, HEAD)
    gated = (scaled.reshape(TOKENS, INNER) * gate).astype(jnp.bfloat16)
    return jnp.dot(gated, w_out, preferred_element_type=jnp.float32).astype(jnp.bfloat16)
```

```python
import functools

import jax
import jax.numpy as jnp
from jax import lax
from jax.experimental import pallas as pl
from jax.experimental.pallas import tpu as pltpu
from jax.sharding import Mesh
from jax.sharding import PartitionSpec as P

HEAD = 64
BLOCK = 64
PAIR = 128
SP = ("z", "x", "c")
SP_TP = ("z", "x", "c", "tp")
AXES = ("z", "x", "c", "tp")
MESH = pl.DeviceIdType.MESH
NORM_FLOOR = 0.5
GROUP_FLOOR = 1.0
EXP_HALF = 0.6065306597126334
f32 = jnp.float32
bf16 = jnp.bfloat16
VMEM_SPEC = pl.BlockSpec(memory_space=pltpu.VMEM)
ANY_SPEC = pl.BlockSpec(memory_space=pl.ANY)
SMEM_SPEC = pl.BlockSpec(memory_space=pltpu.SMEM)


def here():
    return {axis: lax.axis_index(axis) for axis in AXES}


def split(x):
    hi = x.astype(bf16)
    lo = (x - hi.astype(f32)).astype(bf16)
    return hi, lo


def sigmoid(x):
    return 1.0 / (1.0 + jnp.exp(-x))


def gather_project(tokens, gain, wr, wk, wv, wd, wa, wg, proj, edge_out, own, held, last, last_in, wbuf, norm_buf,
                   own_sem, w_sem, send_sem, recv_sem, edge_send, edge_recv):
    me = here()
    y = me["tp"]
    ny = lax.axis_size("tp")
    nx, nc, nz = lax.axis_size("x"), lax.axis_size("c"), lax.axis_size("z")
    right, left = lax.rem(y + 1, ny), lax.rem(y + ny - 1, ny)
    seq = (me["z"] * nx + me["x"]) * nc + me["c"]
    total = nx * nc * nz

    def at(index, tp):
        return {"z": index // (nx * nc), "x": lax.rem(index // nc, nx), "c": lax.rem(index, nc), "tp": tp}

    rows = own.shape[0]
    half = rows // 2
    weights = (wr, wk, wv, wd, wa, wg)
    fetch = pltpu.make_async_copy(tokens, own, own_sem)
    fetch.start()
    w_copies = [pltpu.make_async_copy(w, wbuf.at[i], w_sem.at[i]) for i, w in enumerate(weights)]
    for copy in w_copies:
        copy.start()
    barrier = pltpu.get_barrier_semaphore()
    for peer in (left, right):
        pl.semaphore_signal(barrier, inc=1, device_id={"tp": peer}, device_id_type=MESH)

    sends_edge = jnp.logical_and(y == ny - 1, seq < total - 1)
    gets_edge = seq > 0

    @pl.when(gets_edge)
    def _():
        pl.semaphore_signal(barrier, inc=1, device_id=at(seq - 1, ny - 1), device_id_type=MESH)

    pl.semaphore_wait(barrier, 2 + 4 * sends_edge.astype(jnp.int32))
    fetch.wait()

    def part(h):
        return pl.ds(h * half, half)

    def hop(src, slot, h, to, sem):
        return pltpu.make_async_remote_copy(
            src_ref=src, dst_ref=held.at[slot, part(h)], send_sem=send_sem.at[sem], recv_sem=recv_sem.at[slot, h],
            device_id={"tp": to}, device_id_type=MESH)

    to_right = [hop(own.at[part(h)], 0, h, right, h) for h in (0, 1)]
    to_left = [hop(own.at[part(h)], 2, h, left, 2 + h) for h in (0, 1)]
    on_right = hop(held.at[0, part(0)], 1, 0, right, 4)
    on_left = hop(held.at[2, part(1)], 1, 1, left, 5)
    to_right[0].start()
    to_left[1].start()
    to_right[1].start()
    to_left[0].start()

    last[...] = own[rows - 16:rows, :].astype(f32)[15:16, :]
    edges = [pltpu.make_async_remote_copy(
        src_ref=last, dst_ref=last_in, send_sem=edge_send.at[k], recv_sem=edge_recv,
        device_id=at(lax.rem(seq + 1, total), k), device_id_type=MESH) for k in range(4)]

    @pl.when(sends_edge)
    def _():
        for copy in edges:
            copy.start()

    def normalize(x):
        return (x * lax.rsqrt(jnp.mean(x * x, axis=-1, keepdims=True) + NORM_FLOOR) * gain[...]).astype(bf16)

    def project(block, base, with_edge):
        norm_buf[0:rows, :] = normalize(block[...].astype(f32))
        count = rows + 16 if with_edge else rows
        for i in range(6):
            res = jnp.dot(norm_buf[0:count, :], wbuf[i], preferred_element_type=f32)
            proj[pl.ds(pl.multiple_of(base, 16), rows), 256 * i:256 * (i + 1)] = res[0:rows].astype(bf16)
            if with_edge and i < 3:
                edge_out[0:1, 256 * i:256 * (i + 1)] = res[rows:rows + 1].astype(bf16).astype(f32)

    for copy in w_copies:
        copy.wait()
    project(own, y * rows, False)
    to_right[0].wait_recv()
    on_right.start()
    to_left[1].wait_recv()
    on_left.start()
    to_right[1].wait_recv()
    project(held.at[0], left * rows, False)
    to_left[0].wait_recv()
    project(held.at[2], right * rows, False)

    @pl.when(gets_edge)
    def _():
        edges[0].wait_recv()

    @pl.when(jnp.logical_not(gets_edge))
    def _():
        last_in[...] = jnp.zeros_like(last_in)

    norm_buf[rows:rows + 16, :] = normalize(jnp.broadcast_to(last_in[...], (16, last_in.shape[1])))
    on_right.wait_recv()
    on_left.wait_recv()
    project(held.at[1], lax.rem(y + 2, ny) * rows, True)
    for copy in (*to_right, *to_left, on_right, on_left):
        copy.wait_send()

    @pl.when(sends_edge)
    def _():
        for copy in edges:
            copy.wait_send()


def call_gather(tokens, gain, weights):
    rows, depth = tokens.shape
    width = weights[0].shape[1]
    return pl.pallas_call(
        gather_project,
        out_shape=(jax.ShapeDtypeStruct((4 * rows, 6 * width), bf16), jax.ShapeDtypeStruct((8, 3 * width), f32)),
        in_specs=[ANY_SPEC, VMEM_SPEC] + [ANY_SPEC] * 6,
        out_specs=(VMEM_SPEC, VMEM_SPEC),
        scratch_shapes=[
            pltpu.VMEM((rows, depth), bf16),
            pltpu.VMEM((3, rows, depth), bf16),
            pltpu.VMEM((1, depth), f32),
            pltpu.VMEM((1, depth), f32),
            pltpu.VMEM((6, depth, width), bf16),
            pltpu.VMEM((rows + 16, depth), bf16),
            pltpu.SemaphoreType.DMA(()),
            pltpu.SemaphoreType.DMA((6,)),
            pltpu.SemaphoreType.DMA((6,)),
            pltpu.SemaphoreType.DMA((3, 2)),
            pltpu.SemaphoreType.DMA((4,)),
            pltpu.SemaphoreType.DMA(()),
        ],
        compiler_params=pltpu.CompilerParams(collective_id=0, has_side_effects=True),
        name="gather_project",
    )(tokens, gain, *weights)


def lane_masks(dtype):
    lane = lax.broadcasted_iota(jnp.int32, (1, PAIR), 1)
    low = (lane < HEAD).astype(f32)
    return low.astype(dtype), (1.0 - low).astype(dtype)


def lhs3(x):
    hi, lo = split(x)
    return jnp.concatenate([hi, lo, hi], axis=1)


def diag_parts(x, masks):
    hi, lo = split(x)
    low, high = masks
    bd_hi = jnp.concatenate([hi * low, hi * high], axis=0)
    bd_lo = jnp.concatenate([lo * low, lo * high], axis=0)
    return bd_hi, bd_lo


def rhs_nn(x, masks):
    hi, lo = diag_parts(x, masks)
    return jnp.concatenate([hi, hi, lo], axis=0)


def rhs_nt(x, masks):
    hi, lo = diag_parts(x, masks)
    return jnp.concatenate([hi, hi, lo], axis=1)


def nn(a3, b3):
    return jnp.dot(a3, b3, preferred_element_type=f32)


def nt(a3, b3):
    return lax.dot_general(a3, b3, (((1,), (1,)), ((), ())), preferred_element_type=f32)


def tn(a, b):
    a_hi, a_lo = split(a)
    b_hi, b_lo = split(b)
    return lax.dot_general(
        jnp.concatenate([a_hi, a_lo, a_hi], axis=0), jnp.concatenate([b_hi, b_hi, b_lo], axis=0),
        (((0,), (0,)), ((), ())), preferred_element_type=f32)


def head_sum(x, masks):
    low, high = masks
    ones = jnp.concatenate([jnp.broadcast_to(low, (HEAD, PAIR)), jnp.broadcast_to(high, (HEAD, PAIR))], axis=0)
    hi, lo = split(x)
    return jnp.dot(jnp.concatenate([hi, lo], axis=1), jnp.concatenate([ones, ones], axis=0), preferred_element_type=f32)


def prepare(proj, edge, mix, base, rate_base, drift, reads_out, fixed_out, gate_out, msg,
            recept_s, key_s, value_s, unit_s, rate_s, logs_s, reads_s, fixed_s, trans_s, added_s):
    rows = proj.shape[0]
    width = proj.shape[1] // 6
    pairs = width // PAIR
    chunks = rows // BLOCK
    masks = lane_masks(bf16)
    lane = lax.broadcasted_iota(jnp.int32, (1, PAIR), 1)
    is_low = lane < HEAD
    for j in range(pairs):
        cols = slice(j * PAIR, (j + 1) * PAIR)
        first = lax.broadcasted_iota(jnp.int32, (rows, PAIR), 0) == 0

        def raw(i):
            return proj[:, i * width + j * PAIR:i * width + (j + 1) * PAIR].astype(f32)

        def shifted(i):
            now = raw(i)
            before = jnp.where(first, edge[0:1, i * width + j * PAIR:i * width + (j + 1) * PAIR], pltpu.roll(now, 1, 0))
            return now + (before - now) * mix[i:i + 1, cols]

        recept_s[:, cols] = shifted(0)
        key = shifted(1)
        key_s[:, cols] = key
        value_s[:, cols] = shifted(2)
        unit_s[:, cols] = key * lax.rsqrt(head_sum(key * key, masks) + 1.0)
        rate_s[:, cols] = sigmoid(rate_base[:, cols] + raw(4))
        gate_out[:, cols] = sigmoid(raw(5))
        for c in range(chunks):
            block = slice(c * BLOCK, (c + 1) * BLOCK)
            level = base[:, cols] + raw(3)[block] + drift[0, c * BLOCK]
            logs_s[block, cols] = -EXP_HALF * sigmoid(level)

    place = lax.broadcasted_iota(jnp.int32, (BLOCK, PAIR), 0)
    other = lax.rem(lax.broadcasted_iota(jnp.int32, (BLOCK, PAIR), 1), BLOCK)
    strict = other < place
    inclusive = other <= place
    eye = (other == place).astype(f32)
    tri2 = inclusive.astype(f32).astype(bf16)

    def step(c, _):
        block = pl.ds(pl.multiple_of(c * BLOCK, BLOCK), BLOCK)
        for j in range(pairs):
            cols = slice(j * PAIR, (j + 1) * PAIR)
            logs = logs_s[block, cols]
            unit = unit_s[block, cols]
            key = key_s[block, cols]
            value = value_s[block, cols]
            run = jnp.dot(tri2, jnp.concatenate(split(logs), axis=0), preferred_element_type=f32)
            last = run[BLOCK - 1:BLOCK, :]
            inverse = jnp.exp(-run)
            to_end = jnp.exp(last - run)
            unit_rate = unit * rate_s[block, cols]
            alpha = -unit * jnp.exp(run - logs)
            scaled = recept_s[block, cols] * jnp.exp(run)
            left = lhs3(jnp.concatenate([alpha, scaled], axis=0))
            by_beta = nt(left, rhs_nt(unit_rate * inverse, masks))
            by_key = nt(left, rhs_nt(key * inverse, masks))
            lower = jnp.where(strict, by_beta[:BLOCK], 0.0)
            lower_ak = jnp.where(strict, by_key[:BLOCK], 0.0)
            upper_b = lhs3(jnp.where(inclusive, by_beta[BLOCK:], 0.0))
            upper_k = lhs3(jnp.where(inclusive, by_key[BLOCK:], 0.0))
            solved = eye + jnp.where(lax.div(place, 2) == lax.div(other, 2), lower, 0.0)
            size = 2
            while size < BLOCK:
                inside = jnp.logical_and(
                    lax.div(place, 2 * size) == lax.div(other, 2 * size),
                    lax.div(place, size) != lax.div(other, size))
                corner = jnp.where(inside, lower, 0.0)
                turned = nn(lhs3(solved), rhs_nn(corner, masks))
                solved = solved + nn(lhs3(turned), rhs_nn(solved, masks))
                size *= 2
            value3 = rhs_nn(value, masks)
            solved3 = lhs3(solved)
            solved_alpha = nn(solved3, rhs_nn(alpha, masks))
            pulled = nn(lhs3(lower_ak), value3)
            solved_value = nn(solved3, rhs_nn(pulled, masks))
            reads_s[block, cols] = scaled + nn(upper_b, rhs_nn(solved_alpha, masks))
            fixed_s[block, cols] = nn(upper_b, rhs_nn(solved_value, masks)) + nn(upper_k, value3)
            beta_end = unit_rate * to_end
            cross = tn(solved_alpha, beta_end)
            trans_s[block, cols] = jnp.where(is_low, cross[:BLOCK], cross[BLOCK:]) + eye * jnp.exp(last)
            cross = tn(jnp.concatenate([solved_value, value], axis=0), jnp.concatenate([beta_end, key * to_end], axis=0))
            added_s[block, cols] = jnp.where(is_low, cross[:BLOCK], cross[BLOCK:])
        return 0

    lax.fori_loop(0, chunks, step, 0)

    zero = jnp.zeros((BLOCK, PAIR), f32)
    for j in range(pairs):
        cols = slice(j * PAIR, (j + 1) * PAIR)
        both = jnp.concatenate([eye, zero], axis=0)
        for c in range(chunks):
            block = slice(c * BLOCK, (c + 1) * BLOCK)
            if c == 0:
                reads_out[block, cols] = reads_s[block, cols]
                fixed_out[block, cols] = fixed_s[block, cols]
                both = jnp.concatenate([trans_s[block, cols], added_s[block, cols]], axis=0)
                continue
            reads = lhs3(reads_s[block, cols])
            reads_out[block, cols] = nt(reads, rhs_nt(both[:BLOCK], masks))
            fixed_out[block, cols] = fixed_s[block, cols] + nt(reads, rhs_nt(both[BLOCK:], masks))
            both = nn(lhs3(both), rhs_nn(trans_s[block, cols], masks)) + jnp.concatenate(
                [zero, added_s[block, cols]], axis=0)
        for side in range(2):
            head = 2 * j + side
            packed = pack(both[:BLOCK], side)
            for q in range(2):
                msg[2 * head + q, 0:32, :] = packed
                msg[2 * head + q, 32:48, :] = pack(both[BLOCK + 32 * q:BLOCK + 32 * (q + 1)], side)


def pack(x, side):
    half = x.shape[0] // 2
    is_low = lax.broadcasted_iota(jnp.int32, (half, PAIR), 1) < HEAD
    top, bottom = x[:half], x[half:]
    if side == 0:
        return jnp.where(is_low, top, pltpu.roll(bottom, HEAD, 1))
    return jnp.where(is_low, pltpu.roll(top, HEAD, 1), bottom)


def unpack(x):
    is_low = lax.broadcasted_iota(jnp.int32, x.shape, 1) < HEAD
    return jnp.concatenate([jnp.where(is_low, x, 0.0), jnp.where(is_low, pltpu.roll(x, HEAD, 1), 0.0)], axis=0)


def call_prepare(proj, edge, mix, base, rate_base, drift):
    rows = proj.shape[0]
    width = proj.shape[1] // 6
    wide = jax.ShapeDtypeStruct((rows, width), f32)
    return pl.pallas_call(
        prepare,
        out_shape=(wide, wide, wide, jax.ShapeDtypeStruct((8, 48, PAIR), f32)),
        in_specs=[VMEM_SPEC] * 5 + [SMEM_SPEC],
        out_specs=(VMEM_SPEC,) * 4,
        scratch_shapes=[pltpu.VMEM((rows, width), f32)] * 10,
        name="prepare",
        cost_estimate=pl.CostEstimate(flops=3 * 10**9, bytes_accessed=4 * 10**6, transcendentals=10**6),
    )(proj, edge, mix, base, rate_base, drift)


def state_lhs(x):
    hi = x.astype(bf16).astype(f32)
    joined = hi + pltpu.roll(x - hi, HEAD, 1)
    return jnp.concatenate([joined.astype(bf16), hi.astype(bf16)], axis=1)


def state_rhs(x):
    hi, lo = split(x)
    return jnp.concatenate([hi, hi, lo, jnp.zeros_like(lo)], axis=0)


def carry(msg, start, out, slab, slab_sum, across, pre_map, pre_add, back,
          send1, recv1, send2, recv2, send3, recv3):
    me = here()
    nx, nc, nz = lax.axis_size("x"), lax.axis_size("c"), lax.axis_size("z")
    z = me["z"]
    unit = me["x"] * nc + me["c"]
    units = nx * nc

    def in_slab(index):
        return {"z": z, "x": index // nc, "c": lax.rem(index, nc), "tp": me["tp"]}

    def along(index):
        return {"z": index, "x": me["x"], "c": me["c"], "tp": me["tp"]}

    barrier = pltpu.get_barrier_semaphore()
    for d in range(1, units):
        pl.semaphore_signal(barrier, inc=1, device_id=in_slab(lax.rem(unit + d, units)), device_id_type=MESH)
    for d in range(1, nz):
        pl.semaphore_signal(barrier, inc=1, device_id=along(lax.rem(z + d, nz)), device_id_type=MESH)
    pl.semaphore_wait(barrier, units + nz - 2)

    first = []
    for d in range(1, units):
        peer = lax.rem(unit + d, units)
        copy = pltpu.make_async_remote_copy(
            src_ref=msg.at[peer], dst_ref=slab.at[unit], send_sem=send1.at[d], recv_sem=recv1.at[unit],
            device_id=in_slab(peer), device_id_type=MESH)
        copy.start()
        first.append(copy)
    slab[unit] = msg[unit]

    def landed(buffer, sems, k):
        return pltpu.make_async_remote_copy(
            src_ref=buffer.at[k], dst_ref=buffer.at[k], send_sem=send1.at[0], recv_sem=sems.at[k],
            device_id=in_slab(unit), device_id_type=MESH)

    running = jnp.zeros((96, PAIR), f32)
    row = lax.broadcasted_iota(jnp.int32, (96, PAIR), 0)
    col = lax.broadcasted_iota(jnp.int32, (96, PAIR), 1)
    running = (row == col).astype(f32) * (col < HEAD).astype(f32)
    for k in range(8):
        @pl.when(k != unit)
        def _():
            landed(slab, recv1, k).wait_recv()

        pre_map[k] = state_rhs(running[:HEAD])
        pre_add[k] = running[HEAD:]
        piece = slab[k]
        add = jnp.concatenate([jnp.zeros((HEAD, PAIR), f32), unpack(piece[32:48])], axis=0)
        running = nn(state_lhs(running), state_rhs(unpack(piece[0:32]))) + add
    slab_sum[0:32, :] = pack(running[:HEAD], 0)
    slab_sum[32:48, :] = pack(running[HEAD:], 0)

    def onward(d):
        return pltpu.make_async_remote_copy(
            src_ref=slab_sum, dst_ref=across.at[z], send_sem=send2.at[d], recv_sem=recv2.at[z],
            device_id=along(lax.rem(z + d, nz)), device_id_type=MESH)

    for d in range(1, 8):
        @pl.when(z + d < nz)
        def _():
            onward(d).start()

    head = start[me["x"], pl.ds(pl.multiple_of(me["c"] * 32, 32), 32), :]
    state = jnp.concatenate([head, jnp.zeros((32, PAIR - HEAD), f32)], axis=1)
    for k in range(7):
        @pl.when(k < z)
        def _():
            landed(across, recv2, k).wait_recv()

        piece = across[k]
        new = nn(state_lhs(state), state_rhs(unpack(piece[0:32]))) + unpack(piece[32:48])
        state = jnp.where(k < z, new, state)

    state3 = state_lhs(state)
    for k in range(8):
        back[k] = pack(nn(state3, pre_map[k]) + pre_add[k], 0)
    last = []
    for d in range(1, units):
        peer = lax.rem(unit + d, units)
        copy = pltpu.make_async_remote_copy(
            src_ref=back.at[peer], dst_ref=out.at[unit], send_sem=send3.at[d], recv_sem=recv3.at[unit],
            device_id=in_slab(peer), device_id_type=MESH)
        copy.start()
        last.append(copy)
    out[unit] = back[unit]
    for k in range(8):
        @pl.when(k != unit)
        def _():
            landed(out, recv3, k).wait_recv()
    for copy in first + last:
        copy.wait_send()
    for d in range(1, 8):
        @pl.when(z + d < nz)
        def _():
            onward(d).wait_send()


def call_carry(msg, start):
    return pl.pallas_call(
        carry,
        out_shape=jax.ShapeDtypeStruct((8, 16, PAIR), f32),
        in_specs=[VMEM_SPEC, VMEM_SPEC],
        out_specs=VMEM_SPEC,
        scratch_shapes=[
            pltpu.VMEM((8, 48, PAIR), f32),
            pltpu.VMEM((48, PAIR), f32),
            pltpu.VMEM((8, 48, PAIR), f32),
            pltpu.VMEM((8, 256, PAIR), bf16),
            pltpu.VMEM((8, 32, PAIR), f32),
            pltpu.VMEM((8, 16, PAIR), f32),
        ] + [pltpu.SemaphoreType.DMA((8,))] * 6,
        compiler_params=pltpu.CompilerParams(collective_id=1, has_side_effects=True),
        name="carry",
    )(msg, start)


def finish(reads, fixed, gate, state, gains, w_out, out, gated, token_rows, wbuf, w_sem, send_sem, recv_sem):
    me = here()
    y = me["tp"]
    ny = lax.axis_size("tp")
    fetch = pltpu.make_async_copy(w_out, wbuf, w_sem)
    fetch.start()
    barrier = pltpu.get_barrier_semaphore()
    for d in range(1, 4):
        pl.semaphore_signal(barrier, inc=1, device_id={"tp": lax.rem(y + d, ny)}, device_id_type=MESH)
    rows, width = reads.shape
    share = rows // 4
    masks = lane_masks(bf16)
    is_low = lax.broadcasted_iota(jnp.int32, (16, PAIR), 1) < HEAD
    for j in range(width // PAIR):
        cols = slice(j * PAIR, (j + 1) * PAIR)
        parts = []
        for q in range(2):
            a, b = state[4 * j + q], state[4 * j + 2 + q]
            parts.append(jnp.where(is_low, a, pltpu.roll(b, HEAD, 1)))
            parts.append(jnp.where(is_low, pltpu.roll(a, HEAD, 1), b))
        entering = jnp.concatenate(parts, axis=0)
        mixed = fixed[:, cols] + nt(lhs3(reads[:, cols]), rhs_nt(entering, masks))
        center = mixed - head_sum(mixed, masks) * (1.0 / HEAD)
        spread = head_sum(center * center, masks) * (1.0 / HEAD)
        scaled = center * lax.rsqrt(spread + GROUP_FLOOR) * gains[:, cols]
        gated[:, cols] = (scaled * gate[:, cols]).astype(bf16)
    pl.semaphore_wait(barrier, 3)

    def part(k):
        return pl.ds(pl.multiple_of(k * share, 16), share)

    copies = []
    for d in range(1, 4):
        peer = lax.rem(y + d, ny)
        copy = pltpu.make_async_remote_copy(
            src_ref=gated.at[part(peer)], dst_ref=token_rows.at[d], send_sem=send_sem.at[d], recv_sem=recv_sem.at[d],
            device_id={"tp": peer}, device_id_type=MESH)
        copy.start()
        copies.append(copy)
    fetch.wait()
    token_rows[0] = gated[part(y), :]
    for d in range(1, 4):
        copies[d - 1].wait_recv()
    total = jnp.zeros(out.shape, f32)
    for d in range(4):
        owner = lax.rem(y + ny - d, ny)
        total = total + jnp.dot(token_rows[d], wbuf[pl.ds(pl.multiple_of(owner * width, width), width), :],
                                preferred_element_type=f32)
    out[...] = total.astype(bf16)
    for copy in copies:
        copy.wait_send()


def call_finish(reads, fixed, gate, state, gains, w_out):
    rows, width = reads.shape
    share = rows // 4
    inner, depth = w_out.shape
    return pl.pallas_call(
        finish,
        out_shape=jax.ShapeDtypeStruct((share, depth), bf16),
        in_specs=[VMEM_SPEC] * 5 + [ANY_SPEC],
        out_specs=VMEM_SPEC,
        scratch_shapes=[
            pltpu.VMEM((rows, width), bf16),
            pltpu.VMEM((4, share, width), bf16),
            pltpu.VMEM((inner, depth), bf16),
            pltpu.SemaphoreType.DMA(()),
            pltpu.SemaphoreType.DMA((4,)),
            pltpu.SemaphoreType.DMA((4,)),
        ],
        compiler_params=pltpu.CompilerParams(collective_id=2, has_side_effects=True),
        name="finish",
    )(reads, fixed, gate, state, gains, w_out)


def per_device(tokens, norm_gain, w_recept, w_key, w_value, w_decay, w_rate, w_gate, shift_mix, decay_base, rate_base,
               decay_drift, group_gain, initial_state, w_out):
    proj, edge = call_gather(
        tokens, norm_gain.reshape(1, -1), (w_recept, w_key, w_value, w_decay, w_rate, w_gate))
    reads, fixed, gate, msg = call_prepare(
        proj, edge, shift_mix, decay_base.reshape(1, -1), rate_base.reshape(1, -1), decay_drift.reshape(1, -1))
    state = call_carry(msg, initial_state)
    return call_finish(reads, fixed, gate, state, group_gain.reshape(1, -1), w_out)


def solution(mesh):
    finer = Mesh(mesh.devices.reshape(8, 4, 2, mesh.shape["tp"]), AXES)
    in_specs = (
        P(SP_TP, None),
        P(),
        P(None, "tp"),
        P(None, "tp"),
        P(None, "tp"),
        P(None, "tp"),
        P(None, "tp"),
        P(None, "tp"),
        P(None, "tp"),
        P("tp"),
        P("tp"),
        P(SP),
        P("tp"),
        P("tp", None, None),
        P(),
    )
    return jax.shard_map(
        per_device, mesh=finer, in_specs=in_specs, out_specs=P(SP_TP, None), check_vma=False
    )
```

```python
import functools

import jax
import jax.numpy as jnp
from jax import lax
from jax.experimental import pallas as pl
from jax.experimental.pallas import tpu as pltpu
from jax.sharding import Mesh
from jax.sharding import PartitionSpec as P

HEAD = 64
BLOCK = 64
PAIR = 128
GROUP = 3
SP = ("z", "x", "c")
SP_TP = ("z", "x", "c", "tp")
AXES = ("z", "x", "c", "tp")
MESH = pl.DeviceIdType.MESH
NORM_FLOOR = 0.5
GROUP_FLOOR = 1.0
EXP_HALF = 0.6065306597126334
f32 = jnp.float32
bf16 = jnp.bfloat16
VMEM_SPEC = pl.BlockSpec(memory_space=pltpu.VMEM)
ANY_SPEC = pl.BlockSpec(memory_space=pl.ANY)
SMEM_SPEC = pl.BlockSpec(memory_space=pltpu.SMEM)


def here():
    return {axis: lax.axis_index(axis) for axis in AXES}


def split(x):
    hi = x.astype(bf16)
    lo = (x - hi.astype(f32)).astype(bf16)
    return hi, lo


def sigmoid(x):
    return 1.0 / (1.0 + jnp.exp(-x))


def gather_project(tokens, gain, wr, wk, wv, wd, wa, wg, proj, edge_out, own, held, last, last_in, wbuf, norm_buf,
                   own_sem, w_sem, send_sem, recv_sem, edge_send, edge_recv):
    me = here()
    y = me["tp"]
    ny = lax.axis_size("tp")
    nx, nc, nz = lax.axis_size("x"), lax.axis_size("c"), lax.axis_size("z")
    right, left = lax.rem(y + 1, ny), lax.rem(y + ny - 1, ny)
    seq = (me["z"] * nx + me["x"]) * nc + me["c"]
    total = nx * nc * nz

    def at(index, tp):
        return {"z": index // (nx * nc), "x": lax.rem(index // nc, nx), "c": lax.rem(index, nc), "tp": tp}

    rows = own.shape[0]
    half = rows // 2
    weights = (wr, wk, wv, wd, wa, wg)
    fetch = pltpu.make_async_copy(tokens, own, own_sem)
    fetch.start()
    w_copies = [pltpu.make_async_copy(w, wbuf.at[i], w_sem.at[i]) for i, w in enumerate(weights)]
    for copy in w_copies:
        copy.start()
    barrier = pltpu.get_barrier_semaphore()
    for peer in (left, right):
        pl.semaphore_signal(barrier, inc=1, device_id={"tp": peer}, device_id_type=MESH)

    sends_edge = jnp.logical_and(y == ny - 1, seq < total - 1)
    gets_edge = seq > 0

    @pl.when(gets_edge)
    def _():
        pl.semaphore_signal(barrier, inc=1, device_id=at(seq - 1, ny - 1), device_id_type=MESH)

    pl.semaphore_wait(barrier, 2 + 4 * sends_edge.astype(jnp.int32))
    fetch.wait()

    def part(h):
        return pl.ds(h * half, half)

    def hop(src, slot, h, to, sem):
        return pltpu.make_async_remote_copy(
            src_ref=src, dst_ref=held.at[slot, part(h)], send_sem=send_sem.at[sem], recv_sem=recv_sem.at[slot, h],
            device_id={"tp": to}, device_id_type=MESH)

    to_right = [hop(own.at[part(h)], 0, h, right, h) for h in (0, 1)]
    to_left = [hop(own.at[part(h)], 2, h, left, 2 + h) for h in (0, 1)]
    on_right = hop(held.at[0, part(0)], 1, 0, right, 4)
    on_left = hop(held.at[2, part(1)], 1, 1, left, 5)
    to_right[0].start()
    to_left[1].start()
    to_right[1].start()
    to_left[0].start()

    last[...] = own[rows - 16:rows, :].astype(f32)[15:16, :]
    edges = [pltpu.make_async_remote_copy(
        src_ref=last, dst_ref=last_in, send_sem=edge_send.at[k], recv_sem=edge_recv,
        device_id=at(lax.rem(seq + 1, total), k), device_id_type=MESH) for k in range(4)]

    @pl.when(sends_edge)
    def _():
        for copy in edges:
            copy.start()

    def normalize(x):
        return (x * lax.rsqrt(jnp.mean(x * x, axis=-1, keepdims=True) + NORM_FLOOR) * gain[...]).astype(bf16)

    def project(block, base, with_edge):
        norm_buf[0:rows, :] = normalize(block[...].astype(f32))
        count = rows + 16 if with_edge else rows
        for i in range(6):
            res = jnp.dot(norm_buf[0:count, :], wbuf[i], preferred_element_type=f32)
            proj[pl.ds(pl.multiple_of(base, 16), rows), 256 * i:256 * (i + 1)] = res[0:rows].astype(bf16)
            if with_edge and i < 3:
                edge_out[0:1, 256 * i:256 * (i + 1)] = res[rows:rows + 1].astype(bf16).astype(f32)

    for copy in w_copies:
        copy.wait()
    project(own, y * rows, False)
    to_right[0].wait_recv()
    on_right.start()
    to_left[1].wait_recv()
    on_left.start()
    to_right[1].wait_recv()
    project(held.at[0], left * rows, False)
    to_left[0].wait_recv()
    project(held.at[2], right * rows, False)

    @pl.when(gets_edge)
    def _():
        edges[0].wait_recv()

    @pl.when(jnp.logical_not(gets_edge))
    def _():
        last_in[...] = jnp.zeros_like(last_in)

    norm_buf[rows:rows + 16, :] = normalize(jnp.broadcast_to(last_in[...], (16, last_in.shape[1])))
    on_right.wait_recv()
    on_left.wait_recv()
    project(held.at[1], lax.rem(y + 2, ny) * rows, True)
    for copy in (*to_right, *to_left, on_right, on_left):
        copy.wait_send()

    @pl.when(sends_edge)
    def _():
        for copy in edges:
            copy.wait_send()


def call_gather(tokens, gain, weights):
    rows, depth = tokens.shape
    width = weights[0].shape[1]
    return pl.pallas_call(
        gather_project,
        out_shape=(jax.ShapeDtypeStruct((4 * rows, 6 * width), bf16), jax.ShapeDtypeStruct((8, 3 * width), f32)),
        in_specs=[ANY_SPEC, VMEM_SPEC] + [ANY_SPEC] * 6,
        out_specs=(VMEM_SPEC, VMEM_SPEC),
        scratch_shapes=[
            pltpu.VMEM((rows, depth), bf16),
            pltpu.VMEM((3, rows, depth), bf16),
            pltpu.VMEM((1, depth), f32),
            pltpu.VMEM((1, depth), f32),
            pltpu.VMEM((6, depth, width), bf16),
            pltpu.VMEM((rows + 16, depth), bf16),
            pltpu.SemaphoreType.DMA(()),
            pltpu.SemaphoreType.DMA((6,)),
            pltpu.SemaphoreType.DMA((6,)),
            pltpu.SemaphoreType.DMA((3, 2)),
            pltpu.SemaphoreType.DMA((4,)),
            pltpu.SemaphoreType.DMA(()),
        ],
        compiler_params=pltpu.CompilerParams(collective_id=0, has_side_effects=True),
        name="gather_project",
    )(tokens, gain, *weights)


def lane_masks(dtype):
    lane = lax.broadcasted_iota(jnp.int32, (1, PAIR), 1)
    low = (lane < HEAD).astype(f32)
    return low.astype(dtype), (1.0 - low).astype(dtype)


def lhs3(x):
    hi, lo = split(x)
    return jnp.concatenate([hi, lo, hi], axis=1)


def diag_parts(x, masks):
    hi, lo = split(x)
    low, high = masks
    bd_hi = jnp.concatenate([hi * low, hi * high], axis=0)
    bd_lo = jnp.concatenate([lo * low, lo * high], axis=0)
    return bd_hi, bd_lo


def rhs_nn(x, masks):
    hi, lo = diag_parts(x, masks)
    return jnp.concatenate([hi, hi, lo], axis=0)


def rhs_nt(x, masks):
    hi, lo = diag_parts(x, masks)
    return jnp.concatenate([hi, hi, lo], axis=1)


def nn(a3, b3):
    return jnp.dot(a3, b3, preferred_element_type=f32)


def nt(a3, b3):
    return lax.dot_general(a3, b3, (((1,), (1,)), ((), ())), preferred_element_type=f32)


def tn(a, b):
    a_hi, a_lo = split(a)
    b_hi, b_lo = split(b)
    return lax.dot_general(
        jnp.concatenate([a_hi, a_lo, a_hi], axis=0), jnp.concatenate([b_hi, b_hi, b_lo], axis=0),
        (((0,), (0,)), ((), ())), preferred_element_type=f32)


def head_sum(x, masks):
    low, high = masks
    ones = jnp.concatenate([jnp.broadcast_to(low, (HEAD, PAIR)), jnp.broadcast_to(high, (HEAD, PAIR))], axis=0)
    hi, lo = split(x)
    return jnp.dot(jnp.concatenate([hi, lo], axis=1), jnp.concatenate([ones, ones], axis=0), preferred_element_type=f32)


def state_group(base, edge_row, proj, mix, decay_base, rate_base, drift, store):
    recept_s, value_s, alpha_s, pulled_s, upper_b, upper_k, trans_s, added_s = store
    width = recept_s.shape[1]
    pairs = width // PAIR
    rows = GROUP * BLOCK
    masks = lane_masks(bf16)
    is_low = lax.broadcasted_iota(jnp.int32, (1, PAIR), 1) < HEAD
    place = lax.broadcasted_iota(jnp.int32, (BLOCK, PAIR), 0)
    other = lax.rem(lax.broadcasted_iota(jnp.int32, (BLOCK, PAIR), 1), BLOCK)
    strict = other < place
    inclusive = other <= place
    eye = (other == place).astype(f32)
    tri2 = inclusive.astype(f32).astype(bf16)
    area = pl.ds(pl.multiple_of(base, BLOCK), rows)
    units = [(i, j) for i in range(GROUP) for j in range(pairs)]

    def block(i):
        return pl.ds(pl.multiple_of(base + i * BLOCK, BLOCK), BLOCK)

    def cols(j):
        return slice(j * PAIR, (j + 1) * PAIR)

    logs, unit, rate, key, value, recept = {}, {}, {}, {}, {}, {}
    first = lax.broadcasted_iota(jnp.int32, (rows, PAIR), 0) == 0
    for j in range(pairs):
        def raw(i):
            return proj[area, i * width + j * PAIR:i * width + (j + 1) * PAIR].astype(f32)

        def shifted(i):
            now = raw(i)
            before = jnp.where(first, edge_row(i, j), pltpu.roll(now, 1, 0))
            return now + (before - now) * mix[i:i + 1, cols(j)]

        key_all = shifted(1)
        unit_all = key_all * lax.rsqrt(head_sum(key_all * key_all, masks) + 1.0)
        rate_all = sigmoid(rate_base[:, cols(j)] + raw(4))
        level_all = decay_base[:, cols(j)] + raw(3)
        recept_all = shifted(0)
        value_all = shifted(2)
        for i in range(GROUP):
            at = slice(i * BLOCK, (i + 1) * BLOCK)
            u = (i, j)
            key[u], unit[u], rate[u], value[u], recept[u] = key_all[at], unit_all[at], rate_all[at], value_all[at], recept_all[at]
            logs[u] = -EXP_HALF * sigmoid(level_all[at] + drift[0, base + i * BLOCK])

    run = {u: jnp.dot(tri2, jnp.concatenate(split(logs[u]), axis=0), preferred_element_type=f32) for u in units}
    alpha, scaled, by = {}, {}, {}
    beta_end, key_end = {}, {}
    for u in units:
        last = run[u][BLOCK - 1:BLOCK, :]
        inverse = jnp.exp(-run[u])
        to_end = jnp.exp(last - run[u])
        unit_rate = unit[u] * rate[u]
        alpha[u] = -unit[u] * jnp.exp(run[u] - logs[u])
        scaled[u] = recept[u] * jnp.exp(run[u])
        left = lhs3(jnp.concatenate([alpha[u], scaled[u]], axis=0))
        right = jnp.concatenate([rhs_nt(unit_rate * inverse, masks), rhs_nt(key[u] * inverse, masks)], axis=0)
        by[u] = nt(left, right)
        beta_end[u] = unit_rate * to_end
        key_end[u] = key[u] * to_end
    lower = {u: jnp.where(strict, by[u][:BLOCK, :PAIR], 0.0) for u in units}
    value3 = {u: rhs_nn(value[u], masks) for u in units}
    pulled = {u: nn(lhs3(jnp.where(strict, by[u][:BLOCK, PAIR:], 0.0)), value3[u]) for u in units}
    for u in units:
        i, j = u
        upper_b[block(i), cols(j)] = jnp.where(inclusive, by[u][BLOCK:, :PAIR], 0.0)
        upper_k[block(i), cols(j)] = jnp.where(inclusive, by[u][BLOCK:, PAIR:], 0.0)
        recept_s[block(i), cols(j)] = scaled[u]
        value_s[block(i), cols(j)] = value[u]
    solved = {u: eye + jnp.where(lax.div(place, 2) == lax.div(other, 2), lower[u], 0.0) for u in units}
    size = 2
    while size < BLOCK:
        inside = jnp.logical_and(
            lax.div(place, 2 * size) == lax.div(other, 2 * size), lax.div(place, size) != lax.div(other, size))
        turned = {u: nn(lhs3(solved[u]), rhs_nn(jnp.where(inside, lower[u], 0.0), masks)) for u in units}
        solved = {u: solved[u] + nn(lhs3(turned[u]), rhs_nn(solved[u], masks)) for u in units}
        size *= 2
    both = {u: nn(lhs3(solved[u]), jnp.concatenate([rhs_nn(alpha[u], masks), rhs_nn(pulled[u], masks)], axis=1))
            for u in units}
    for u in units:
        i, j = u
        alpha_s[block(i), cols(j)] = both[u][:, :PAIR]
        pulled_s[block(i), cols(j)] = both[u][:, PAIR:]
        cross = tn(both[u][:, :PAIR], beta_end[u])
        trans_s[block(i), cols(j)] = jnp.where(is_low, cross[:BLOCK], cross[BLOCK:]) + eye * jnp.exp(run[u][BLOCK - 1:BLOCK, :])
        cross = tn(jnp.concatenate([both[u][:, PAIR:], value[u]], axis=0),
                   jnp.concatenate([beta_end[u], key_end[u]], axis=0))
        added_s[block(i), cols(j)] = jnp.where(is_low, cross[:BLOCK], cross[BLOCK:])


def compose(trans_s, added_s, before_s, msg):
    width = trans_s.shape[1]
    pairs = width // PAIR
    chunks = trans_s.shape[0] // BLOCK
    masks = lane_masks(bf16)
    zero = jnp.zeros((BLOCK, PAIR), f32)
    both = {}
    for c in range(chunks):
        block = slice(c * BLOCK, (c + 1) * BLOCK)
        for j in range(pairs):
            cols = slice(j * PAIR, (j + 1) * PAIR)
            if c == 0:
                both[j] = jnp.concatenate([trans_s[block, cols], added_s[block, cols]], axis=0)
                continue
            before_s[c, :, cols] = both[j]
            both[j] = nn(lhs3(both[j]), rhs_nn(trans_s[block, cols], masks)) + jnp.concatenate(
                [zero, added_s[block, cols]], axis=0)
    for j in range(pairs):
        for side in range(2):
            head = 2 * j + side
            packed = pack(both[j][:BLOCK], side)
            for q in range(2):
                msg[2 * head + q, 0:32, :] = packed
                msg[2 * head + q, 32:48, :] = pack(both[j][BLOCK + 32 * q:BLOCK + 32 * (q + 1)], side)


def read_chunks(proj, store, before_s, reads_out, fixed_out, gate_out):
    recept_s, value_s, alpha_s, pulled_s, upper_b, upper_k, trans_s, added_s = store
    width = recept_s.shape[1]
    pairs = width // PAIR
    masks = lane_masks(bf16)
    for c in range(recept_s.shape[0] // BLOCK):
        block = slice(c * BLOCK, (c + 1) * BLOCK)
        for j in range(pairs):
            cols = slice(j * PAIR, (j + 1) * PAIR)
            upper = lhs3(upper_b[block, cols])
            both = nn(upper, jnp.concatenate(
                [rhs_nn(alpha_s[block, cols], masks), rhs_nn(pulled_s[block, cols], masks)], axis=1))
            reads = recept_s[block, cols] + both[:, :PAIR]
            fixed = both[:, PAIR:] + nn(lhs3(upper_k[block, cols]), rhs_nn(value_s[block, cols], masks))
            if c > 0:
                both = nt(lhs3(reads), jnp.concatenate(
                    [rhs_nt(before_s[c, :BLOCK, cols], masks), rhs_nt(before_s[c, BLOCK:, cols], masks)], axis=0))
                reads = both[:, :PAIR]
                fixed = fixed + both[:, PAIR:]
            reads_out[block, cols] = reads
            fixed_out[block, cols] = fixed
            gate_out[block, cols] = sigmoid(proj[block, 5 * width + j * PAIR:5 * width + (j + 1) * PAIR].astype(f32))


def prepare(proj, edge, mix, base, rate_base, drift, reads_out, fixed_out, gate_out, msg, before_s, *store):
    rows = proj.shape[0]
    width = proj.shape[1] // 6
    group = GROUP * BLOCK
    for g in range(rows // group):
        def edge_row(i, j):
            at = slice(i * width + j * PAIR, i * width + (j + 1) * PAIR)
            if g == 0:
                return edge[0:1, at]
            return proj[g * group - 16:g * group, at].astype(f32)[15:16]

        state_group(g * group, edge_row, proj, mix, base, rate_base, drift, store)
    compose(store[6], store[7], before_s, msg)
    read_chunks(proj, store, before_s, reads_out, fixed_out, gate_out)


def pack(x, side):
    half = x.shape[0] // 2
    is_low = lax.broadcasted_iota(jnp.int32, (half, PAIR), 1) < HEAD
    top, bottom = x[:half], x[half:]
    if side == 0:
        return jnp.where(is_low, top, pltpu.roll(bottom, HEAD, 1))
    return jnp.where(is_low, pltpu.roll(top, HEAD, 1), bottom)


def unpack(x):
    is_low = lax.broadcasted_iota(jnp.int32, x.shape, 1) < HEAD
    return jnp.concatenate([jnp.where(is_low, x, 0.0), jnp.where(is_low, pltpu.roll(x, HEAD, 1), 0.0)], axis=0)


def call_prepare(proj, edge, mix, base, rate_base, drift):
    rows = proj.shape[0]
    width = proj.shape[1] // 6
    wide = jax.ShapeDtypeStruct((rows, width), f32)
    return pl.pallas_call(
        prepare,
        out_shape=(wide, wide, wide, jax.ShapeDtypeStruct((8, 48, PAIR), f32)),
        in_specs=[VMEM_SPEC] * 5 + [SMEM_SPEC],
        out_specs=(VMEM_SPEC,) * 4,
        scratch_shapes=[pltpu.VMEM((rows // BLOCK, 2 * BLOCK, width), f32)] + [pltpu.VMEM((rows, width), f32)] * 8,
        name="prepare",
        cost_estimate=pl.CostEstimate(flops=3 * 10**9, bytes_accessed=4 * 10**6, transcendentals=10**6),
    )(proj, edge, mix, base, rate_base, drift)


def state_lhs(x):
    hi = x.astype(bf16).astype(f32)
    joined = hi + pltpu.roll(x - hi, HEAD, 1)
    return jnp.concatenate([joined.astype(bf16), hi.astype(bf16)], axis=1)


def state_rhs(x):
    hi, lo = split(x)
    return jnp.concatenate([hi, hi, lo, jnp.zeros_like(lo)], axis=0)


def carry(msg, start, out, slab, slab_sum, across, pre_map, pre_add, back,
          send1, recv1, send2, recv2, send3, recv3):
    me = here()
    nx, nc, nz = lax.axis_size("x"), lax.axis_size("c"), lax.axis_size("z")
    z = me["z"]
    unit = me["x"] * nc + me["c"]
    units = nx * nc

    def in_slab(index):
        return {"z": z, "x": index // nc, "c": lax.rem(index, nc), "tp": me["tp"]}

    def along(index):
        return {"z": index, "x": me["x"], "c": me["c"], "tp": me["tp"]}

    barrier = pltpu.get_barrier_semaphore()
    for d in range(1, units):
        pl.semaphore_signal(barrier, inc=1, device_id=in_slab(lax.rem(unit + d, units)), device_id_type=MESH)
    for d in range(1, nz):
        pl.semaphore_signal(barrier, inc=1, device_id=along(lax.rem(z + d, nz)), device_id_type=MESH)
    pl.semaphore_wait(barrier, units + nz - 2)

    first = []
    for d in range(1, units):
        peer = lax.rem(unit + d, units)
        copy = pltpu.make_async_remote_copy(
            src_ref=msg.at[peer], dst_ref=slab.at[unit], send_sem=send1.at[d], recv_sem=recv1.at[unit],
            device_id=in_slab(peer), device_id_type=MESH)
        copy.start()
        first.append(copy)
    slab[unit] = msg[unit]

    def landed(buffer, sems, k):
        return pltpu.make_async_remote_copy(
            src_ref=buffer.at[k], dst_ref=buffer.at[k], send_sem=send1.at[0], recv_sem=sems.at[k],
            device_id=in_slab(unit), device_id_type=MESH)

    running = jnp.zeros((96, PAIR), f32)
    row = lax.broadcasted_iota(jnp.int32, (96, PAIR), 0)
    col = lax.broadcasted_iota(jnp.int32, (96, PAIR), 1)
    running = (row == col).astype(f32) * (col < HEAD).astype(f32)
    for k in range(8):
        @pl.when(k != unit)
        def _():
            landed(slab, recv1, k).wait_recv()

        pre_map[k] = state_rhs(running[:HEAD])
        pre_add[k] = running[HEAD:]
        piece = slab[k]
        add = jnp.concatenate([jnp.zeros((HEAD, PAIR), f32), unpack(piece[32:48])], axis=0)
        running = nn(state_lhs(running), state_rhs(unpack(piece[0:32]))) + add
    slab_sum[0:32, :] = pack(running[:HEAD], 0)
    slab_sum[32:48, :] = pack(running[HEAD:], 0)

    def onward(d):
        return pltpu.make_async_remote_copy(
            src_ref=slab_sum, dst_ref=across.at[z], send_sem=send2.at[d], recv_sem=recv2.at[z],
            device_id=along(lax.rem(z + d, nz)), device_id_type=MESH)

    for d in range(1, 8):
        @pl.when(z + d < nz)
        def _():
            onward(d).start()

    head = start[me["x"], pl.ds(pl.multiple_of(me["c"] * 32, 32), 32), :]
    state = jnp.concatenate([head, jnp.zeros((32, PAIR - HEAD), f32)], axis=1)
    for k in range(7):
        @pl.when(k < z)
        def _():
            landed(across, recv2, k).wait_recv()

        piece = across[k]
        new = nn(state_lhs(state), state_rhs(unpack(piece[0:32]))) + unpack(piece[32:48])
        state = jnp.where(k < z, new, state)

    state3 = state_lhs(state)
    for k in range(8):
        back[k] = pack(nn(state3, pre_map[k]) + pre_add[k], 0)
    last = []
    for d in range(1, units):
        peer = lax.rem(unit + d, units)
        copy = pltpu.make_async_remote_copy(
            src_ref=back.at[peer], dst_ref=out.at[unit], send_sem=send3.at[d], recv_sem=recv3.at[unit],
            device_id=in_slab(peer), device_id_type=MESH)
        copy.start()
        last.append(copy)
    out[unit] = back[unit]
    for k in range(8):
        @pl.when(k != unit)
        def _():
            landed(out, recv3, k).wait_recv()
    for copy in first + last:
        copy.wait_send()
    for d in range(1, 8):
        @pl.when(z + d < nz)
        def _():
            onward(d).wait_send()


def call_carry(msg, start):
    return pl.pallas_call(
        carry,
        out_shape=jax.ShapeDtypeStruct((8, 16, PAIR), f32),
        in_specs=[VMEM_SPEC, VMEM_SPEC],
        out_specs=VMEM_SPEC,
        scratch_shapes=[
            pltpu.VMEM((8, 48, PAIR), f32),
            pltpu.VMEM((48, PAIR), f32),
            pltpu.VMEM((8, 48, PAIR), f32),
            pltpu.VMEM((8, 256, PAIR), bf16),
            pltpu.VMEM((8, 32, PAIR), f32),
            pltpu.VMEM((8, 16, PAIR), f32),
        ] + [pltpu.SemaphoreType.DMA((8,))] * 6,
        compiler_params=pltpu.CompilerParams(collective_id=1, has_side_effects=True),
        name="carry",
    )(msg, start)


def finish(reads, fixed, gate, state, gains, w_out, out, gated, token_rows, wbuf, w_sem, send_sem, recv_sem):
    me = here()
    y = me["tp"]
    ny = lax.axis_size("tp")
    fetch = pltpu.make_async_copy(w_out, wbuf, w_sem)
    fetch.start()
    barrier = pltpu.get_barrier_semaphore()
    for d in range(1, 4):
        pl.semaphore_signal(barrier, inc=1, device_id={"tp": lax.rem(y + d, ny)}, device_id_type=MESH)
    rows, width = reads.shape
    share = rows // 4
    masks = lane_masks(bf16)
    is_low = lax.broadcasted_iota(jnp.int32, (16, PAIR), 1) < HEAD
    for j in range(width // PAIR):
        cols = slice(j * PAIR, (j + 1) * PAIR)
        parts = []
        for q in range(2):
            a, b = state[4 * j + q], state[4 * j + 2 + q]
            parts.append(jnp.where(is_low, a, pltpu.roll(b, HEAD, 1)))
            parts.append(jnp.where(is_low, pltpu.roll(a, HEAD, 1), b))
        entering = jnp.concatenate(parts, axis=0)
        mixed = fixed[:, cols] + nt(lhs3(reads[:, cols]), rhs_nt(entering, masks))
        center = mixed - head_sum(mixed, masks) * (1.0 / HEAD)
        spread = head_sum(center * center, masks) * (1.0 / HEAD)
        scaled = center * lax.rsqrt(spread + GROUP_FLOOR) * gains[:, cols]
        gated[:, cols] = (scaled * gate[:, cols]).astype(bf16)
    pl.semaphore_wait(barrier, 3)

    def part(k):
        return pl.ds(pl.multiple_of(k * share, 16), share)

    copies = []
    for d in range(1, 4):
        peer = lax.rem(y + d, ny)
        copy = pltpu.make_async_remote_copy(
            src_ref=gated.at[part(peer)], dst_ref=token_rows.at[d], send_sem=send_sem.at[d], recv_sem=recv_sem.at[d],
            device_id={"tp": peer}, device_id_type=MESH)
        copy.start()
        copies.append(copy)
    fetch.wait()
    token_rows[0] = gated[part(y), :]
    for d in range(1, 4):
        copies[d - 1].wait_recv()
    total = jnp.zeros(out.shape, f32)
    for d in range(4):
        owner = lax.rem(y + ny - d, ny)
        total = total + jnp.dot(token_rows[d], wbuf[pl.ds(pl.multiple_of(owner * width, width), width), :],
                                preferred_element_type=f32)
    out[...] = total.astype(bf16)
    for copy in copies:
        copy.wait_send()


def call_finish(reads, fixed, gate, state, gains, w_out):
    rows, width = reads.shape
    share = rows // 4
    inner, depth = w_out.shape
    return pl.pallas_call(
        finish,
        out_shape=jax.ShapeDtypeStruct((share, depth), bf16),
        in_specs=[VMEM_SPEC] * 5 + [ANY_SPEC],
        out_specs=VMEM_SPEC,
        scratch_shapes=[
            pltpu.VMEM((rows, width), bf16),
            pltpu.VMEM((4, share, width), bf16),
            pltpu.VMEM((inner, depth), bf16),
            pltpu.SemaphoreType.DMA(()),
            pltpu.SemaphoreType.DMA((4,)),
            pltpu.SemaphoreType.DMA((4,)),
        ],
        compiler_params=pltpu.CompilerParams(collective_id=2, has_side_effects=True),
        name="finish",
    )(reads, fixed, gate, state, gains, w_out)


def per_device(tokens, norm_gain, w_recept, w_key, w_value, w_decay, w_rate, w_gate, shift_mix, decay_base, rate_base,
               decay_drift, group_gain, initial_state, w_out):
    proj, edge = call_gather(
        tokens, norm_gain.reshape(1, -1), (w_recept, w_key, w_value, w_decay, w_rate, w_gate))
    reads, fixed, gate, msg = call_prepare(
        proj, edge, shift_mix, decay_base.reshape(1, -1), rate_base.reshape(1, -1), decay_drift.reshape(1, -1))
    state = call_carry(msg, initial_state)
    return call_finish(reads, fixed, gate, state, group_gain.reshape(1, -1), w_out)


def solution(mesh):
    finer = Mesh(mesh.devices.reshape(8, 4, 2, mesh.shape["tp"]), AXES)
    in_specs = (
        P(SP_TP, None),
        P(),
        P(None, "tp"),
        P(None, "tp"),
        P(None, "tp"),
        P(None, "tp"),
        P(None, "tp"),
        P(None, "tp"),
        P(None, "tp"),
        P("tp"),
        P("tp"),
        P(SP),
        P("tp"),
        P("tp", None, None),
        P(),
    )
    return jax.shard_map(
        per_device, mesh=finer, in_specs=in_specs, out_specs=P(SP_TP, None), check_vma=False
    )
```

```python
import functools

import jax
import jax.numpy as jnp
from jax import lax
from jax.experimental import pallas as pl
from jax.experimental.pallas import tpu as pltpu
from jax.sharding import Mesh
from jax.sharding import PartitionSpec as P

HEAD = 64
BLOCK = 64
PAIR = 128
GROUP = 3
SP = ("z", "x", "c")
SP_TP = ("z", "x", "c", "tp")
AXES = ("z", "x", "c", "tp")
MESH = pl.DeviceIdType.MESH
NORM_FLOOR = 0.5
GROUP_FLOOR = 1.0
EXP_HALF = 0.6065306597126334
f32 = jnp.float32
bf16 = jnp.bfloat16
VMEM_SPEC = pl.BlockSpec(memory_space=pltpu.VMEM)
ANY_SPEC = pl.BlockSpec(memory_space=pl.ANY)
SMEM_SPEC = pl.BlockSpec(memory_space=pltpu.SMEM)


def here():
    return {axis: lax.axis_index(axis) for axis in AXES}


def split(x):
    hi = x.astype(bf16)
    lo = (x - hi.astype(f32)).astype(bf16)
    return hi, lo


def sigmoid(x):
    return 1.0 / (1.0 + jnp.exp(-x))


def lane_masks(dtype):
    lane = lax.broadcasted_iota(jnp.int32, (1, PAIR), 1)
    low = (lane < HEAD).astype(f32)
    return low.astype(dtype), (1.0 - low).astype(dtype)


def lhs3(x):
    hi, lo = split(x)
    return jnp.concatenate([hi, lo, hi], axis=1)


def diag_parts(x, masks):
    hi, lo = split(x)
    low, high = masks
    bd_hi = jnp.concatenate([hi * low, hi * high], axis=0)
    bd_lo = jnp.concatenate([lo * low, lo * high], axis=0)
    return bd_hi, bd_lo


def rhs_nn(x, masks):
    hi, lo = diag_parts(x, masks)
    return jnp.concatenate([hi, hi, lo], axis=0)


def rhs_nt(x, masks):
    hi, lo = diag_parts(x, masks)
    return jnp.concatenate([hi, hi, lo], axis=1)


def nn(a3, b3):
    return jnp.dot(a3, b3, preferred_element_type=f32)


def nt(a3, b3):
    return lax.dot_general(a3, b3, (((1,), (1,)), ((), ())), preferred_element_type=f32)


def tn(a, b):
    a_hi, a_lo = split(a)
    b_hi, b_lo = split(b)
    return lax.dot_general(
        jnp.concatenate([a_hi, a_lo, a_hi], axis=0), jnp.concatenate([b_hi, b_hi, b_lo], axis=0),
        (((0,), (0,)), ((), ())), preferred_element_type=f32)


def head_sum(x, masks):
    low, high = masks
    ones = jnp.concatenate([jnp.broadcast_to(low, (HEAD, PAIR)), jnp.broadcast_to(high, (HEAD, PAIR))], axis=0)
    hi, lo = split(x)
    return jnp.dot(jnp.concatenate([hi, lo], axis=1), jnp.concatenate([ones, ones], axis=0), preferred_element_type=f32)


def state_group(base, edge_row, proj, mix, decay_base, rate_base, drift, store):
    recept_s, value_s, alpha_s, pulled_s, upper_b, upper_k, trans_s, added_s = store
    width = recept_s.shape[1]
    pairs = width // PAIR
    rows = GROUP * BLOCK
    masks = lane_masks(bf16)
    is_low = lax.broadcasted_iota(jnp.int32, (1, PAIR), 1) < HEAD
    place = lax.broadcasted_iota(jnp.int32, (BLOCK, PAIR), 0)
    other = lax.rem(lax.broadcasted_iota(jnp.int32, (BLOCK, PAIR), 1), BLOCK)
    strict = other < place
    inclusive = other <= place
    eye = (other == place).astype(f32)
    tri2 = inclusive.astype(f32).astype(bf16)
    area = pl.ds(pl.multiple_of(base, BLOCK), rows)
    units = [(i, j) for i in range(GROUP) for j in range(pairs)]

    def block(i):
        return pl.ds(pl.multiple_of(base + i * BLOCK, BLOCK), BLOCK)

    def cols(j):
        return slice(j * PAIR, (j + 1) * PAIR)

    logs, unit, rate, key, value, recept = {}, {}, {}, {}, {}, {}
    first = lax.broadcasted_iota(jnp.int32, (rows, PAIR), 0) == 0
    for j in range(pairs):
        def raw(i):
            return proj[area, i * width + j * PAIR:i * width + (j + 1) * PAIR].astype(f32)

        def shifted(i):
            now = raw(i)
            before = jnp.where(first, edge_row(i, j), pltpu.roll(now, 1, 0))
            return now + (before - now) * mix[i:i + 1, cols(j)]

        key_all = shifted(1)
        unit_all = key_all * lax.rsqrt(head_sum(key_all * key_all, masks) + 1.0)
        rate_all = sigmoid(rate_base[:, cols(j)] + raw(4))
        level_all = decay_base[:, cols(j)] + raw(3)
        recept_all = shifted(0)
        value_all = shifted(2)
        for i in range(GROUP):
            at = slice(i * BLOCK, (i + 1) * BLOCK)
            u = (i, j)
            key[u], unit[u], rate[u], value[u], recept[u] = key_all[at], unit_all[at], rate_all[at], value_all[at], recept_all[at]
            logs[u] = -EXP_HALF * sigmoid(level_all[at] + drift[base + i * BLOCK])

    run = {u: jnp.dot(tri2, jnp.concatenate(split(logs[u]), axis=0), preferred_element_type=f32) for u in units}
    alpha, scaled, by = {}, {}, {}
    beta_end, key_end = {}, {}
    for u in units:
        last = run[u][BLOCK - 1:BLOCK, :]
        inverse = jnp.exp(-run[u])
        to_end = jnp.exp(last - run[u])
        unit_rate = unit[u] * rate[u]
        alpha[u] = -unit[u] * jnp.exp(run[u] - logs[u])
        scaled[u] = recept[u] * jnp.exp(run[u])
        left = lhs3(jnp.concatenate([alpha[u], scaled[u]], axis=0))
        right = jnp.concatenate([rhs_nt(unit_rate * inverse, masks), rhs_nt(key[u] * inverse, masks)], axis=0)
        by[u] = nt(left, right)
        beta_end[u] = unit_rate * to_end
        key_end[u] = key[u] * to_end
    lower = {u: jnp.where(strict, by[u][:BLOCK, :PAIR], 0.0) for u in units}
    value3 = {u: rhs_nn(value[u], masks) for u in units}
    pulled = {u: nn(lhs3(jnp.where(strict, by[u][:BLOCK, PAIR:], 0.0)), value3[u]) for u in units}
    for u in units:
        i, j = u
        upper_b[block(i), cols(j)] = jnp.where(inclusive, by[u][BLOCK:, :PAIR], 0.0)
        upper_k[block(i), cols(j)] = jnp.where(inclusive, by[u][BLOCK:, PAIR:], 0.0)
        recept_s[block(i), cols(j)] = scaled[u]
        value_s[block(i), cols(j)] = value[u]
    solved = {u: eye + jnp.where(lax.div(place, 2) == lax.div(other, 2), lower[u], 0.0) for u in units}
    size = 2
    while size < BLOCK:
        inside = jnp.logical_and(
            lax.div(place, 2 * size) == lax.div(other, 2 * size), lax.div(place, size) != lax.div(other, size))
        turned = {u: nn(lhs3(solved[u]), rhs_nn(jnp.where(inside, lower[u], 0.0), masks)) for u in units}
        solved = {u: solved[u] + nn(lhs3(turned[u]), rhs_nn(solved[u], masks)) for u in units}
        size *= 2
    both = {u: nn(lhs3(solved[u]), jnp.concatenate([rhs_nn(alpha[u], masks), rhs_nn(pulled[u], masks)], axis=1))
            for u in units}
    for u in units:
        i, j = u
        alpha_s[block(i), cols(j)] = both[u][:, :PAIR]
        pulled_s[block(i), cols(j)] = both[u][:, PAIR:]
        cross = tn(both[u][:, :PAIR], beta_end[u])
        trans_s[block(i), cols(j)] = jnp.where(is_low, cross[:BLOCK], cross[BLOCK:]) + eye * jnp.exp(run[u][BLOCK - 1:BLOCK, :])
        cross = tn(jnp.concatenate([both[u][:, PAIR:], value[u]], axis=0),
                   jnp.concatenate([beta_end[u], key_end[u]], axis=0))
        added_s[block(i), cols(j)] = jnp.where(is_low, cross[:BLOCK], cross[BLOCK:])


def compose(trans_s, added_s, before_s, msg):
    width = trans_s.shape[1]
    pairs = width // PAIR
    chunks = trans_s.shape[0] // BLOCK
    masks = lane_masks(bf16)
    zero = jnp.zeros((BLOCK, PAIR), f32)
    both = {}
    for c in range(chunks):
        block = slice(c * BLOCK, (c + 1) * BLOCK)
        for j in range(pairs):
            cols = slice(j * PAIR, (j + 1) * PAIR)
            if c == 0:
                both[j] = jnp.concatenate([trans_s[block, cols], added_s[block, cols]], axis=0)
                continue
            before_s[c, :, cols] = both[j]
            both[j] = nn(lhs3(both[j]), rhs_nn(trans_s[block, cols], masks)) + jnp.concatenate(
                [zero, added_s[block, cols]], axis=0)
    for j in range(pairs):
        for side in range(2):
            head = 2 * j + side
            packed = pack(both[j][:BLOCK], side)
            for q in range(2):
                msg[2 * head + q, 0:32, :] = packed
                msg[2 * head + q, 32:48, :] = pack(both[j][BLOCK + 32 * q:BLOCK + 32 * (q + 1)], side)


def read_chunks(chunks, proj, store, before_s, reads_out, fixed_out, gate_out):
    recept_s, value_s, alpha_s, pulled_s, upper_b, upper_k, trans_s, added_s = store
    width = recept_s.shape[1]
    pairs = width // PAIR
    masks = lane_masks(bf16)
    for c in chunks:
        block = slice(c * BLOCK, (c + 1) * BLOCK)
        for j in range(pairs):
            cols = slice(j * PAIR, (j + 1) * PAIR)
            upper = lhs3(upper_b[block, cols])
            both = nn(upper, jnp.concatenate(
                [rhs_nn(alpha_s[block, cols], masks), rhs_nn(pulled_s[block, cols], masks)], axis=1))
            reads = recept_s[block, cols] + both[:, :PAIR]
            fixed = both[:, PAIR:] + nn(lhs3(upper_k[block, cols]), rhs_nn(value_s[block, cols], masks))
            if c > 0:
                both = nt(lhs3(reads), jnp.concatenate(
                    [rhs_nt(before_s[c, :BLOCK, cols], masks), rhs_nt(before_s[c, BLOCK:, cols], masks)], axis=0))
                reads = both[:, :PAIR]
                fixed = fixed + both[:, PAIR:]
            reads_out[block, cols] = reads
            fixed_out[block, cols] = fixed
            gate_out[block, cols] = sigmoid(proj[block, 5 * width + j * PAIR:5 * width + (j + 1) * PAIR].astype(f32))


def pack(x, side):
    half = x.shape[0] // 2
    is_low = lax.broadcasted_iota(jnp.int32, (half, PAIR), 1) < HEAD
    top, bottom = x[:half], x[half:]
    if side == 0:
        return jnp.where(is_low, top, pltpu.roll(bottom, HEAD, 1))
    return jnp.where(is_low, pltpu.roll(top, HEAD, 1), bottom)


def unpack(x):
    is_low = lax.broadcasted_iota(jnp.int32, x.shape, 1) < HEAD
    return jnp.concatenate([jnp.where(is_low, x, 0.0), jnp.where(is_low, pltpu.roll(x, HEAD, 1), 0.0)], axis=0)


def state_lhs(x):
    hi = x.astype(bf16).astype(f32)
    joined = hi + pltpu.roll(x - hi, HEAD, 1)
    return jnp.concatenate([joined.astype(bf16), hi.astype(bf16)], axis=1)


def state_rhs(x):
    hi, lo = split(x)
    return jnp.concatenate([hi, hi, lo, jnp.zeros_like(lo)], axis=0)


def layer(tokens, gain, wr, wk, wv, wd, wa, wg, mix, decay_base, rate_base, drift, group_gain, start, w_out, out,
          own, held, last, last_in, wbuf, norm_buf, proj, edge_s, before_s, msg, reads_s, fixed_s, gate_s,
          slab, slab_sum, across, pre_map, pre_add, back, entering, gated, token_rows, w_out_buf,
          own_sem, w_sem, out_sem, hop_send, hop_recv, edge_send, edge_recv,
          send1, recv1, send2, recv2, send3, recv3, send4, recv4, *store):
    me = here()
    y, z = me["tp"], me["z"]
    ny, nx, nc, nz = lax.axis_size("tp"), lax.axis_size("x"), lax.axis_size("c"), lax.axis_size("z")
    right, left = lax.rem(y + 1, ny), lax.rem(y + ny - 1, ny)
    far = lax.rem(y + 2, ny)
    unit = me["x"] * nc + me["c"]
    units = nx * nc
    seq = z * units + unit
    total = units * nz
    rows = own.shape[0]
    half = rows // 2
    width = wbuf.shape[2]

    def at(index, tp):
        return {"z": index // units, "x": lax.rem(index // nc, nx), "c": lax.rem(index, nc), "tp": tp}

    def in_slab(index):
        return {"z": z, "x": index // nc, "c": lax.rem(index, nc), "tp": y}

    def along(index):
        return {"z": index, "x": me["x"], "c": me["c"], "tp": y}

    def remote(src, dst, send, recv, to):
        return pltpu.make_async_remote_copy(
            src_ref=src, dst_ref=dst, send_sem=send, recv_sem=recv, device_id=to, device_id_type=MESH)

    def greet(to):
        pl.semaphore_signal(barrier, inc=1, device_id=to, device_id_type=MESH)

    fetch = pltpu.make_async_copy(tokens, own, own_sem)
    fetch.start()
    w_copies = [pltpu.make_async_copy(w, wbuf.at[i], w_sem.at[i]) for i, w in enumerate((wr, wk, wv, wd, wa, wg))]
    for copy in w_copies:
        copy.start()
    barrier = pltpu.get_barrier_semaphore()
    for d in range(1, 4):
        greet({"tp": lax.rem(y + d, ny)})
    for d in range(1, 8):
        greet(in_slab(lax.rem(unit + d, units)))
        greet(along(lax.rem(z + d, nz)))
    ends_stretch = jnp.logical_and(y == ny - 1, seq < total - 1)
    has_before = seq > 0

    @pl.when(has_before)
    def _():
        greet(at(seq - 1, ny - 1))

    pl.semaphore_wait(barrier, 17 + 4 * ends_stretch.astype(jnp.int32))
    fetch.wait()

    def part(h):
        return pl.ds(h * half, half)

    def hop(src, slot, h, to, sem):
        return remote(src, held.at[slot, part(h)], hop_send.at[sem], hop_recv.at[slot, h], {"tp": to})

    to_right = [hop(own.at[part(h)], 0, h, right, h) for h in (0, 1)]
    to_left = [hop(own.at[part(h)], 2, h, left, 2 + h) for h in (0, 1)]
    on_right = hop(held.at[0, part(0)], 1, 0, right, 4)
    on_left = hop(held.at[2, part(1)], 1, 1, left, 5)
    to_right[0].start()
    to_left[1].start()
    to_right[1].start()
    to_left[0].start()

    last[...] = own[rows - 16:rows, :].astype(f32)[15:16, :]
    edges = [remote(last, last_in.at[0], edge_send.at[k], edge_recv.at[0], at(lax.rem(seq + 1, total), k))
             for k in range(4)]
    inner = [remote(last, last_in.at[1], edge_send.at[4 + k], edge_recv.at[1], {"tp": 2 + k}) for k in range(2)]

    @pl.when(ends_stretch)
    def _():
        for copy in edges:
            copy.start()

    @pl.when(y == 1)
    def _():
        for copy in inner:
            copy.start()

    out_copy = pltpu.make_async_copy(w_out, w_out_buf, out_sem)
    out_copy.start()

    def normalize(x):
        return (x * lax.rsqrt(jnp.mean(x * x, axis=-1, keepdims=True) + NORM_FLOOR) * gain[...]).astype(bf16)

    def project(block, owner, with_edge):
        base = pl.multiple_of(owner * rows, 16)
        norm_buf[0:rows, :] = normalize(block[...].astype(f32))
        count = rows + 16 if with_edge else rows
        for i in range(6):
            res = jnp.dot(norm_buf[0:count, :], wbuf[i], preferred_element_type=f32)
            proj[pl.ds(base, rows), width * i:width * (i + 1)] = res[0:rows].astype(bf16)
            if with_edge and i < 3:
                edge_s[:, width * i:width * (i + 1)] = res[rows:].astype(bf16).astype(f32)

    for copy in w_copies:
        copy.wait()
    project(own, y, False)
    to_right[0].wait_recv()
    on_right.start()
    to_left[1].wait_recv()
    on_left.start()

    @pl.when(has_before)
    def _():
        edges[0].wait_recv()

    @pl.when(jnp.logical_not(has_before))
    def _():
        last_in[0] = jnp.zeros_like(last)

    @pl.when(y >= 2)
    def _():
        inner[0].wait_recv()

    @pl.when(y < 2)
    def _():
        last_in[1] = jnp.zeros_like(last)

    norm_buf[rows:, :] = jnp.concatenate(
        [jnp.broadcast_to(normalize(last_in[k]), (8, own.shape[1])) for k in range(2)], axis=0)
    to_right[1].wait_recv()
    project(held.at[0], left, True)
    to_left[0].wait_recv()
    project(held.at[2], right, False)

    group = GROUP * BLOCK
    early = y < 2

    def columns(i, j):
        return slice(i * width + j * PAIR, i * width + (j + 1) * PAIR)

    def first_edge(i, j):
        return jnp.where(early, edge_s[0:1, columns(i, j)], edge_s[8:9, columns(i, j)])

    def second_edge(i, j):
        return jnp.where(early, proj[group - 16:group, columns(i, j)].astype(f32)[15:16], edge_s[0:1, columns(i, j)])

    own_base = jnp.where(early, 0, group)
    state_group(own_base, first_edge, proj, mix, decay_base, rate_base, drift, store)
    on_right.wait_recv()
    on_left.wait_recv()
    project(held.at[1], far, False)
    state_group(group - own_base, second_edge, proj, mix, decay_base, rate_base, drift, store)
    compose(store[6], store[7], before_s, msg)

    def landed(buffer, sems, k):
        return remote(buffer.at[k], buffer.at[k], send1.at[0], sems.at[k], in_slab(unit))

    first = []
    for d in range(1, 8):
        peer = lax.rem(unit + d, units)
        first.append(remote(msg.at[peer], slab.at[unit], send1.at[d], recv1.at[unit], in_slab(peer)))
        first[-1].start()
    slab[unit] = msg[unit]
    read_chunks((0, 1), proj, store, before_s, reads_s, fixed_s, gate_s)

    row = lax.broadcasted_iota(jnp.int32, (96, PAIR), 0)
    col = lax.broadcasted_iota(jnp.int32, (96, PAIR), 1)
    running = (row == col).astype(f32) * (col < HEAD).astype(f32)
    for k in range(8):
        @pl.when(k != unit)
        def _():
            landed(slab, recv1, k).wait_recv()

    for k in range(8):
        pre_map[k] = state_rhs(running[:HEAD])
        pre_add[k] = running[HEAD:]
        piece = slab[k]
        add = jnp.concatenate([jnp.zeros((HEAD, PAIR), f32), unpack(piece[32:48])], axis=0)
        running = nn(state_lhs(running), state_rhs(unpack(piece[0:32]))) + add
    slab_sum[0:32, :] = pack(running[:HEAD], 0)
    slab_sum[32:48, :] = pack(running[HEAD:], 0)

    def onward(d):
        return remote(slab_sum, across.at[z], send2.at[d], recv2.at[z], along(lax.rem(z + d, nz)))

    for d in (4, 3, 2, 1, 5, 6, 7):
        @pl.when(z + d < nz)
        def _():
            onward(d).start()

    read_chunks((2, 3, 4, 5), proj, store, before_s, reads_s, fixed_s, gate_s)
    begin = start[me["x"], pl.ds(pl.multiple_of(me["c"] * 32, 32), 32), :]
    state = jnp.concatenate([begin, jnp.zeros((32, PAIR - HEAD), f32)], axis=1)
    for k in range(7):
        @pl.when(k < z)
        def _():
            landed(across, recv2, k).wait_recv()

    for k in range(7):
        piece = across[k]
        new = nn(state_lhs(state), state_rhs(unpack(piece[0:32]))) + unpack(piece[32:48])
        state = jnp.where(k < z, new, state)
    state3 = state_lhs(state)
    for k in range(8):
        back[k] = pack(nn(state3, pre_map[k]) + pre_add[k], 0)
    third = []
    for d in range(1, 8):
        peer = lax.rem(unit + d, units)
        third.append(remote(back.at[peer], entering.at[unit], send3.at[d], recv3.at[unit], in_slab(peer)))
        third[-1].start()
    entering[unit] = back[unit]
    for k in range(8):
        @pl.when(k != unit)
        def _():
            landed(entering, recv3, k).wait_recv()

    masks = lane_masks(bf16)
    is_low = lax.broadcasted_iota(jnp.int32, (16, PAIR), 1) < HEAD
    turned = []
    for j in range(width // PAIR):
        parts = []
        for q in range(2):
            a, b = entering[4 * j + q], entering[4 * j + 2 + q]
            parts.append(jnp.where(is_low, a, pltpu.roll(b, HEAD, 1)))
            parts.append(jnp.where(is_low, pltpu.roll(a, HEAD, 1), b))
        turned.append(rhs_nt(jnp.concatenate(parts, axis=0), masks))

    def share(k):
        return pl.ds(pl.multiple_of(k * rows, 16), rows)

    def gate_rows(at_rows):
        for j in range(width // PAIR):
            cols = slice(j * PAIR, (j + 1) * PAIR)
            mixed = fixed_s[at_rows, cols] + nt(lhs3(reads_s[at_rows, cols]), turned[j])
            center = mixed - head_sum(mixed, masks) * (1.0 / HEAD)
            spread = head_sum(center * center, masks) * (1.0 / HEAD)
            scaled = center * lax.rsqrt(spread + GROUP_FLOOR) * group_gain[:, cols]
            gated[at_rows, cols] = (scaled * gate_s[at_rows, cols]).astype(bf16)

    fourth = {}
    for d in (2, 1, 3):
        peer = lax.rem(y + d, ny)
        gate_rows(share(peer))
        fourth[d] = remote(gated.at[share(peer)], token_rows.at[d], send4.at[d], recv4.at[d], {"tp": peer})
    for d in (2, 1, 3):
        fourth[d].start()
    gate_rows(share(y))
    out_copy.wait()

    def product(block, owner):
        return jnp.dot(block, w_out_buf[pl.ds(pl.multiple_of(owner * width, width), width), :],
                       preferred_element_type=f32)

    result = product(gated[share(y), :], y)
    for d in (1, 3, 2):
        fourth[d].wait_recv()
        result = result + product(token_rows[d], lax.rem(y + ny - d, ny))
    out[...] = result.astype(bf16)

    for copy in (*to_right, *to_left, on_right, on_left, *first, *third, *fourth.values()):
        copy.wait_send()
    for d in range(1, 8):
        @pl.when(z + d < nz)
        def _():
            onward(d).wait_send()

    @pl.when(ends_stretch)
    def _():
        for copy in edges:
            copy.wait_send()

    @pl.when(y == 1)
    def _():
        for copy in inner:
            copy.wait_send()


def call_layer(tokens, gain, weights, mix, decay_base, rate_base, drift, group_gain, start, w_out):
    rows, depth = tokens.shape
    width = weights[0].shape[1]
    inner = w_out.shape[0]
    length = 4 * rows
    dma = pltpu.SemaphoreType.DMA
    return pl.pallas_call(
        layer,
        out_shape=jax.ShapeDtypeStruct((rows, depth), bf16),
        in_specs=[ANY_SPEC, VMEM_SPEC] + [ANY_SPEC] * 6 + [VMEM_SPEC] * 3 + [SMEM_SPEC] + [VMEM_SPEC] * 2 + [ANY_SPEC],
        out_specs=VMEM_SPEC,
        scratch_shapes=[
            pltpu.VMEM((rows, depth), bf16),
            pltpu.VMEM((3, rows, depth), bf16),
            pltpu.VMEM((1, depth), f32),
            pltpu.VMEM((2, 1, depth), f32),
            pltpu.VMEM((6, depth, width), bf16),
            pltpu.VMEM((rows + 16, depth), bf16),
            pltpu.VMEM((length, 6 * width), bf16),
            pltpu.VMEM((16, 3 * width), f32),
            pltpu.VMEM((length // BLOCK, 2 * BLOCK, width), f32),
            pltpu.VMEM((8, 48, PAIR), f32),
            pltpu.VMEM((length, width), f32),
            pltpu.VMEM((length, width), f32),
            pltpu.VMEM((length, width), f32),
            pltpu.VMEM((8, 48, PAIR), f32),
            pltpu.VMEM((48, PAIR), f32),
            pltpu.VMEM((8, 48, PAIR), f32),
            pltpu.VMEM((8, 256, PAIR), bf16),
            pltpu.VMEM((8, 32, PAIR), f32),
            pltpu.VMEM((8, 16, PAIR), f32),
            pltpu.VMEM((8, 16, PAIR), f32),
            pltpu.VMEM((length, width), bf16),
            pltpu.VMEM((4, rows, width), bf16),
            pltpu.VMEM((inner, depth), bf16),
            dma(()), dma((6,)), dma(()), dma((6,)), dma((3, 2)), dma((6,)), dma((2,)),
            dma((8,)), dma((8,)), dma((8,)), dma((8,)), dma((8,)), dma((8,)), dma((4,)), dma((4,)),
        ] + [pltpu.VMEM((length, width), f32)] * 8,
        compiler_params=pltpu.CompilerParams(collective_id=0, has_side_effects=True),
        name="layer",
    )(tokens, gain, *weights, mix, decay_base, rate_base, drift, group_gain, start, w_out)


def per_device(tokens, norm_gain, w_recept, w_key, w_value, w_decay, w_rate, w_gate, shift_mix, decay_base, rate_base,
               decay_drift, group_gain, initial_state, w_out):
    return call_layer(
        tokens, norm_gain.reshape(1, -1), (w_recept, w_key, w_value, w_decay, w_rate, w_gate), shift_mix,
        decay_base.reshape(1, -1), rate_base.reshape(1, -1), decay_drift, group_gain.reshape(1, -1), initial_state, w_out)


def solution(mesh):
    finer = Mesh(mesh.devices.reshape(8, 4, 2, mesh.shape["tp"]), AXES)
    in_specs = (
        P(SP_TP, None),
        P(),
        P(None, "tp"),
        P(None, "tp"),
        P(None, "tp"),
        P(None, "tp"),
        P(None, "tp"),
        P(None, "tp"),
        P(None, "tp"),
        P("tp"),
        P("tp"),
        P(SP),
        P("tp"),
        P("tp", None, None),
        P(),
    )
    return jax.shard_map(
        per_device, mesh=finer, in_specs=in_specs, out_specs=P(SP_TP, None), check_vma=False
    )
```

```python
import functools

import jax
import jax.numpy as jnp
from jax import lax
from jax.experimental import pallas as pl
from jax.experimental.pallas import tpu as pltpu
from jax.sharding import Mesh
from jax.sharding import PartitionSpec as P

HEAD = 64
BLOCK = 64
PAIR = 128
GROUP = 3
SP = ("z", "x", "c")
SP_TP = ("z", "x", "c", "tp")
AXES = ("z", "x", "c", "tp")
MESH = pl.DeviceIdType.MESH
NORM_FLOOR = 0.5
GROUP_FLOOR = 1.0
EXP_HALF = 0.6065306597126334
f32 = jnp.float32
bf16 = jnp.bfloat16
VMEM_SPEC = pl.BlockSpec(memory_space=pltpu.VMEM)
ANY_SPEC = pl.BlockSpec(memory_space=pl.ANY)
SMEM_SPEC = pl.BlockSpec(memory_space=pltpu.SMEM)


def here():
    return {axis: lax.axis_index(axis) for axis in AXES}


def split(x):
    hi = x.astype(bf16)
    lo = (x - hi.astype(f32)).astype(bf16)
    return hi, lo


def sigmoid(x):
    return 1.0 / (1.0 + jnp.exp(-x))


def lane_masks(dtype):
    lane = lax.broadcasted_iota(jnp.int32, (1, PAIR), 1)
    low = (lane < HEAD).astype(f32)
    return low.astype(dtype), (1.0 - low).astype(dtype)


def lhs3(x):
    hi, lo = split(x)
    return jnp.concatenate([hi, lo, hi], axis=1)


def diag_parts(x, masks):
    hi, lo = split(x)
    low, high = masks
    bd_hi = jnp.concatenate([hi * low, hi * high], axis=0)
    bd_lo = jnp.concatenate([lo * low, lo * high], axis=0)
    return bd_hi, bd_lo


def rhs_nn(x, masks):
    hi, lo = diag_parts(x, masks)
    return jnp.concatenate([hi, hi, lo], axis=0)


def rhs_nt(x, masks):
    hi, lo = diag_parts(x, masks)
    return jnp.concatenate([hi, hi, lo], axis=1)


def nn(a3, b3):
    return jnp.dot(a3, b3, preferred_element_type=f32)


def nt(a3, b3):
    return lax.dot_general(a3, b3, (((1,), (1,)), ((), ())), preferred_element_type=f32)


def tn(a, b):
    a_hi, a_lo = split(a)
    b_hi, b_lo = split(b)
    return lax.dot_general(
        jnp.concatenate([a_hi, a_lo, a_hi], axis=0), jnp.concatenate([b_hi, b_hi, b_lo], axis=0),
        (((0,), (0,)), ((), ())), preferred_element_type=f32)


def head_sum(x, masks):
    low, high = masks
    ones = jnp.concatenate([jnp.broadcast_to(low, (HEAD, PAIR)), jnp.broadcast_to(high, (HEAD, PAIR))], axis=0)
    hi, lo = split(x)
    return jnp.dot(jnp.concatenate([hi, lo], axis=1), jnp.concatenate([ones, ones], axis=0), preferred_element_type=f32)


def state_group(base, edge_row, proj, mix, decay_base, rate_base, drift, store):
    recept_s, value_s, alpha_s, pulled_s, upper_b, upper_k, trans_s, added_s = store
    width = recept_s.shape[1]
    pairs = width // PAIR
    rows = GROUP * BLOCK
    masks = lane_masks(bf16)
    is_low = lax.broadcasted_iota(jnp.int32, (1, PAIR), 1) < HEAD
    place = lax.broadcasted_iota(jnp.int32, (BLOCK, PAIR), 0)
    other = lax.rem(lax.broadcasted_iota(jnp.int32, (BLOCK, PAIR), 1), BLOCK)
    strict = other < place
    inclusive = other <= place
    eye = (other == place).astype(f32)
    tri2 = inclusive.astype(f32).astype(bf16)
    area = pl.ds(pl.multiple_of(base, BLOCK), rows)
    units = [(i, j) for i in range(GROUP) for j in range(pairs)]

    def block(i):
        return pl.ds(pl.multiple_of(base + i * BLOCK, BLOCK), BLOCK)

    def cols(j):
        return slice(j * PAIR, (j + 1) * PAIR)

    logs, unit, rate, key, value, recept = {}, {}, {}, {}, {}, {}
    first = lax.broadcasted_iota(jnp.int32, (rows, PAIR), 0) == 0
    for j in range(pairs):
        def raw(i):
            return proj[area, i * width + j * PAIR:i * width + (j + 1) * PAIR].astype(f32)

        def shifted(i):
            now = raw(i)
            before = jnp.where(first, edge_row(i, j), pltpu.roll(now, 1, 0))
            return now + (before - now) * mix[i:i + 1, cols(j)]

        key_all = shifted(1)
        unit_all = key_all * lax.rsqrt(head_sum(key_all * key_all, masks) + 1.0)
        rate_all = sigmoid(rate_base[:, cols(j)] + raw(4))
        level_all = decay_base[:, cols(j)] + raw(3)
        recept_all = shifted(0)
        value_all = shifted(2)
        for i in range(GROUP):
            at = slice(i * BLOCK, (i + 1) * BLOCK)
            u = (i, j)
            key[u], unit[u], rate[u], value[u], recept[u] = key_all[at], unit_all[at], rate_all[at], value_all[at], recept_all[at]
            logs[u] = -EXP_HALF * sigmoid(level_all[at] + drift[base + i * BLOCK])

    run = {u: jnp.dot(tri2, jnp.concatenate(split(logs[u]), axis=0), preferred_element_type=f32) for u in units}
    alpha, scaled, by = {}, {}, {}
    beta_end, key_end = {}, {}
    for u in units:
        last = run[u][BLOCK - 1:BLOCK, :]
        inverse = jnp.exp(-run[u])
        to_end = jnp.exp(last - run[u])
        unit_rate = unit[u] * rate[u]
        alpha[u] = -unit[u] * jnp.exp(run[u] - logs[u])
        scaled[u] = recept[u] * jnp.exp(run[u])
        left = lhs3(jnp.concatenate([alpha[u], scaled[u]], axis=0))
        right = jnp.concatenate([rhs_nt(unit_rate * inverse, masks), rhs_nt(key[u] * inverse, masks)], axis=0)
        by[u] = nt(left, right)
        beta_end[u] = unit_rate * to_end
        key_end[u] = key[u] * to_end
    lower = {u: jnp.where(strict, by[u][:BLOCK, :PAIR], 0.0) for u in units}
    value3 = {u: rhs_nn(value[u], masks) for u in units}
    pulled = {u: nn(lhs3(jnp.where(strict, by[u][:BLOCK, PAIR:], 0.0)), value3[u]) for u in units}
    for u in units:
        i, j = u
        upper_b[block(i), cols(j)] = jnp.where(inclusive, by[u][BLOCK:, :PAIR], 0.0)
        upper_k[block(i), cols(j)] = jnp.where(inclusive, by[u][BLOCK:, PAIR:], 0.0)
        recept_s[block(i), cols(j)] = scaled[u]
        value_s[block(i), cols(j)] = value[u]
    solved = {u: eye + jnp.where(lax.div(place, 2) == lax.div(other, 2), lower[u], 0.0) for u in units}
    size = 2
    while size < BLOCK:
        inside = jnp.logical_and(
            lax.div(place, 2 * size) == lax.div(other, 2 * size), lax.div(place, size) != lax.div(other, size))
        turned = {u: nn(lhs3(solved[u]), rhs_nn(jnp.where(inside, lower[u], 0.0), masks)) for u in units}
        solved = {u: solved[u] + nn(lhs3(turned[u]), rhs_nn(solved[u], masks)) for u in units}
        size *= 2
    both = {u: nn(lhs3(solved[u]), jnp.concatenate([rhs_nn(alpha[u], masks), rhs_nn(pulled[u], masks)], axis=1))
            for u in units}
    for u in units:
        i, j = u
        alpha_s[block(i), cols(j)] = both[u][:, :PAIR]
        pulled_s[block(i), cols(j)] = both[u][:, PAIR:]
        cross = tn(both[u][:, :PAIR], beta_end[u])
        trans_s[block(i), cols(j)] = jnp.where(is_low, cross[:BLOCK], cross[BLOCK:]) + eye * jnp.exp(run[u][BLOCK - 1:BLOCK, :])
        cross = tn(jnp.concatenate([both[u][:, PAIR:], value[u]], axis=0),
                   jnp.concatenate([beta_end[u], key_end[u]], axis=0))
        added_s[block(i), cols(j)] = jnp.where(is_low, cross[:BLOCK], cross[BLOCK:])


def compose(trans_s, added_s, before_s, msg):
    width = trans_s.shape[1]
    pairs = width // PAIR
    chunks = trans_s.shape[0] // BLOCK
    masks = lane_masks(bf16)
    zero = jnp.zeros((BLOCK, PAIR), f32)
    both = {}
    for c in range(chunks):
        block = slice(c * BLOCK, (c + 1) * BLOCK)
        for j in range(pairs):
            cols = slice(j * PAIR, (j + 1) * PAIR)
            if c == 0:
                both[j] = jnp.concatenate([trans_s[block, cols], added_s[block, cols]], axis=0)
                continue
            before_s[c, :, cols] = both[j]
            both[j] = nn(lhs3(both[j]), rhs_nn(trans_s[block, cols], masks)) + jnp.concatenate(
                [zero, added_s[block, cols]], axis=0)
    for j in range(pairs):
        for side in range(2):
            head = 2 * j + side
            packed = pack(both[j][:BLOCK] - unit_eye(), side).astype(bf16)
            for q in range(2):
                msg[2 * head + q, 0:32, :] = packed
                msg[2 * head + q, 32:48, :] = pack(both[j][BLOCK + 32 * q:BLOCK + 32 * (q + 1)], side).astype(bf16)


def read_chunks(chunks, proj, store, before_s, reads_out, fixed_out, gate_out):
    recept_s, value_s, alpha_s, pulled_s, upper_b, upper_k, trans_s, added_s = store
    width = recept_s.shape[1]
    pairs = width // PAIR
    masks = lane_masks(bf16)
    for c in chunks:
        block = slice(c * BLOCK, (c + 1) * BLOCK)
        for j in range(pairs):
            cols = slice(j * PAIR, (j + 1) * PAIR)
            upper = lhs3(upper_b[block, cols])
            both = nn(upper, jnp.concatenate(
                [rhs_nn(alpha_s[block, cols], masks), rhs_nn(pulled_s[block, cols], masks)], axis=1))
            reads = recept_s[block, cols] + both[:, :PAIR]
            fixed = both[:, PAIR:] + nn(lhs3(upper_k[block, cols]), rhs_nn(value_s[block, cols], masks))
            if c > 0:
                both = nt(lhs3(reads), jnp.concatenate(
                    [rhs_nt(before_s[c, :BLOCK, cols], masks), rhs_nt(before_s[c, BLOCK:, cols], masks)], axis=0))
                reads = both[:, :PAIR]
                fixed = fixed + both[:, PAIR:]
            reads_out[block, cols] = reads
            fixed_out[block, cols] = fixed
            gate_out[block, cols] = sigmoid(proj[block, 5 * width + j * PAIR:5 * width + (j + 1) * PAIR].astype(f32))


def pack(x, side):
    half = x.shape[0] // 2
    is_low = lax.broadcasted_iota(jnp.int32, (half, PAIR), 1) < HEAD
    top, bottom = x[:half], x[half:]
    if side == 0:
        return jnp.where(is_low, top, pltpu.roll(bottom, HEAD, 1))
    return jnp.where(is_low, pltpu.roll(top, HEAD, 1), bottom)


def fold(x):
    half = x.shape[0] // 2
    is_low = lax.broadcasted_iota(jnp.int32, (half, PAIR), 1) < HEAD
    return jnp.where(is_low, x[:half], x[half:])


def unfold(x):
    is_low = lax.broadcasted_iota(jnp.int32, x.shape, 1) < HEAD
    other = pltpu.roll(x, HEAD, 1)
    return jnp.concatenate([jnp.where(is_low, x, other), jnp.where(is_low, other, x)], axis=0)


def twice(change):
    change = change.astype(bf16)
    return jnp.concatenate([change, change], axis=0)


def settled(x):
    hi, lo = split(x)
    return hi.astype(f32) + lo.astype(f32)


def through_map(x, change2):
    is_low = lax.broadcasted_iota(jnp.int32, x.shape, 1) < HEAD
    hi, lo = (part.astype(f32) for part in split(x))
    return settled(hi + lo + jnp.dot(jnp.where(is_low, hi, lo).astype(bf16), change2, preferred_element_type=f32))


def unit_eye():
    row = lax.broadcasted_iota(jnp.int32, (HEAD, PAIR), 0)
    col = lax.rem(lax.broadcasted_iota(jnp.int32, (HEAD, PAIR), 1), HEAD)
    return (row == col).astype(f32)


class Map:
    def __init__(self, change, added):
        self.change, self.added = change, added
        self.operand = twice(change)

    def then(self, later):
        eye = unit_eye()
        change = through_map(self.change + eye, later.operand) - eye
        return Map(change, through_map(self.added, later.operand) + later.added)

    def apply(self, state):
        return through_map(state, self.operand) + self.added

    def message(self):
        return jnp.concatenate([fold(self.change), fold(self.added)], axis=0).astype(bf16)


def map_of(piece):
    piece = piece.astype(f32)
    return Map(unfold(piece[0:32]), unfold(piece[32:48]))


def layer(tokens, gain, wr, wk, wv, wd, wa, wg, mix, decay_base, rate_base, drift, group_gain, start, w_out, out,
          own, held, last, last_in, wbuf, norm_buf, proj, edge_s, before_s, msg, reads_s, fixed_s, gate_s,
          slab, slab_sum, across, pre_map, pre_add, back, entering, gated, token_rows, w_out_buf,
          own_sem, w_sem, out_sem, hop_send, hop_recv, edge_send, edge_recv,
          send1, recv1, send2, recv2, send3, recv3, send4, recv4, *store):
    me = here()
    y, z = me["tp"], me["z"]
    ny, nx, nc, nz = lax.axis_size("tp"), lax.axis_size("x"), lax.axis_size("c"), lax.axis_size("z")
    right, left = lax.rem(y + 1, ny), lax.rem(y + ny - 1, ny)
    far = lax.rem(y + 2, ny)
    unit = me["x"] * nc + me["c"]
    units = nx * nc
    seq = z * units + unit
    total = units * nz
    rows = own.shape[0]
    half = rows // 2
    width = wbuf.shape[2]

    def at(index, tp):
        return {"z": index // units, "x": lax.rem(index // nc, nx), "c": lax.rem(index, nc), "tp": tp}

    def in_slab(index):
        return {"z": z, "x": index // nc, "c": lax.rem(index, nc), "tp": y}

    def along(index):
        return {"z": index, "x": me["x"], "c": me["c"], "tp": y}

    def remote(src, dst, send, recv, to):
        return pltpu.make_async_remote_copy(
            src_ref=src, dst_ref=dst, send_sem=send, recv_sem=recv, device_id=to, device_id_type=MESH)

    def greet(to):
        pl.semaphore_signal(barrier, inc=1, device_id=to, device_id_type=MESH)

    fetch = pltpu.make_async_copy(tokens, own, own_sem)
    fetch.start()
    w_copies = [pltpu.make_async_copy(w, wbuf.at[i], w_sem.at[i]) for i, w in enumerate((wr, wk, wv, wd, wa, wg))]
    for copy in w_copies:
        copy.start()
    barrier = pltpu.get_barrier_semaphore()
    for d in range(1, 4):
        greet({"tp": lax.rem(y + d, ny)})
    for d in range(1, 8):
        greet(in_slab(lax.rem(unit + d, units)))
        greet(along(lax.rem(z + d, nz)))
    ends_stretch = jnp.logical_and(y == ny - 1, seq < total - 1)
    has_before = seq > 0

    @pl.when(has_before)
    def _():
        greet(at(seq - 1, ny - 1))

    pl.semaphore_wait(barrier, 17 + 4 * ends_stretch.astype(jnp.int32))
    fetch.wait()

    def part(h):
        return pl.ds(h * half, half)

    def hop(src, slot, h, to, sem):
        return remote(src, held.at[slot, part(h)], hop_send.at[sem], hop_recv.at[slot, h], {"tp": to})

    to_right = [hop(own.at[part(h)], 0, h, right, h) for h in (0, 1)]
    to_left = [hop(own.at[part(h)], 2, h, left, 2 + h) for h in (0, 1)]
    on_right = hop(held.at[0, part(0)], 1, 0, right, 4)
    on_left = hop(held.at[2, part(1)], 1, 1, left, 5)
    to_right[0].start()
    to_left[1].start()
    to_right[1].start()
    to_left[0].start()

    last[...] = own[rows - 16:rows, :].astype(f32)[15:16, :]
    edges = [remote(last, last_in.at[0], edge_send.at[k], edge_recv.at[0], at(lax.rem(seq + 1, total), k))
             for k in range(4)]
    inner = [remote(last, last_in.at[1], edge_send.at[4 + k], edge_recv.at[1], {"tp": 2 + k}) for k in range(2)]

    @pl.when(ends_stretch)
    def _():
        for copy in edges:
            copy.start()

    @pl.when(y == 1)
    def _():
        for copy in inner:
            copy.start()

    out_copy = pltpu.make_async_copy(w_out, w_out_buf, out_sem)
    out_copy.start()

    def normalize(x):
        return (x * lax.rsqrt(jnp.mean(x * x, axis=-1, keepdims=True) + NORM_FLOOR) * gain[...]).astype(bf16)

    def project(block, owner, with_edge):
        base = pl.multiple_of(owner * rows, 16)
        norm_buf[0:rows, :] = normalize(block[...].astype(f32))
        count = rows + 16 if with_edge else rows
        for i in range(6):
            res = jnp.dot(norm_buf[0:count, :], wbuf[i], preferred_element_type=f32)
            proj[pl.ds(base, rows), width * i:width * (i + 1)] = res[0:rows].astype(bf16)
            if with_edge and i < 3:
                edge_s[:, width * i:width * (i + 1)] = res[rows:].astype(bf16).astype(f32)

    for copy in w_copies:
        copy.wait()
    project(own, y, False)
    to_right[0].wait_recv()
    on_right.start()
    to_left[1].wait_recv()
    on_left.start()

    @pl.when(has_before)
    def _():
        edges[0].wait_recv()

    @pl.when(jnp.logical_not(has_before))
    def _():
        last_in[0] = jnp.zeros_like(last)

    @pl.when(y >= 2)
    def _():
        inner[0].wait_recv()

    @pl.when(y < 2)
    def _():
        last_in[1] = jnp.zeros_like(last)

    norm_buf[rows:, :] = jnp.concatenate(
        [jnp.broadcast_to(normalize(last_in[k]), (8, own.shape[1])) for k in range(2)], axis=0)
    to_right[1].wait_recv()
    project(held.at[0], left, True)
    to_left[0].wait_recv()
    project(held.at[2], right, False)

    group = GROUP * BLOCK
    early = y < 2

    def columns(i, j):
        return slice(i * width + j * PAIR, i * width + (j + 1) * PAIR)

    def first_edge(i, j):
        return jnp.where(early, edge_s[0:1, columns(i, j)], edge_s[8:9, columns(i, j)])

    def second_edge(i, j):
        return jnp.where(early, proj[group - 16:group, columns(i, j)].astype(f32)[15:16], edge_s[0:1, columns(i, j)])

    own_base = jnp.where(early, 0, group)
    state_group(own_base, first_edge, proj, mix, decay_base, rate_base, drift, store)
    on_right.wait_recv()
    on_left.wait_recv()
    project(held.at[1], far, False)
    state_group(group - own_base, second_edge, proj, mix, decay_base, rate_base, drift, store)
    compose(store[6], store[7], before_s, msg)

    def landed(buffer, sems, k):
        return remote(buffer.at[k], buffer.at[k], send1.at[0], sems.at[k], in_slab(unit))

    first = []
    for d in range(1, 8):
        peer = lax.rem(unit + d, units)
        first.append(remote(msg.at[peer], slab.at[unit], send1.at[d], recv1.at[unit], in_slab(peer)))
        first[-1].start()
    slab[unit] = msg[unit]
    read_chunks((0, 1), proj, store, before_s, reads_s, fixed_s, gate_s)

    for k in range(8):
        @pl.when(k != unit)
        def _():
            landed(slab, recv1, k).wait_recv()

    one = [map_of(slab[k]) for k in range(8)]
    two = [one[2 * k].then(one[2 * k + 1]) for k in range(4)]
    four = [two[2 * k].then(two[2 * k + 1]) for k in range(2)]
    slab_sum[...] = four[0].then(four[1]).message()

    def onward(d):
        return remote(slab_sum, across.at[z], send2.at[d], recv2.at[z], along(lax.rem(z + d, nz)))

    for d in (4, 3, 2, 1, 5, 6, 7):
        @pl.when(z + d < nz)
        def _():
            onward(d).start()

    six = four[0].then(two[2])
    before = (one[0], two[0], two[0].then(one[2]), four[0], four[0].then(one[4]), six, six.then(one[6]))
    for k in range(7):
        pre_map[k] = before[k].operand
        pre_add[k] = before[k].added
    read_chunks((2, 3, 4, 5), proj, store, before_s, reads_s, fixed_s, gate_s)
    begin = start[me["x"], pl.ds(pl.multiple_of(me["c"] * 32, 32), 32), :]
    state = jnp.concatenate([begin, begin], axis=1)
    for k in range(7):
        @pl.when(k < z)
        def _():
            landed(across, recv2, k).wait_recv()

    one = [map_of(jnp.where(k < z, across[k].astype(f32), 0.0)) for k in range(7)]
    late = one[3].then(one[4]).then(one[5].then(one[6]))
    state = late.apply(one[1].then(one[2]).apply(one[0].apply(state)))
    back[0] = fold(state).astype(bf16)
    for k in range(7):
        back[k + 1] = fold(through_map(state, pre_map[k]) + pre_add[k]).astype(bf16)
    third = []
    for d in range(1, 8):
        peer = lax.rem(unit + d, units)
        third.append(remote(back.at[peer], entering.at[unit], send3.at[d], recv3.at[unit], in_slab(peer)))
        third[-1].start()
    entering[unit] = back[unit]
    for k in range(8):
        @pl.when(k != unit)
        def _():
            landed(entering, recv3, k).wait_recv()

    masks = lane_masks(bf16)
    is_low = lax.broadcasted_iota(jnp.int32, (16, PAIR), 1) < HEAD
    turned = []
    for j in range(width // PAIR):
        parts = []
        for q in range(2):
            a, b = entering[4 * j + q].astype(f32), entering[4 * j + 2 + q].astype(f32)
            parts.append(jnp.where(is_low, a, pltpu.roll(b, HEAD, 1)))
            parts.append(jnp.where(is_low, pltpu.roll(a, HEAD, 1), b))
        diagonal = diag_parts(jnp.concatenate(parts, axis=0), masks)[0]
        turned.append(jnp.concatenate([diagonal, diagonal], axis=1))

    def share(k):
        return pl.ds(pl.multiple_of(k * rows, 16), rows)

    def gate_rows(areas):
        units = [(at_rows, j) for at_rows in areas for j in range(width // PAIR)]

        def cols(j):
            return slice(j * PAIR, (j + 1) * PAIR)

        mixed = [fixed_s[r, cols(j)] + nt(jnp.concatenate(split(reads_s[r, cols(j)]), axis=1), turned[j]) for r, j in units]
        center = [m - head_sum(m, masks) * (1.0 / HEAD) for m in mixed]
        spread = [head_sum(m * m, masks) * (1.0 / HEAD) for m in center]
        for (r, j), m, v in zip(units, center, spread):
            scaled = m * lax.rsqrt(v + GROUP_FLOOR) * group_gain[:, cols(j)]
            gated[r, cols(j)] = (scaled * gate_s[r, cols(j)]).astype(bf16)

    fourth = {}
    for d in (2, 1, 3):
        peer = lax.rem(y + d, ny)
        fourth[d] = remote(gated.at[share(peer)], token_rows.at[d], send4.at[d], recv4.at[d], {"tp": peer})
    gate_rows([share(lax.rem(y + d, ny)) for d in (2, 1, 3)])
    for d in (2, 1, 3):
        fourth[d].start()
    gate_rows([share(y)])
    out_copy.wait()

    def product(block, owner):
        return jnp.dot(block, w_out_buf[pl.ds(pl.multiple_of(owner * width, width), width), :],
                       preferred_element_type=f32)

    result = product(gated[share(y), :], y)
    for d in (1, 3, 2):
        fourth[d].wait_recv()
        result = result + product(token_rows[d], lax.rem(y + ny - d, ny))
    out[...] = result.astype(bf16)

    for copy in (*to_right, *to_left, on_right, on_left, *first, *third, *fourth.values()):
        copy.wait_send()
    for d in range(1, 8):
        @pl.when(z + d < nz)
        def _():
            onward(d).wait_send()

    @pl.when(ends_stretch)
    def _():
        for copy in edges:
            copy.wait_send()

    @pl.when(y == 1)
    def _():
        for copy in inner:
            copy.wait_send()


def call_layer(tokens, gain, weights, mix, decay_base, rate_base, drift, group_gain, start, w_out):
    rows, depth = tokens.shape
    width = weights[0].shape[1]
    inner = w_out.shape[0]
    length = 4 * rows
    dma = pltpu.SemaphoreType.DMA
    return pl.pallas_call(
        layer,
        out_shape=jax.ShapeDtypeStruct((rows, depth), bf16),
        in_specs=[ANY_SPEC, VMEM_SPEC] + [ANY_SPEC] * 6 + [VMEM_SPEC] * 3 + [SMEM_SPEC] + [VMEM_SPEC] * 2 + [ANY_SPEC],
        out_specs=VMEM_SPEC,
        scratch_shapes=[
            pltpu.VMEM((rows, depth), bf16),
            pltpu.VMEM((3, rows, depth), bf16),
            pltpu.VMEM((1, depth), f32),
            pltpu.VMEM((2, 1, depth), f32),
            pltpu.VMEM((6, depth, width), bf16),
            pltpu.VMEM((rows + 16, depth), bf16),
            pltpu.VMEM((length, 6 * width), bf16),
            pltpu.VMEM((16, 3 * width), f32),
            pltpu.VMEM((length // BLOCK, 2 * BLOCK, width), f32),
            pltpu.VMEM((8, 48, PAIR), bf16),
            pltpu.VMEM((length, width), f32),
            pltpu.VMEM((length, width), f32),
            pltpu.VMEM((length, width), f32),
            pltpu.VMEM((8, 48, PAIR), bf16),
            pltpu.VMEM((48, PAIR), bf16),
            pltpu.VMEM((8, 48, PAIR), bf16),
            pltpu.VMEM((7, PAIR, PAIR), bf16),
            pltpu.VMEM((7, 32, PAIR), f32),
            pltpu.VMEM((8, 16, PAIR), bf16),
            pltpu.VMEM((8, 16, PAIR), bf16),
            pltpu.VMEM((length, width), bf16),
            pltpu.VMEM((4, rows, width), bf16),
            pltpu.VMEM((inner, depth), bf16),
            dma(()), dma((6,)), dma(()), dma((6,)), dma((3, 2)), dma((6,)), dma((2,)),
            dma((8,)), dma((8,)), dma((8,)), dma((8,)), dma((8,)), dma((8,)), dma((4,)), dma((4,)),
        ] + [pltpu.VMEM((length, width), f32)] * 8,
        compiler_params=pltpu.CompilerParams(collective_id=0, has_side_effects=True),
        name="layer",
    )(tokens, gain, *weights, mix, decay_base, rate_base, drift, group_gain, start, w_out)


def per_device(tokens, norm_gain, w_recept, w_key, w_value, w_decay, w_rate, w_gate, shift_mix, decay_base, rate_base,
               decay_drift, group_gain, initial_state, w_out):
    return call_layer(
        tokens, norm_gain.reshape(1, -1), (w_recept, w_key, w_value, w_decay, w_rate, w_gate), shift_mix,
        decay_base.reshape(1, -1), rate_base.reshape(1, -1), decay_drift, group_gain.reshape(1, -1), initial_state, w_out)


def solution(mesh):
    finer = Mesh(mesh.devices.reshape(8, 4, 2, mesh.shape["tp"]), AXES)
    in_specs = (
        P(SP_TP, None),
        P(),
        P(None, "tp"),
        P(None, "tp"),
        P(None, "tp"),
        P(None, "tp"),
        P(None, "tp"),
        P(None, "tp"),
        P(None, "tp"),
        P("tp"),
        P("tp"),
        P(SP),
        P("tp"),
        P("tp", None, None),
        P(),
    )
    return jax.shard_map(
        per_device, mesh=finer, in_specs=in_specs, out_specs=P(SP_TP, None), check_vma=False
    )
```

```python
import functools

import jax
import jax.numpy as jnp
from jax import lax
from jax.experimental import pallas as pl
from jax.experimental.pallas import tpu as pltpu
from jax.sharding import Mesh
from jax.sharding import PartitionSpec as P

HEAD = 64
BLOCK = 64
PAIR = 128
GROUP = 3
SP = ("z", "x", "c")
SP_TP = ("z", "x", "c", "tp")
AXES = ("z", "x", "c", "tp")
MESH = pl.DeviceIdType.MESH
NORM_FLOOR = 0.5
GROUP_FLOOR = 1.0
EXP_HALF = 0.6065306597126334
f32 = jnp.float32
bf16 = jnp.bfloat16
VMEM_SPEC = pl.BlockSpec(memory_space=pltpu.VMEM)
ANY_SPEC = pl.BlockSpec(memory_space=pl.ANY)
SMEM_SPEC = pl.BlockSpec(memory_space=pltpu.SMEM)


def here():
    return {axis: lax.axis_index(axis) for axis in AXES}


def split(x):
    hi = x.astype(bf16)
    lo = (x - hi.astype(f32)).astype(bf16)
    return hi, lo


def sigmoid(x):
    return 1.0 / (1.0 + jnp.exp(-x))


def lane_masks(dtype):
    lane = lax.broadcasted_iota(jnp.int32, (1, PAIR), 1)
    low = (lane < HEAD).astype(f32)
    return low.astype(dtype), (1.0 - low).astype(dtype)


def lhs3(x):
    hi, lo = split(x)
    return jnp.concatenate([hi, lo, hi], axis=1)


def diag_parts(x, masks):
    hi, lo = split(x)
    low, high = masks
    bd_hi = jnp.concatenate([hi * low, hi * high], axis=0)
    bd_lo = jnp.concatenate([lo * low, lo * high], axis=0)
    return bd_hi, bd_lo


def rhs_nn(x, masks):
    hi, lo = diag_parts(x, masks)
    return jnp.concatenate([hi, hi, lo], axis=0)


def rhs_nt(x, masks):
    hi, lo = diag_parts(x, masks)
    return jnp.concatenate([hi, hi, lo], axis=1)


def nn(a3, b3):
    return jnp.dot(a3, b3, preferred_element_type=f32)


def nt(a3, b3):
    return lax.dot_general(a3, b3, (((1,), (1,)), ((), ())), preferred_element_type=f32)


def once(a, b, masks):
    low, high = masks
    b = b.astype(bf16)
    return nn(a.astype(bf16), jnp.concatenate([b * low, b * high], axis=0))


def settled(x):
    hi, lo = split(x)
    return hi.astype(f32) + lo.astype(f32)


def tn(a, b):
    a_hi, a_lo = split(a)
    b_hi, b_lo = split(b)
    return lax.dot_general(
        jnp.concatenate([a_hi, a_lo, a_hi], axis=0), jnp.concatenate([b_hi, b_hi, b_lo], axis=0),
        (((0,), (0,)), ((), ())), preferred_element_type=f32)


def head_sum(x, masks):
    low, high = masks
    ones = jnp.concatenate([jnp.broadcast_to(low, (HEAD, PAIR)), jnp.broadcast_to(high, (HEAD, PAIR))], axis=0)
    hi, lo = split(x)
    return jnp.dot(jnp.concatenate([hi, lo], axis=1), jnp.concatenate([ones, ones], axis=0), preferred_element_type=f32)


def state_group(base, edge_row, proj, mix, decay_base, rate_base, drift, store):
    recept_s, value_s, alpha_s, pulled_s, upper_b, upper_k, trans_s, added_s = store
    width = recept_s.shape[1]
    pairs = width // PAIR
    rows = GROUP * BLOCK
    masks = lane_masks(bf16)
    is_low = lax.broadcasted_iota(jnp.int32, (1, PAIR), 1) < HEAD
    place = lax.broadcasted_iota(jnp.int32, (BLOCK, PAIR), 0)
    other = lax.rem(lax.broadcasted_iota(jnp.int32, (BLOCK, PAIR), 1), BLOCK)
    strict = other < place
    inclusive = other <= place
    eye = (other == place).astype(f32)
    tri2 = inclusive.astype(f32).astype(bf16)
    area = pl.ds(pl.multiple_of(base, BLOCK), rows)
    units = [(i, j) for i in range(GROUP) for j in range(pairs)]

    def block(i):
        return pl.ds(pl.multiple_of(base + i * BLOCK, BLOCK), BLOCK)

    def cols(j):
        return slice(j * PAIR, (j + 1) * PAIR)

    logs, unit, rate, key, value, recept = {}, {}, {}, {}, {}, {}
    first = lax.broadcasted_iota(jnp.int32, (rows, PAIR), 0) == 0
    for j in range(pairs):
        def raw(i):
            return proj[area, i * width + j * PAIR:i * width + (j + 1) * PAIR].astype(f32)

        def shifted(i):
            now = raw(i)
            before = jnp.where(first, edge_row(i, j), pltpu.roll(now, 1, 0))
            return now + (before - now) * mix[i:i + 1, cols(j)]

        key_all = shifted(1)
        unit_all = key_all * lax.rsqrt(head_sum(key_all * key_all, masks) + 1.0)
        rate_all = sigmoid(rate_base[:, cols(j)] + raw(4))
        level_all = decay_base[:, cols(j)] + raw(3)
        recept_all = shifted(0)
        value_all = shifted(2)
        for i in range(GROUP):
            at = slice(i * BLOCK, (i + 1) * BLOCK)
            u = (i, j)
            key[u], unit[u], rate[u], value[u], recept[u] = key_all[at], unit_all[at], rate_all[at], value_all[at], recept_all[at]
            logs[u] = -EXP_HALF * sigmoid(level_all[at] + drift[base + i * BLOCK])

    run = {u: jnp.dot(tri2, jnp.concatenate(split(logs[u]), axis=0), preferred_element_type=f32) for u in units}
    alpha, scaled, by = {}, {}, {}
    beta_end, key_end = {}, {}
    for u in units:
        last = run[u][BLOCK - 1:BLOCK, :]
        inverse = jnp.exp(-run[u])
        to_end = jnp.exp(last - run[u])
        unit_rate = unit[u] * rate[u]
        alpha[u] = -unit[u] * jnp.exp(run[u] - logs[u])
        scaled[u] = recept[u] * jnp.exp(run[u])
        left = lhs3(jnp.concatenate([alpha[u], scaled[u]], axis=0))
        right = jnp.concatenate([rhs_nt(unit_rate * inverse, masks), rhs_nt(key[u] * inverse, masks)], axis=0)
        by[u] = nt(left, right)
        beta_end[u] = unit_rate * to_end
        key_end[u] = key[u] * to_end
    lower = {u: jnp.where(strict, by[u][:BLOCK, :PAIR], 0.0) for u in units}
    value3 = {u: rhs_nn(value[u], masks) for u in units}
    pulled = {u: nn(lhs3(jnp.where(strict, by[u][:BLOCK, PAIR:], 0.0)), value3[u]) for u in units}
    for u in units:
        i, j = u
        upper_b[block(i), cols(j)] = jnp.where(inclusive, by[u][BLOCK:, :PAIR], 0.0)
        upper_k[block(i), cols(j)] = jnp.where(inclusive, by[u][BLOCK:, PAIR:], 0.0)
        recept_s[block(i), cols(j)] = scaled[u]
        value_s[block(i), cols(j)] = value[u]
    inner = {u: jnp.where(lax.div(place, 4) == lax.div(other, 4), lower[u], 0.0) for u in units}
    square = {u: nn(lhs3(inner[u]), rhs_nn(inner[u], masks)) for u in units}
    solved = {u: eye + inner[u] + square[u] + nn(lhs3(inner[u]), rhs_nn(square[u], masks)) for u in units}
    for size in (4, 16):
        outside = jnp.logical_and(
            lax.div(place, 4 * size) == lax.div(other, 4 * size), lax.div(place, size) != lax.div(other, size))
        solved = {u: settled(solved[u]) for u in units}
        ahead = {u: settled(nn(lhs3(solved[u]), rhs_nn(jnp.where(outside, lower[u], 0.0), masks))) for u in units}
        grown = {u: nn(lhs3(ahead[u]), jnp.concatenate(
            [rhs_nn(ahead[u], masks), rhs_nn(solved[u], masks)], axis=1)) for u in units}
        solved = {u: settled(solved[u] + grown[u][:, PAIR:]) for u in units}
        solved = {u: solved[u] + nn(lhs3(grown[u][:, :PAIR]), rhs_nn(solved[u], masks)) for u in units}
    both = {u: nn(lhs3(solved[u]), jnp.concatenate([rhs_nn(alpha[u], masks), rhs_nn(pulled[u], masks)], axis=1))
            for u in units}
    for u in units:
        i, j = u
        alpha_s[block(i), cols(j)] = both[u][:, :PAIR]
        pulled_s[block(i), cols(j)] = both[u][:, PAIR:]
        cross = tn(both[u][:, :PAIR], beta_end[u])
        trans_s[block(i), cols(j)] = jnp.where(is_low, cross[:BLOCK], cross[BLOCK:]) + eye * jnp.exp(run[u][BLOCK - 1:BLOCK, :])
        cross = tn(jnp.concatenate([both[u][:, PAIR:], value[u]], axis=0),
                   jnp.concatenate([beta_end[u], key_end[u]], axis=0))
        added_s[block(i), cols(j)] = jnp.where(is_low, cross[:BLOCK], cross[BLOCK:])


def compose(trans_s, added_s, before_s, msg):
    width = trans_s.shape[1]
    pairs = width // PAIR
    chunks = trans_s.shape[0] // BLOCK
    masks = lane_masks(bf16)
    zero = jnp.zeros((BLOCK, PAIR), f32)
    both = {}
    for c in range(chunks):
        block = slice(c * BLOCK, (c + 1) * BLOCK)
        for j in range(pairs):
            cols = slice(j * PAIR, (j + 1) * PAIR)
            if c == 0:
                both[j] = jnp.concatenate([trans_s[block, cols], added_s[block, cols]], axis=0)
                continue
            before_s[c, :, cols] = both[j]
            both[j] = nn(lhs3(both[j]), rhs_nn(trans_s[block, cols], masks)) + jnp.concatenate(
                [zero, added_s[block, cols]], axis=0)
    for j in range(pairs):
        for side in range(2):
            head = 2 * j + side
            packed = pack(both[j][:BLOCK] - unit_eye(), side).astype(bf16)
            for q in range(2):
                msg[2 * head + q, 0:32, :] = packed
                msg[2 * head + q, 32:48, :] = pack(both[j][BLOCK + 32 * q:BLOCK + 32 * (q + 1)], side).astype(bf16)


def read_chunks(chunks, proj, store, before_s, reads_out, fixed_out, gate_out):
    recept_s, value_s, alpha_s, pulled_s, upper_b, upper_k, trans_s, added_s = store
    width = recept_s.shape[1]
    pairs = width // PAIR
    masks = lane_masks(bf16)
    for c in chunks:
        block = slice(c * BLOCK, (c + 1) * BLOCK)
        for j in range(pairs):
            cols = slice(j * PAIR, (j + 1) * PAIR)
            upper = lhs3(upper_b[block, cols])
            both = nn(upper, jnp.concatenate(
                [rhs_nn(alpha_s[block, cols], masks), rhs_nn(pulled_s[block, cols], masks)], axis=1))
            reads = recept_s[block, cols] + both[:, :PAIR]
            fixed = both[:, PAIR:] + nn(lhs3(upper_k[block, cols]), rhs_nn(value_s[block, cols], masks))
            if c > 0:
                both = nt(lhs3(reads), jnp.concatenate(
                    [rhs_nt(before_s[c, :BLOCK, cols], masks), rhs_nt(before_s[c, BLOCK:, cols], masks)], axis=0))
                reads = both[:, :PAIR]
                fixed = fixed + both[:, PAIR:]
            reads_out[block, cols] = reads
            fixed_out[block, cols] = fixed
            gate_out[block, cols] = sigmoid(proj[block, 5 * width + j * PAIR:5 * width + (j + 1) * PAIR].astype(f32))


def pack(x, side):
    half = x.shape[0] // 2
    is_low = lax.broadcasted_iota(jnp.int32, (half, PAIR), 1) < HEAD
    top, bottom = x[:half], x[half:]
    if side == 0:
        return jnp.where(is_low, top, pltpu.roll(bottom, HEAD, 1))
    return jnp.where(is_low, pltpu.roll(top, HEAD, 1), bottom)


def fold(x):
    half = x.shape[0] // 2
    is_low = lax.broadcasted_iota(jnp.int32, (half, PAIR), 1) < HEAD
    return jnp.where(is_low, x[:half], x[half:])


def unfold(x):
    is_low = lax.broadcasted_iota(jnp.int32, x.shape, 1) < HEAD
    other = pltpu.roll(x, HEAD, 1)
    return jnp.concatenate([jnp.where(is_low, x, other), jnp.where(is_low, other, x)], axis=0)


def twice(change):
    change = change.astype(bf16)
    return jnp.concatenate([change, change], axis=0)


def through_map(x, change2):
    is_low = lax.broadcasted_iota(jnp.int32, x.shape, 1) < HEAD
    hi, lo = (part.astype(f32) for part in split(x))
    return settled(hi + lo + jnp.dot(jnp.where(is_low, hi, lo).astype(bf16), change2, preferred_element_type=f32))


def unit_eye():
    row = lax.broadcasted_iota(jnp.int32, (HEAD, PAIR), 0)
    col = lax.rem(lax.broadcasted_iota(jnp.int32, (HEAD, PAIR), 1), HEAD)
    return (row == col).astype(f32)


class Map:
    def __init__(self, change, added):
        self.change, self.added = change, added
        self.operand = twice(change)

    def then(self, later):
        eye = unit_eye()
        change = through_map(self.change + eye, later.operand) - eye
        return Map(change, through_map(self.added, later.operand) + later.added)

    def apply(self, state):
        return through_map(state, self.operand) + self.added

    def message(self):
        return jnp.concatenate([fold(self.change), fold(self.added)], axis=0).astype(bf16)


def map_of(piece):
    piece = piece.astype(f32)
    return Map(unfold(piece[0:32]), unfold(piece[32:48]))


def layer(tokens, gain, wr, wk, wv, wd, wa, wg, mix, decay_base, rate_base, drift, group_gain, start, w_out, out,
          own, normed, mate_rows, others, last, last_in, wbuf, proj, edge_s, before_s, msg, reads_s, fixed_s, gate_s,
          slab, slab_sum, across, pre_map, pre_add, back, entering, gated, token_rows, w_out_buf,
          own_sem, w_sem, out_sem, hop_send, hop_recv, edge_send, edge_recv,
          send1, recv1, send2, recv2, send3, recv3, send4, recv4, ready_a, ready_b, *store):
    me = here()
    y, z = me["tp"], me["z"]
    ny, nx, nc, nz = lax.axis_size("tp"), lax.axis_size("x"), lax.axis_size("c"), lax.axis_size("z")
    far = lax.rem(y + 2, ny)
    unit = me["x"] * nc + me["c"]
    units = nx * nc
    seq = z * units + unit
    total = units * nz
    rows = own.shape[0]
    half = rows // 2
    width = wbuf.shape[2]

    def at(index, tp):
        return {"z": index // units, "x": lax.rem(index // nc, nx), "c": lax.rem(index, nc), "tp": tp}

    def in_slab(index):
        return {"z": z, "x": index // nc, "c": lax.rem(index, nc), "tp": y}

    def along(index):
        return {"z": index, "x": me["x"], "c": me["c"], "tp": y}

    def remote(src, dst, send, recv, to):
        return pltpu.make_async_remote_copy(
            src_ref=src, dst_ref=dst, send_sem=send, recv_sem=recv, device_id=to, device_id_type=MESH)

    def greet(to):
        pl.semaphore_signal(barrier, inc=1, device_id=to, device_id_type=MESH)

    fetch = pltpu.make_async_copy(tokens, own, own_sem)
    fetch.start()
    w_copies = [pltpu.make_async_copy(w, wbuf.at[i], w_sem.at[i]) for i, w in enumerate((wr, wk, wv, wd, wa, wg))]
    barrier = pltpu.get_barrier_semaphore()
    odd = lax.rem(y, 2)
    mate = y + 1 - 2 * odd
    beside = lax.rem(y + 2 * odd + ny - 1, ny)
    x_up, x_down = lax.rem(me["x"] + 1, nx), lax.rem(me["x"] + nx - 1, nx)
    z_up, z_down = lax.rem(z + 1, nz), lax.rem(z + nz - 1, nz)
    near = [{"tp": mate}, {"tp": beside}, {"c": 1 - me["c"]}, {"z": z_up}, {"z": z_down}, {"x": x_up}, {"x": x_down}]
    for to in near:
        greet(to)
    for x in (x_up, x_down):
        greet({"x": x, "c": 1 - me["c"]})
    ends_stretch = jnp.logical_and(y == ny - 1, seq < total - 1)
    has_before = seq > 0

    def normalize(x):
        return (x * lax.rsqrt(jnp.mean(x * x, axis=-1, keepdims=True) + NORM_FLOOR) * gain[...]).astype(bf16)

    fetch.wait()
    for copy in w_copies:
        copy.start()
    normed[...] = normalize(own[...].astype(f32))
    last[...] = normed[rows - 16:rows, :].astype(f32)[15:16, :]
    pl.semaphore_wait(barrier, 9)
    top, low_half = pl.ds(0, half), pl.ds(half, half)

    def quarter(k):
        return others.at[pl.ds(k * half, half)]

    def hop(src, dst, sem, to):
        return remote(src, dst, hop_send.at[sem], hop_recv.at[sem], {"tp": to})

    mate_top = hop(normed.at[top], mate_rows.at[top], 0, mate)
    mate_low = hop(normed.at[low_half], mate_rows.at[low_half], 1, mate)
    beside_low = hop(normed.at[low_half], quarter(0), 2, beside)
    far_top = hop(mate_rows.at[top], quarter(1), 3, beside)
    beside_top = hop(normed.at[top], quarter(2), 4, beside)
    far_low = hop(quarter(0), quarter(3), 5, mate)
    mate_top.start()
    beside_low.start()

    for to in near:
        pl.semaphore_signal(ready_a, inc=1, device_id=to, device_id_type=MESH)

    out_copy = pltpu.make_async_copy(w_out, w_out_buf, out_sem)
    out_copy.start()

    def project(block, parts):
        for i in range(6):
            res = jnp.dot(block[...], wbuf[i], preferred_element_type=f32)
            at_row = 0
            for base, count in parts:
                area = pl.ds(pl.multiple_of(base, 16), count)
                proj[area, width * i:width * (i + 1)] = res[at_row:at_row + count].astype(bf16)
                at_row += count
            if block is mate_rows and i < 3:
                edge_s[:, width * i:width * (i + 1)] = res[rows:].astype(bf16).astype(f32)

    for copy in w_copies:
        copy.wait()
    project(normed, [(y * rows, rows)])
    pl.semaphore_wait(ready_a, 7)
    for to in near[:3] + near[5:] + [{"z": lax.rem(z + 2, nz)}, {"z": lax.rem(z + nz - 2, nz)}]:
        pl.semaphore_signal(ready_b, inc=1, device_id=to, device_id_type=MESH)

    edge = remote(last, last_in.at[0], edge_send.at[3], edge_recv.at[0], at(lax.rem(seq + 1, total), ny - 1))
    spread_edge = [remote(last_in.at[0], last_in.at[0], edge_send.at[k], edge_recv.at[0], {"tp": k}) for k in range(3)]
    inner = [remote(last, last_in.at[1], edge_send.at[4 + k], edge_recv.at[1], {"tp": 2 + k}) for k in range(2)]
    spreads = jnp.logical_and(y == ny - 1, has_before)

    @pl.when(ends_stretch)
    def _():
        edge.start()

    @pl.when(y == 1)
    def _():
        for copy in inner:
            copy.start()

    mate_top.wait_send()
    mate_low.start()

    @pl.when(spreads)
    def _():
        edge.wait_recv()
        for copy in spread_edge:
            copy.start()

    mate_top.wait_recv()
    far_top.start()
    beside_low.wait_recv()
    mate_low.wait_send()
    far_low.start()

    @pl.when(jnp.logical_and(y < ny - 1, has_before))
    def _():
        edge.wait_recv()

    @pl.when(jnp.logical_not(has_before))
    def _():
        last_in[0] = jnp.zeros_like(last)

    @pl.when(y >= 2)
    def _():
        inner[0].wait_recv()

    @pl.when(y < 2)
    def _():
        last_in[1] = jnp.zeros_like(last)

    mate_rows[rows:, :] = jnp.concatenate(
        [jnp.broadcast_to(last_in[k], (8, own.shape[1])) for k in range(2)], axis=0).astype(bf16)
    mate_low.wait_recv()
    beside_low.wait_send()
    far_top.wait_send()
    beside_top.start()
    project(mate_rows, [(mate * rows, rows)])

    group = GROUP * BLOCK
    early = y < 2

    def columns(i, j):
        return slice(i * width + j * PAIR, i * width + (j + 1) * PAIR)

    def first_edge(i, j):
        return jnp.where(early, edge_s[0:1, columns(i, j)], edge_s[8:9, columns(i, j)])

    def second_edge(i, j):
        return jnp.where(early, proj[group - 16:group, columns(i, j)].astype(f32)[15:16], edge_s[0:1, columns(i, j)])

    own_base = jnp.where(early, 0, group)
    state_group(own_base, first_edge, proj, mix, decay_base, rate_base, drift, store)
    pl.semaphore_wait(ready_b, 7)
    far_top.wait_recv()
    project(others.at[pl.ds(0, rows)], [(beside * rows + half, half), (far * rows, half)])
    beside_top.wait_recv()
    far_low.wait_recv()
    project(others.at[pl.ds(rows, rows)], [(beside * rows, half), (far * rows + half, half)])
    state_group(group - own_base, second_edge, proj, mix, decay_base, rate_base, drift, store)
    compose(store[6], store[7], before_s, msg)

    def landed(buffer, sems, k):
        return remote(buffer.at[k], buffer.at[k], send1.at[0], sems.at[k], in_slab(unit))

    first = []
    for d in range(1, 8):
        peer = lax.rem(unit + d, units)
        first.append(remote(msg.at[peer], slab.at[unit], send1.at[d], recv1.at[unit], in_slab(peer)))
        first[-1].start()
    slab[unit] = msg[unit]
    read_chunks((0, 1), proj, store, before_s, reads_s, fixed_s, gate_s)

    for k in range(8):
        @pl.when(k != unit)
        def _():
            landed(slab, recv1, k).wait_recv()

    one = [map_of(slab[k]) for k in range(8)]
    two = [one[2 * k].then(one[2 * k + 1]) for k in range(4)]
    four = [two[2 * k].then(two[2 * k + 1]) for k in range(2)]
    slab_sum[...] = four[0].then(four[1]).message()

    def onward(d):
        return remote(slab_sum, across.at[z], send2.at[d], recv2.at[z], along(lax.rem(z + d, nz)))

    for d in (4, 3, 2, 1, 5, 6, 7):
        @pl.when(z + d < nz)
        def _():
            onward(d).start()

    six = four[0].then(two[2])
    before = (one[0], two[0], two[0].then(one[2]), four[0], four[0].then(one[4]), six, six.then(one[6]))
    for k in range(7):
        pre_map[k] = before[k].operand
        pre_add[k] = before[k].added
    read_chunks((2, 3, 4, 5), proj, store, before_s, reads_s, fixed_s, gate_s)
    begin = start[me["x"], pl.ds(pl.multiple_of(me["c"] * 32, 32), 32), :]
    state = jnp.concatenate([begin, begin], axis=1)
    for k in range(7):
        @pl.when(k < z)
        def _():
            landed(across, recv2, k).wait_recv()

    one = [map_of(jnp.where(k < z, across[k].astype(f32), 0.0)) for k in range(7)]
    late = one[3].then(one[4]).then(one[5].then(one[6]))
    state = late.apply(one[1].then(one[2]).apply(one[0].apply(state)))
    back[0] = fold(state).astype(bf16)
    for k in range(7):
        back[k + 1] = fold(through_map(state, pre_map[k]) + pre_add[k]).astype(bf16)
    third = []
    for d in range(1, 8):
        peer = lax.rem(unit + d, units)
        third.append(remote(back.at[peer], entering.at[unit], send3.at[d], recv3.at[unit], in_slab(peer)))
        third[-1].start()
    entering[unit] = back[unit]
    for k in range(8):
        @pl.when(k != unit)
        def _():
            landed(entering, recv3, k).wait_recv()

    masks = lane_masks(bf16)
    is_low = lax.broadcasted_iota(jnp.int32, (16, PAIR), 1) < HEAD
    turned = []
    for j in range(width // PAIR):
        parts = []
        for q in range(2):
            a, b = entering[4 * j + q].astype(f32), entering[4 * j + 2 + q].astype(f32)
            parts.append(jnp.where(is_low, a, pltpu.roll(b, HEAD, 1)))
            parts.append(jnp.where(is_low, pltpu.roll(a, HEAD, 1), b))
        diagonal = diag_parts(jnp.concatenate(parts, axis=0), masks)[0]
        turned.append(jnp.concatenate([diagonal, diagonal], axis=1))

    def share(k):
        return pl.ds(pl.multiple_of(k * rows, 16), rows)

    def gate_rows(areas):
        units = [(at_rows, j) for at_rows in areas for j in range(width // PAIR)]

        def cols(j):
            return slice(j * PAIR, (j + 1) * PAIR)

        mixed = [fixed_s[r, cols(j)] + nt(jnp.concatenate(split(reads_s[r, cols(j)]), axis=1), turned[j]) for r, j in units]
        center = [m - head_sum(m, masks) * (1.0 / HEAD) for m in mixed]
        spread = [head_sum(m * m, masks) * (1.0 / HEAD) for m in center]
        for (r, j), m, v in zip(units, center, spread):
            scaled = m * lax.rsqrt(v + GROUP_FLOOR) * group_gain[:, cols(j)]
            gated[r, cols(j)] = (scaled * gate_s[r, cols(j)]).astype(bf16)

    fourth = {}
    for d in (2, 1, 3):
        peer = lax.rem(y + d, ny)
        fourth[d] = remote(gated.at[share(peer)], token_rows.at[d], send4.at[d], recv4.at[d], {"tp": peer})
    gate_rows([share(lax.rem(y + d, ny)) for d in (2, 1, 3)])
    for d in (2, 1, 3):
        fourth[d].start()
    gate_rows([share(y)])
    out_copy.wait()

    def product(block, owner):
        return jnp.dot(block, w_out_buf[pl.ds(pl.multiple_of(owner * width, width), width), :],
                       preferred_element_type=f32)

    result = product(gated[share(y), :], y)
    for d in (1, 3, 2):
        fourth[d].wait_recv()
        result = result + product(token_rows[d], lax.rem(y + ny - d, ny))
    out[...] = result.astype(bf16)

    for copy in (beside_top, far_low, *first, *third, *fourth.values()):
        copy.wait_send()
    for d in range(1, 8):
        @pl.when(z + d < nz)
        def _():
            onward(d).wait_send()

    @pl.when(ends_stretch)
    def _():
        edge.wait_send()

    @pl.when(spreads)
    def _():
        for copy in spread_edge:
            copy.wait_send()

    @pl.when(y == 1)
    def _():
        for copy in inner:
            copy.wait_send()


def call_layer(tokens, gain, weights, mix, decay_base, rate_base, drift, group_gain, start, w_out):
    rows, depth = tokens.shape
    width = weights[0].shape[1]
    inner = w_out.shape[0]
    length = 4 * rows
    dma = pltpu.SemaphoreType.DMA
    return pl.pallas_call(
        layer,
        out_shape=jax.ShapeDtypeStruct((rows, depth), bf16),
        in_specs=[ANY_SPEC, VMEM_SPEC] + [ANY_SPEC] * 6 + [VMEM_SPEC] * 3 + [SMEM_SPEC] + [VMEM_SPEC] * 2 + [ANY_SPEC],
        out_specs=VMEM_SPEC,
        scratch_shapes=[
            pltpu.VMEM((rows, depth), bf16),
            pltpu.VMEM((rows, depth), bf16),
            pltpu.VMEM((rows + 16, depth), bf16),
            pltpu.VMEM((2 * rows, depth), bf16),
            pltpu.VMEM((1, depth), f32),
            pltpu.VMEM((2, 1, depth), f32),
            pltpu.VMEM((6, depth, width), bf16),
            pltpu.VMEM((length, 6 * width), bf16),
            pltpu.VMEM((16, 3 * width), f32),
            pltpu.VMEM((length // BLOCK, 2 * BLOCK, width), f32),
            pltpu.VMEM((8, 48, PAIR), bf16),
            pltpu.VMEM((length, width), f32),
            pltpu.VMEM((length, width), f32),
            pltpu.VMEM((length, width), f32),
            pltpu.VMEM((8, 48, PAIR), bf16),
            pltpu.VMEM((48, PAIR), bf16),
            pltpu.VMEM((8, 48, PAIR), bf16),
            pltpu.VMEM((7, PAIR, PAIR), bf16),
            pltpu.VMEM((7, 32, PAIR), f32),
            pltpu.VMEM((8, 16, PAIR), bf16),
            pltpu.VMEM((8, 16, PAIR), bf16),
            pltpu.VMEM((length, width), bf16),
            pltpu.VMEM((4, rows, width), bf16),
            pltpu.VMEM((inner, depth), bf16),
            dma(()), dma((6,)), dma(()), dma((6,)), dma((6,)), dma((6,)), dma((2,)),
            dma((8,)), dma((8,)), dma((8,)), dma((8,)), dma((8,)), dma((8,)), dma((4,)), dma((4,)),
            pltpu.SemaphoreType.REGULAR, pltpu.SemaphoreType.REGULAR,
        ] + [pltpu.VMEM((length, width), f32)] * 8,
        compiler_params=pltpu.CompilerParams(collective_id=0, has_side_effects=True),
        name="layer",
    )(tokens, gain, *weights, mix, decay_base, rate_base, drift, group_gain, start, w_out)


def per_device(tokens, norm_gain, w_recept, w_key, w_value, w_decay, w_rate, w_gate, shift_mix, decay_base, rate_base,
               decay_drift, group_gain, initial_state, w_out):
    return call_layer(
        tokens, norm_gain.reshape(1, -1), (w_recept, w_key, w_value, w_decay, w_rate, w_gate), shift_mix,
        decay_base.reshape(1, -1), rate_base.reshape(1, -1), decay_drift, group_gain.reshape(1, -1), initial_state, w_out)


def solution(mesh):
    finer = Mesh(mesh.devices.reshape(8, 4, 2, mesh.shape["tp"]), AXES)
    in_specs = (
        P(SP_TP, None),
        P(),
        P(None, "tp"),
        P(None, "tp"),
        P(None, "tp"),
        P(None, "tp"),
        P(None, "tp"),
        P(None, "tp"),
        P(None, "tp"),
        P("tp"),
        P("tp"),
        P(SP),
        P("tp"),
        P("tp", None, None),
        P(),
    )
    return jax.shard_map(
        per_device, mesh=finer, in_specs=in_specs, out_specs=P(SP_TP, None), check_vma=False
    )
```

```python
import functools

import jax
import jax.numpy as jnp
from jax import lax
from jax.experimental import pallas as pl
from jax.experimental.pallas import tpu as pltpu
from jax.sharding import Mesh
from jax.sharding import PartitionSpec as P

HEAD = 64
BLOCK = 64
PAIR = 128
GROUP = 3
SP = ("z", "x", "c")
SP_TP = ("z", "x", "c", "tp")
AXES = ("z", "x", "c", "tp")
MESH = pl.DeviceIdType.MESH
NORM_FLOOR = 0.5
GROUP_FLOOR = 1.0
EXP_HALF = 0.6065306597126334
f32 = jnp.float32
bf16 = jnp.bfloat16
VMEM_SPEC = pl.BlockSpec(memory_space=pltpu.VMEM)
ANY_SPEC = pl.BlockSpec(memory_space=pl.ANY)
SMEM_SPEC = pl.BlockSpec(memory_space=pltpu.SMEM)


def here():
    return {axis: lax.axis_index(axis) for axis in AXES}


def split(x):
    hi = x.astype(bf16)
    lo = (x - hi.astype(f32)).astype(bf16)
    return hi, lo


def sigmoid(x):
    return 1.0 / (1.0 + jnp.exp(-x))


def lane_masks(dtype):
    lane = lax.broadcasted_iota(jnp.int32, (1, PAIR), 1)
    low = (lane < HEAD).astype(f32)
    return low.astype(dtype), (1.0 - low).astype(dtype)


def lhs3(x):
    hi, lo = split(x)
    return jnp.concatenate([hi, lo, hi], axis=1)


def diag_parts(x, masks):
    hi, lo = split(x)
    low, high = masks
    bd_hi = jnp.concatenate([hi * low, hi * high], axis=0)
    bd_lo = jnp.concatenate([lo * low, lo * high], axis=0)
    return bd_hi, bd_lo


def rhs_nn(x, masks):
    hi, lo = diag_parts(x, masks)
    return jnp.concatenate([hi, hi, lo], axis=0)


def rhs_nt(x, masks):
    hi, lo = diag_parts(x, masks)
    return jnp.concatenate([hi, hi, lo], axis=1)


def rhs_turned(x, masks):
    hi, lo = diag_parts(x, masks)
    hi, lo = hi.T, lo.T
    return jnp.concatenate([hi, hi, lo], axis=0)


def nn(a3, b3):
    return jnp.dot(a3, b3, preferred_element_type=f32)


def nt(a3, b3):
    return lax.dot_general(a3, b3, (((1,), (1,)), ((), ())), preferred_element_type=f32)


def once(a, b, masks):
    low, high = masks
    b = b.astype(bf16)
    return nn(a.astype(bf16), jnp.concatenate([b * low, b * high], axis=0))


def settled(x):
    hi, lo = split(x)
    return hi.astype(f32) + lo.astype(f32)


def tn(a, b):
    a_hi, a_lo = split(a)
    b_hi, b_lo = split(b)
    return lax.dot_general(
        jnp.concatenate([a_hi, a_lo, a_hi], axis=0), jnp.concatenate([b_hi, b_hi, b_lo], axis=0),
        (((0,), (0,)), ((), ())), preferred_element_type=f32)


def head_sum(x, masks):
    low, high = masks
    ones = jnp.concatenate([jnp.broadcast_to(low, (HEAD, PAIR)), jnp.broadcast_to(high, (HEAD, PAIR))], axis=0)
    hi, lo = split(x)
    return jnp.dot(jnp.concatenate([hi, lo], axis=1), jnp.concatenate([ones, ones], axis=0), preferred_element_type=f32)


def state_group(base, edge_row, proj, mix, decay_base, rate_base, drift, store):
    recept_s, value_s, alpha_s, pulled_s, upper_b, upper_k, trans_s, added_s = store
    width = recept_s.shape[1]
    pairs = width // PAIR
    rows = GROUP * BLOCK
    masks = lane_masks(bf16)
    is_low = lax.broadcasted_iota(jnp.int32, (1, PAIR), 1) < HEAD
    place = lax.broadcasted_iota(jnp.int32, (BLOCK, PAIR), 0)
    other = lax.rem(lax.broadcasted_iota(jnp.int32, (BLOCK, PAIR), 1), BLOCK)
    strict = other < place
    inclusive = other <= place
    eye = (other == place).astype(f32)
    tri2 = inclusive.astype(f32).astype(bf16)
    area = pl.ds(pl.multiple_of(base, BLOCK), rows)
    units = [(i, j) for i in range(GROUP) for j in range(pairs)]

    def block(i):
        return pl.ds(pl.multiple_of(base + i * BLOCK, BLOCK), BLOCK)

    def cols(j):
        return slice(j * PAIR, (j + 1) * PAIR)

    logs, unit, rate, key, value, recept = {}, {}, {}, {}, {}, {}
    first = lax.broadcasted_iota(jnp.int32, (rows, PAIR), 0) == 0
    for j in range(pairs):
        def raw(i):
            return proj[area, i * width + j * PAIR:i * width + (j + 1) * PAIR].astype(f32)

        def shifted(i):
            now = raw(i)
            before = jnp.where(first, edge_row(i, j), pltpu.roll(now, 1, 0))
            return now + (before - now) * mix[i:i + 1, cols(j)]

        key_all = shifted(1)
        unit_all = key_all * lax.rsqrt(head_sum(key_all * key_all, masks) + 1.0)
        rate_all = sigmoid(rate_base[:, cols(j)] + raw(4))
        level_all = decay_base[:, cols(j)] + raw(3)
        recept_all = shifted(0)
        value_all = shifted(2)
        for i in range(GROUP):
            at = slice(i * BLOCK, (i + 1) * BLOCK)
            u = (i, j)
            key[u], unit[u], rate[u], value[u], recept[u] = key_all[at], unit_all[at], rate_all[at], value_all[at], recept_all[at]
            logs[u] = -EXP_HALF * sigmoid(level_all[at] + drift[base + i * BLOCK])

    run = {u: jnp.dot(tri2, jnp.concatenate(split(logs[u]), axis=0), preferred_element_type=f32) for u in units}
    alpha, scaled, by = {}, {}, {}
    beta_end, key_end = {}, {}
    for u in units:
        last = run[u][BLOCK - 1:BLOCK, :]
        inverse = jnp.exp(-run[u])
        to_end = jnp.exp(last - run[u])
        unit_rate = unit[u] * rate[u]
        alpha[u] = -unit[u] * jnp.exp(run[u] - logs[u])
        scaled[u] = recept[u] * jnp.exp(run[u])
        left = lhs3(jnp.concatenate([alpha[u], scaled[u]], axis=0))
        right = jnp.concatenate([rhs_turned(unit_rate * inverse, masks), rhs_turned(key[u] * inverse, masks)], axis=1)
        by[u] = nn(left, right)
        beta_end[u] = unit_rate * to_end
        key_end[u] = key[u] * to_end
    lower = {u: jnp.where(strict, by[u][:BLOCK, :PAIR], 0.0) for u in units}
    value3 = {u: rhs_nn(value[u], masks) for u in units}
    pulled = {u: nn(lhs3(jnp.where(strict, by[u][:BLOCK, PAIR:], 0.0)), value3[u]) for u in units}
    for u in units:
        i, j = u
        upper_b[block(i), cols(j)] = jnp.where(inclusive, by[u][BLOCK:, :PAIR], 0.0)
        upper_k[block(i), cols(j)] = jnp.where(inclusive, by[u][BLOCK:, PAIR:], 0.0)
        recept_s[block(i), cols(j)] = scaled[u]
        value_s[block(i), cols(j)] = value[u]
    inner = {u: jnp.where(lax.div(place, 4) == lax.div(other, 4), lower[u], 0.0) for u in units}
    square = {u: nn(lhs3(inner[u]), rhs_nn(inner[u], masks)) for u in units}
    solved = {u: eye + inner[u] + square[u] + nn(lhs3(inner[u]), rhs_nn(square[u], masks)) for u in units}
    for size in (4, 16):
        outside = jnp.logical_and(
            lax.div(place, 4 * size) == lax.div(other, 4 * size), lax.div(place, size) != lax.div(other, size))
        solved = {u: settled(solved[u]) for u in units}
        ahead = {u: settled(nn(lhs3(solved[u]), rhs_nn(jnp.where(outside, lower[u], 0.0), masks))) for u in units}
        grown = {u: nn(lhs3(ahead[u]), jnp.concatenate(
            [rhs_nn(ahead[u], masks), rhs_nn(solved[u], masks)], axis=1)) for u in units}
        solved = {u: settled(solved[u] + grown[u][:, PAIR:]) for u in units}
        solved = {u: solved[u] + nn(lhs3(grown[u][:, :PAIR]), rhs_nn(solved[u], masks)) for u in units}
    both = {u: nn(lhs3(solved[u]), jnp.concatenate([rhs_nn(alpha[u], masks), rhs_nn(pulled[u], masks)], axis=1))
            for u in units}
    for u in units:
        i, j = u
        alpha_s[block(i), cols(j)] = both[u][:, :PAIR]
        pulled_s[block(i), cols(j)] = both[u][:, PAIR:]
        cross = tn(both[u][:, :PAIR], beta_end[u])
        trans_s[block(i), cols(j)] = jnp.where(is_low, cross[:BLOCK], cross[BLOCK:]) + eye * jnp.exp(run[u][BLOCK - 1:BLOCK, :])
        cross = tn(jnp.concatenate([both[u][:, PAIR:], value[u]], axis=0),
                   jnp.concatenate([beta_end[u], key_end[u]], axis=0))
        added_s[block(i), cols(j)] = jnp.where(is_low, cross[:BLOCK], cross[BLOCK:])


def compose_half(base, trans_s, added_s, before_s):
    width = trans_s.shape[1]
    pairs = width // PAIR
    masks = lane_masks(bf16)
    zero = jnp.zeros((BLOCK, PAIR), f32)
    both = {}
    for c in range(GROUP):
        block = pl.ds(pl.multiple_of(base + c * BLOCK, BLOCK), BLOCK)
        for j in range(pairs):
            cols = slice(j * PAIR, (j + 1) * PAIR)
            if c == 0:
                both[j] = jnp.concatenate([trans_s[block, cols], added_s[block, cols]], axis=0)
                continue
            before_s[base // BLOCK + c, :, cols] = both[j]
            both[j] = nn(lhs3(both[j]), rhs_nn(trans_s[block, cols], masks)) + jnp.concatenate(
                [zero, added_s[block, cols]], axis=0)
    return both


def join_halves(first, second, msg, half_s):
    masks = lane_masks(bf16)
    for j in range(len(first)):
        half_s[:, j * PAIR:(j + 1) * PAIR] = first[j]
        both = nn(lhs3(first[j]), rhs_nn(second[j][:BLOCK], masks))
        change = both[:BLOCK] - unit_eye()
        added = both[BLOCK:] + second[j][BLOCK:]
        for side in range(2):
            head = 2 * j + side
            packed = pack(change, side).astype(bf16)
            for q in range(2):
                msg[2 * head + q, 0:32, :] = packed
                msg[2 * head + q, 32:48, :] = pack(added[32 * q:32 * (q + 1)], side).astype(bf16)


def read_chunks(chunks, proj, store, before_s, half_s, reads_out, fixed_out, gate_out):
    recept_s, value_s, alpha_s, pulled_s, upper_b, upper_k, trans_s, added_s = store
    width = recept_s.shape[1]
    pairs = width // PAIR
    masks = lane_masks(bf16)
    for c in chunks:
        block = slice(c * BLOCK, (c + 1) * BLOCK)
        for j in range(pairs):
            cols = slice(j * PAIR, (j + 1) * PAIR)
            upper = lhs3(upper_b[block, cols])
            both = nn(upper, jnp.concatenate(
                [rhs_nn(alpha_s[block, cols], masks), rhs_nn(pulled_s[block, cols], masks)], axis=1))
            reads = recept_s[block, cols] + both[:, :PAIR]
            fixed = both[:, PAIR:] + nn(lhs3(upper_k[block, cols]), rhs_nn(value_s[block, cols], masks))
            for earlier in ([before_s.at[c]] if c % GROUP else []) + ([half_s] if c >= GROUP else []):
                both = nt(lhs3(reads), jnp.concatenate(
                    [rhs_nt(earlier[:BLOCK, cols], masks), rhs_nt(earlier[BLOCK:, cols], masks)], axis=0))
                reads = both[:, :PAIR]
                fixed = fixed + both[:, PAIR:]
            reads_out[block, cols] = reads
            fixed_out[block, cols] = fixed
            gate_out[block, cols] = sigmoid(proj[block, 5 * width + j * PAIR:5 * width + (j + 1) * PAIR].astype(f32))


def pack(x, side):
    half = x.shape[0] // 2
    is_low = lax.broadcasted_iota(jnp.int32, (half, PAIR), 1) < HEAD
    top, bottom = x[:half], x[half:]
    if side == 0:
        return jnp.where(is_low, top, pltpu.roll(bottom, HEAD, 1))
    return jnp.where(is_low, pltpu.roll(top, HEAD, 1), bottom)


def fold(x):
    half = x.shape[0] // 2
    is_low = lax.broadcasted_iota(jnp.int32, (half, PAIR), 1) < HEAD
    return jnp.where(is_low, x[:half], x[half:])


def unfold(x):
    is_low = lax.broadcasted_iota(jnp.int32, x.shape, 1) < HEAD
    other = pltpu.roll(x, HEAD, 1)
    return jnp.concatenate([jnp.where(is_low, x, other), jnp.where(is_low, other, x)], axis=0)


def twice(change):
    change = change.astype(bf16)
    return jnp.concatenate([change, change], axis=0)


def through_map(x, change2):
    is_low = lax.broadcasted_iota(jnp.int32, x.shape, 1) < HEAD
    hi, lo = (part.astype(f32) for part in split(x))
    return settled(hi + lo + jnp.dot(jnp.where(is_low, hi, lo).astype(bf16), change2, preferred_element_type=f32))


def unit_eye():
    row = lax.broadcasted_iota(jnp.int32, (HEAD, PAIR), 0)
    col = lax.rem(lax.broadcasted_iota(jnp.int32, (HEAD, PAIR), 1), HEAD)
    return (row == col).astype(f32)


class Map:
    def __init__(self, change, added):
        self.change, self.added = change, added
        self.operand = twice(change)

    def then(self, later):
        eye = unit_eye()
        change = through_map(self.change + eye, later.operand) - eye
        return Map(change, through_map(self.added, later.operand) + later.added)

    def apply(self, state):
        return through_map(state, self.operand) + self.added

    def message(self):
        return jnp.concatenate([fold(self.change), fold(self.added)], axis=0).astype(bf16)


def map_of(piece):
    piece = piece.astype(f32)
    return Map(unfold(piece[0:32]), unfold(piece[32:48]))


def layer(tokens, gain, wr, wk, wv, wd, wa, wg, mix, decay_base, rate_base, drift, group_gain, start, w_out, out,
          own, normed, mate_rows, others, last, last_in, wbuf, proj, edge_s, before_s, half_s, half_own, msg, reads_s, fixed_s, gate_s,
          slab, slab_sum, across, pre_map, pre_add, back, entering, gated, token_rows, w_out_buf,
          own_sem, w_sem, out_sem, hop_send, hop_recv, edge_send, edge_recv,
          send1, recv1, send2, recv2, send3, recv3, send4, recv4, ready_a, ready_b, *store):
    me = here()
    y, z = me["tp"], me["z"]
    ny, nx, nc, nz = lax.axis_size("tp"), lax.axis_size("x"), lax.axis_size("c"), lax.axis_size("z")
    far = lax.rem(y + 2, ny)
    unit = me["x"] * nc + me["c"]
    units = nx * nc
    seq = z * units + unit
    total = units * nz
    rows = own.shape[0]
    half = rows // 2
    width = wbuf.shape[2]

    def at(index, tp):
        return {"z": index // units, "x": lax.rem(index // nc, nx), "c": lax.rem(index, nc), "tp": tp}

    def in_slab(index):
        return {"z": z, "x": index // nc, "c": lax.rem(index, nc), "tp": y}

    def along(index):
        return {"z": index, "x": me["x"], "c": me["c"], "tp": y}

    def remote(src, dst, send, recv, to):
        return pltpu.make_async_remote_copy(
            src_ref=src, dst_ref=dst, send_sem=send, recv_sem=recv, device_id=to, device_id_type=MESH)

    def greet(to):
        pl.semaphore_signal(barrier, inc=1, device_id=to, device_id_type=MESH)

    fetch = pltpu.make_async_copy(tokens, own, own_sem)
    fetch.start()
    w_copies = [pltpu.make_async_copy(w, wbuf.at[i], w_sem.at[i]) for i, w in enumerate((wr, wk, wv, wd, wa, wg))]
    barrier = pltpu.get_barrier_semaphore()
    odd = lax.rem(y, 2)
    mate = y + 1 - 2 * odd
    beside = lax.rem(y + 2 * odd + ny - 1, ny)
    x_up, x_down = lax.rem(me["x"] + 1, nx), lax.rem(me["x"] + nx - 1, nx)
    z_up, z_down = lax.rem(z + 1, nz), lax.rem(z + nz - 1, nz)
    near = [{"tp": mate}, {"tp": beside}, {"c": 1 - me["c"]}, {"z": z_up}, {"z": z_down}, {"x": x_up}, {"x": x_down}]
    for to in near:
        greet(to)
    for x in (x_up, x_down):
        greet({"x": x, "c": 1 - me["c"]})
    ends_stretch = jnp.logical_and(y == ny - 1, seq < total - 1)
    has_before = seq > 0

    def normalize(x):
        return (x * lax.rsqrt(jnp.mean(x * x, axis=-1, keepdims=True) + NORM_FLOOR) * gain[...]).astype(bf16)

    fetch.wait()
    for copy in w_copies:
        copy.start()
    normed[...] = normalize(own[...].astype(f32))
    last[...] = normed[rows - 16:rows, :].astype(f32)[15:16, :]
    pl.semaphore_wait(barrier, 9)
    top, low_half = pl.ds(0, half), pl.ds(half, half)

    def quarter(k):
        return others.at[pl.ds(k * half, half)]

    def hop(src, dst, sem, to):
        return remote(src, dst, hop_send.at[sem], hop_recv.at[sem], {"tp": to})

    mate_top = hop(normed.at[top], mate_rows.at[top], 0, mate)
    mate_low = hop(normed.at[low_half], mate_rows.at[low_half], 1, mate)
    beside_low = hop(normed.at[low_half], quarter(0), 2, beside)
    far_top = hop(mate_rows.at[top], quarter(1), 3, beside)
    beside_top = hop(normed.at[top], quarter(2), 4, beside)
    far_low = hop(quarter(0), quarter(3), 5, mate)
    mate_top.start()
    beside_low.start()

    for to in near:
        pl.semaphore_signal(ready_a, inc=1, device_id=to, device_id_type=MESH)

    out_copy = pltpu.make_async_copy(w_out, w_out_buf, out_sem)
    out_copy.start()

    def project(block, parts):
        for i in range(6):
            res = jnp.dot(block[...], wbuf[i], preferred_element_type=f32)
            at_row = 0
            for base, count in parts:
                area = pl.ds(pl.multiple_of(base, 16), count)
                proj[area, width * i:width * (i + 1)] = res[at_row:at_row + count].astype(bf16)
                at_row += count
            if block is mate_rows and i < 3:
                edge_s[:, width * i:width * (i + 1)] = res[rows:].astype(bf16).astype(f32)

    for copy in w_copies:
        copy.wait()
    project(normed, [(y * rows, rows)])
    pl.semaphore_wait(ready_a, 7)
    for to in near[:3] + near[5:] + [{"z": lax.rem(z + 2, nz)}, {"z": lax.rem(z + nz - 2, nz)}]:
        pl.semaphore_signal(ready_b, inc=1, device_id=to, device_id_type=MESH)

    edge = remote(last, last_in.at[0], edge_send.at[3], edge_recv.at[0], at(lax.rem(seq + 1, total), ny - 1))
    spread_edge = [remote(last_in.at[0], last_in.at[0], edge_send.at[k], edge_recv.at[0], {"tp": k}) for k in range(3)]
    inner = [remote(last, last_in.at[1], edge_send.at[4 + k], edge_recv.at[1], {"tp": 2 + k}) for k in range(2)]
    spreads = jnp.logical_and(y == ny - 1, has_before)

    @pl.when(ends_stretch)
    def _():
        edge.start()

    @pl.when(y == 1)
    def _():
        for copy in inner:
            copy.start()

    mate_top.wait_send()
    mate_low.start()
    beside_low.wait_send()
    beside_top.start()

    @pl.when(spreads)
    def _():
        edge.wait_recv()
        for copy in spread_edge:
            copy.start()

    mate_top.wait_recv()
    beside_low.wait_recv()
    beside_top.wait_send()
    far_top.start()
    mate_low.wait_send()
    far_low.start()

    @pl.when(jnp.logical_and(y < ny - 1, has_before))
    def _():
        edge.wait_recv()

    @pl.when(jnp.logical_not(has_before))
    def _():
        last_in[0] = jnp.zeros_like(last)

    @pl.when(y >= 2)
    def _():
        inner[0].wait_recv()

    @pl.when(y < 2)
    def _():
        last_in[1] = jnp.zeros_like(last)

    mate_rows[rows:, :] = jnp.concatenate(
        [jnp.broadcast_to(last_in[k], (8, own.shape[1])) for k in range(2)], axis=0).astype(bf16)
    mate_low.wait_recv()
    project(mate_rows, [(mate * rows, rows)])

    group = GROUP * BLOCK
    early = y < 2

    def columns(i, j):
        return slice(i * width + j * PAIR, i * width + (j + 1) * PAIR)

    def first_edge(i, j):
        return jnp.where(early, edge_s[0:1, columns(i, j)], edge_s[8:9, columns(i, j)])

    def second_edge(i, j):
        return jnp.where(early, proj[group - 16:group, columns(i, j)].astype(f32)[15:16], edge_s[0:1, columns(i, j)])

    own_base = jnp.where(early, 0, group)
    state_group(own_base, first_edge, proj, mix, decay_base, rate_base, drift, store)
    own_half = compose_half(own_base, store[6], store[7], before_s)
    for j, both in own_half.items():
        half_own[:, j * PAIR:(j + 1) * PAIR] = both
    pl.semaphore_wait(ready_b, 7)
    far_top.wait_recv()
    beside_top.wait_recv()
    far_low.wait_recv()
    project(others, [(beside * rows + half, half), (far * rows, half), (beside * rows, half), (far * rows + half, half)])
    state_group(group - own_base, second_edge, proj, mix, decay_base, rate_base, drift, store)
    other_half = compose_half(group - own_base, store[6], store[7], before_s)
    ours = {j: half_own[:, j * PAIR:(j + 1) * PAIR] for j in other_half}
    join_halves({j: jnp.where(early, ours[j], other_half[j]) for j in ours},
                {j: jnp.where(early, other_half[j], ours[j]) for j in ours}, msg, half_s)

    def landed(buffer, sems, k):
        return remote(buffer.at[k], buffer.at[k], send1.at[0], sems.at[k], in_slab(unit))

    first = []
    for d in (4, 3, 5, 2, 6, 1, 7):
        peer = lax.rem(unit + d, units)
        first.append(remote(msg.at[peer], slab.at[unit], send1.at[d], recv1.at[unit], in_slab(peer)))
        first[-1].start()
    slab[unit] = msg[unit]
    read_chunks((0, 1, 2, 3), proj, store, before_s, half_s, reads_s, fixed_s, gate_s)

    for k in range(8):
        @pl.when(k != unit)
        def _():
            landed(slab, recv1, k).wait_recv()

    one = [map_of(slab[k]) for k in range(8)]
    two = [one[2 * k].then(one[2 * k + 1]) for k in range(4)]
    four = [two[2 * k].then(two[2 * k + 1]) for k in range(2)]
    slab_sum[...] = four[0].then(four[1]).message()

    def onward(d):
        return remote(slab_sum, across.at[z], send2.at[d], recv2.at[z], along(lax.rem(z + d, nz)))

    for d in (4, 5, 3, 6, 2, 7, 1):
        @pl.when(z + d < nz)
        def _():
            onward(d).start()

    six = four[0].then(two[2])
    before = (one[0], two[0], two[0].then(one[2]), four[0], four[0].then(one[4]), six, six.then(one[6]))
    for k in range(7):
        pre_map[k] = before[k].operand
        pre_add[k] = before[k].added
    read_chunks((4, 5), proj, store, before_s, half_s, reads_s, fixed_s, gate_s)
    begin = start[me["x"], pl.ds(pl.multiple_of(me["c"] * 32, 32), 32), :]
    state = jnp.concatenate([begin, begin], axis=1)
    for k in range(7):
        @pl.when(k < z)
        def _():
            landed(across, recv2, k).wait_recv()

    one = [map_of(jnp.where(k < z, across[k].astype(f32), 0.0)) for k in range(7)]
    late = one[3].then(one[4]).then(one[5].then(one[6]))
    state = late.apply(one[1].then(one[2]).apply(one[0].apply(state)))
    back[0] = fold(state).astype(bf16)
    for k in range(7):
        back[k + 1] = fold(through_map(state, pre_map[k]) + pre_add[k]).astype(bf16)
    third = []
    for d in (4, 3, 5, 2, 6, 1, 7):
        peer = lax.rem(unit + d, units)
        third.append(remote(back.at[peer], entering.at[unit], send3.at[d], recv3.at[unit], in_slab(peer)))
        third[-1].start()
    entering[unit] = back[unit]
    for k in range(8):
        @pl.when(k != unit)
        def _():
            landed(entering, recv3, k).wait_recv()

    masks = lane_masks(bf16)
    is_low = lax.broadcasted_iota(jnp.int32, (16, PAIR), 1) < HEAD
    turned = []
    for j in range(width // PAIR):
        parts = []
        for q in range(2):
            a, b = entering[4 * j + q].astype(f32), entering[4 * j + 2 + q].astype(f32)
            parts.append(jnp.where(is_low, a, pltpu.roll(b, HEAD, 1)))
            parts.append(jnp.where(is_low, pltpu.roll(a, HEAD, 1), b))
        diagonal = diag_parts(jnp.concatenate(parts, axis=0), masks)[0]
        turned.append(jnp.concatenate([diagonal, diagonal], axis=1))

    def share(k):
        return pl.ds(pl.multiple_of(k * rows, 16), rows)

    def gate_rows(areas):
        units = [(at_rows, j) for at_rows in areas for j in range(width // PAIR)]

        def cols(j):
            return slice(j * PAIR, (j + 1) * PAIR)

        mixed = [fixed_s[r, cols(j)] + nt(jnp.concatenate(split(reads_s[r, cols(j)]), axis=1), turned[j]) for r, j in units]
        center = [m - head_sum(m, masks) * (1.0 / HEAD) for m in mixed]
        spread = [head_sum(m * m, masks) * (1.0 / HEAD) for m in center]
        for (r, j), m, v in zip(units, center, spread):
            scaled = m * lax.rsqrt(v + GROUP_FLOOR) * group_gain[:, cols(j)]
            gated[r, cols(j)] = (scaled * gate_s[r, cols(j)]).astype(bf16)

    fourth = {}
    for d in (2, 1, 3):
        peer = lax.rem(y + d, ny)
        fourth[d] = remote(gated.at[share(peer)], token_rows.at[d], send4.at[d], recv4.at[d], {"tp": peer})
    gate_rows([share(lax.rem(y + d, ny)) for d in (2, 1, 3)])
    for d in (2, 1, 3):
        fourth[d].start()
    gate_rows([share(y)])
    out_copy.wait()

    def product(block, owner):
        return jnp.dot(block, w_out_buf[pl.ds(pl.multiple_of(owner * width, width), width), :],
                       preferred_element_type=f32)

    result = product(gated[share(y), :], y)
    for d in (1, 3, 2):
        fourth[d].wait_recv()
        result = result + product(token_rows[d], lax.rem(y + ny - d, ny))
    out[...] = result.astype(bf16)

    for copy in (far_top, far_low, *first, *third, *fourth.values()):
        copy.wait_send()
    for d in range(1, 8):
        @pl.when(z + d < nz)
        def _():
            onward(d).wait_send()

    @pl.when(ends_stretch)
    def _():
        edge.wait_send()

    @pl.when(spreads)
    def _():
        for copy in spread_edge:
            copy.wait_send()

    @pl.when(y == 1)
    def _():
        for copy in inner:
            copy.wait_send()


def call_layer(tokens, gain, weights, mix, decay_base, rate_base, drift, group_gain, start, w_out):
    rows, depth = tokens.shape
    width = weights[0].shape[1]
    inner = w_out.shape[0]
    length = 4 * rows
    dma = pltpu.SemaphoreType.DMA
    return pl.pallas_call(
        layer,
        out_shape=jax.ShapeDtypeStruct((rows, depth), bf16),
        in_specs=[ANY_SPEC, VMEM_SPEC] + [ANY_SPEC] * 6 + [VMEM_SPEC] * 3 + [SMEM_SPEC] + [VMEM_SPEC] * 2 + [ANY_SPEC],
        out_specs=VMEM_SPEC,
        scratch_shapes=[
            pltpu.VMEM((rows, depth), bf16),
            pltpu.VMEM((rows, depth), bf16),
            pltpu.VMEM((rows + 16, depth), bf16),
            pltpu.VMEM((2 * rows, depth), bf16),
            pltpu.VMEM((1, depth), f32),
            pltpu.VMEM((2, 1, depth), f32),
            pltpu.VMEM((6, depth, width), bf16),
            pltpu.VMEM((length, 6 * width), bf16),
            pltpu.VMEM((16, 3 * width), f32),
            pltpu.VMEM((length // BLOCK, 2 * BLOCK, width), f32),
            pltpu.VMEM((2 * BLOCK, width), f32),
            pltpu.VMEM((2 * BLOCK, width), f32),
            pltpu.VMEM((8, 48, PAIR), bf16),
            pltpu.VMEM((length, width), f32),
            pltpu.VMEM((length, width), f32),
            pltpu.VMEM((length, width), f32),
            pltpu.VMEM((8, 48, PAIR), bf16),
            pltpu.VMEM((48, PAIR), bf16),
            pltpu.VMEM((8, 48, PAIR), bf16),
            pltpu.VMEM((7, PAIR, PAIR), bf16),
            pltpu.VMEM((7, 32, PAIR), f32),
            pltpu.VMEM((8, 16, PAIR), bf16),
            pltpu.VMEM((8, 16, PAIR), bf16),
            pltpu.VMEM((length, width), bf16),
            pltpu.VMEM((4, rows, width), bf16),
            pltpu.VMEM((inner, depth), bf16),
            dma(()), dma((6,)), dma(()), dma((6,)), dma((6,)), dma((6,)), dma((2,)),
            dma((8,)), dma((8,)), dma((8,)), dma((8,)), dma((8,)), dma((8,)), dma((4,)), dma((4,)),
            pltpu.SemaphoreType.REGULAR, pltpu.SemaphoreType.REGULAR,
        ] + [pltpu.VMEM((length, width), f32)] * 8,
        compiler_params=pltpu.CompilerParams(collective_id=0, has_side_effects=True),
        name="layer",
    )(tokens, gain, *weights, mix, decay_base, rate_base, drift, group_gain, start, w_out)


def per_device(tokens, norm_gain, w_recept, w_key, w_value, w_decay, w_rate, w_gate, shift_mix, decay_base, rate_base,
               decay_drift, group_gain, initial_state, w_out):
    return call_layer(
        tokens, norm_gain.reshape(1, -1), (w_recept, w_key, w_value, w_decay, w_rate, w_gate), shift_mix,
        decay_base.reshape(1, -1), rate_base.reshape(1, -1), decay_drift, group_gain.reshape(1, -1), initial_state, w_out)


def solution(mesh):
    finer = Mesh(mesh.devices.reshape(8, 4, 2, mesh.shape["tp"]), AXES)
    in_specs = (
        P(SP_TP, None),
        P(),
        P(None, "tp"),
        P(None, "tp"),
        P(None, "tp"),
        P(None, "tp"),
        P(None, "tp"),
        P(None, "tp"),
        P(None, "tp"),
        P("tp"),
        P("tp"),
        P(SP),
        P("tp"),
        P("tp", None, None),
        P(),
    )
    return jax.shard_map(
        per_device, mesh=finer, in_specs=in_specs, out_specs=P(SP_TP, None), check_vma=False
    )
```

```python
import functools

import jax
import jax.numpy as jnp
from jax import lax
from jax.experimental import pallas as pl
from jax.experimental.pallas import tpu as pltpu
from jax.sharding import Mesh
from jax.sharding import PartitionSpec as P

HEAD = 64
BLOCK = 64
PAIR = 128
GROUP = 3
SP = ("z", "x", "c")
SP_TP = ("z", "x", "c", "tp")
AXES = ("z", "x", "c", "tp")
MESH = pl.DeviceIdType.MESH
NORM_FLOOR = 0.5
GROUP_FLOOR = 1.0
EXP_HALF = 0.6065306597126334
f32 = jnp.float32
bf16 = jnp.bfloat16
VMEM_SPEC = pl.BlockSpec(memory_space=pltpu.VMEM)
ANY_SPEC = pl.BlockSpec(memory_space=pl.ANY)
SMEM_SPEC = pl.BlockSpec(memory_space=pltpu.SMEM)


def here():
    return {axis: lax.axis_index(axis) for axis in AXES}


def split(x):
    hi = x.astype(bf16)
    lo = (x - hi.astype(f32)).astype(bf16)
    return hi, lo


def sigmoid(x):
    return 1.0 / (1.0 + jnp.exp(-x))


def lane_masks(dtype):
    lane = lax.broadcasted_iota(jnp.int32, (1, PAIR), 1)
    low = (lane < HEAD).astype(f32)
    return low.astype(dtype), (1.0 - low).astype(dtype)


def lhs3(x):
    hi, lo = split(x)
    return jnp.concatenate([hi, lo, hi], axis=1)


def diag_parts(x, masks):
    hi, lo = split(x)
    low, high = masks
    bd_hi = jnp.concatenate([hi * low, hi * high], axis=0)
    bd_lo = jnp.concatenate([lo * low, lo * high], axis=0)
    return bd_hi, bd_lo


def rhs_nn(x, masks):
    hi, lo = diag_parts(x, masks)
    return jnp.concatenate([hi, hi, lo], axis=0)


def rhs_nt(x, masks):
    hi, lo = diag_parts(x, masks)
    return jnp.concatenate([hi, hi, lo], axis=1)


def rhs_turned(x, masks):
    hi, lo = diag_parts(x, masks)
    hi, lo = hi.T, lo.T
    return jnp.concatenate([hi, hi, lo], axis=0)


def nn(a3, b3):
    return jnp.dot(a3, b3, preferred_element_type=f32)


def nt(a3, b3):
    return lax.dot_general(a3, b3, (((1,), (1,)), ((), ())), preferred_element_type=f32)


def once(a, b, masks):
    low, high = masks
    b = b.astype(bf16)
    return nn(a.astype(bf16), jnp.concatenate([b * low, b * high], axis=0))


def settled(x):
    hi, lo = split(x)
    return hi.astype(f32) + lo.astype(f32)


def turned_once(a, b):
    return lax.dot_general(
        a.astype(bf16), b.astype(bf16), (((0,), (0,)), ((), ())), preferred_element_type=f32)


def head_sum(x, masks):
    low, high = masks
    ones = jnp.concatenate([jnp.broadcast_to(low, (HEAD, PAIR)), jnp.broadcast_to(high, (HEAD, PAIR))], axis=0)
    hi, lo = split(x)
    return jnp.dot(jnp.concatenate([hi, lo], axis=1), jnp.concatenate([ones, ones], axis=0), preferred_element_type=f32)


def state_group(base, edge_row, proj, mix, decay_base, rate_base, drift, store):
    recept_s, value_s, alpha_s, pulled_s, upper_b, upper_k, trans_s, added_s = store
    width = recept_s.shape[1]
    pairs = width // PAIR
    rows = GROUP * BLOCK
    masks = lane_masks(bf16)
    is_low = lax.broadcasted_iota(jnp.int32, (1, PAIR), 1) < HEAD
    place = lax.broadcasted_iota(jnp.int32, (BLOCK, PAIR), 0)
    other = lax.rem(lax.broadcasted_iota(jnp.int32, (BLOCK, PAIR), 1), BLOCK)
    strict = other < place
    inclusive = other <= place
    eye = (other == place).astype(f32)
    tri2 = inclusive.astype(f32).astype(bf16)
    area = pl.ds(pl.multiple_of(base, BLOCK), rows)
    units = [(i, j) for i in range(GROUP) for j in range(pairs)]

    def block(i):
        return pl.ds(pl.multiple_of(base + i * BLOCK, BLOCK), BLOCK)

    def cols(j):
        return slice(j * PAIR, (j + 1) * PAIR)

    logs, unit, rate, key, value, recept = {}, {}, {}, {}, {}, {}
    first = lax.broadcasted_iota(jnp.int32, (rows, PAIR), 0) == 0
    for j in range(pairs):
        def raw(i):
            return proj[area, i * width + j * PAIR:i * width + (j + 1) * PAIR].astype(f32)

        def shifted(i):
            now = raw(i)
            before = jnp.where(first, edge_row(i, j), pltpu.roll(now, 1, 0))
            return now + (before - now) * mix[i:i + 1, cols(j)]

        key_all = shifted(1)
        unit_all = key_all * lax.rsqrt(head_sum(key_all * key_all, masks) + 1.0)
        rate_all = sigmoid(rate_base[:, cols(j)] + raw(4))
        level_all = decay_base[:, cols(j)] + raw(3)
        recept_all = shifted(0)
        value_all = shifted(2)
        for i in range(GROUP):
            at = slice(i * BLOCK, (i + 1) * BLOCK)
            u = (i, j)
            key[u], unit[u], rate[u], value[u], recept[u] = key_all[at], unit_all[at], rate_all[at], value_all[at], recept_all[at]
            logs[u] = -EXP_HALF * sigmoid(level_all[at] + drift[base + i * BLOCK])

    run = {u: jnp.dot(tri2, jnp.concatenate(split(logs[u]), axis=0), preferred_element_type=f32) for u in units}
    alpha, scaled, by = {}, {}, {}
    beta_end, key_end = {}, {}
    for u in units:
        last = run[u][BLOCK - 1:BLOCK, :]
        inverse = jnp.exp(-run[u])
        to_end = jnp.exp(last - run[u])
        unit_rate = unit[u] * rate[u]
        alpha[u] = -unit[u] * jnp.exp(run[u] - logs[u])
        scaled[u] = recept[u] * jnp.exp(run[u])
        left = lhs3(jnp.concatenate([alpha[u], scaled[u]], axis=0))
        right = jnp.concatenate([rhs_turned(unit_rate * inverse, masks), rhs_turned(key[u] * inverse, masks)], axis=1)
        by[u] = nn(left, right)
        beta_end[u] = unit_rate * to_end
        key_end[u] = key[u] * to_end
    lower = {u: jnp.where(strict, by[u][:BLOCK, :PAIR], 0.0) for u in units}
    value3 = {u: rhs_nn(value[u], masks) for u in units}
    pulled = {u: nn(lhs3(jnp.where(strict, by[u][:BLOCK, PAIR:], 0.0)), value3[u]) for u in units}
    for u in units:
        i, j = u
        upper_b[block(i), cols(j)] = jnp.where(inclusive, by[u][BLOCK:, :PAIR], 0.0)
        upper_k[block(i), cols(j)] = jnp.where(inclusive, by[u][BLOCK:, PAIR:], 0.0)
        recept_s[block(i), cols(j)] = scaled[u]
        value_s[block(i), cols(j)] = value[u]
    inner = {u: jnp.where(lax.div(place, 4) == lax.div(other, 4), lower[u], 0.0) for u in units}
    square = {u: nn(lhs3(inner[u]), rhs_nn(inner[u], masks)) for u in units}
    solved = {u: eye + inner[u] + square[u] + nn(lhs3(inner[u]), rhs_nn(square[u], masks)) for u in units}
    for size in (4, 16):
        outside = jnp.logical_and(
            lax.div(place, 4 * size) == lax.div(other, 4 * size), lax.div(place, size) != lax.div(other, size))
        solved = {u: settled(solved[u]) for u in units}
        ahead = {u: settled(nn(lhs3(solved[u]), rhs_nn(jnp.where(outside, lower[u], 0.0), masks))) for u in units}
        grown = {u: nn(lhs3(ahead[u]), jnp.concatenate(
            [rhs_nn(ahead[u], masks), rhs_nn(solved[u], masks)], axis=1)) for u in units}
        solved = {u: settled(solved[u] + grown[u][:, PAIR:]) for u in units}
        solved = {u: solved[u] + nn(lhs3(grown[u][:, :PAIR]), rhs_nn(solved[u], masks)) for u in units}
    both = {u: nn(lhs3(solved[u]), jnp.concatenate([rhs_nn(alpha[u], masks), rhs_nn(pulled[u], masks)], axis=1))
            for u in units}
    for u in units:
        i, j = u
        alpha_s[block(i), cols(j)] = both[u][:, :PAIR]
        pulled_s[block(i), cols(j)] = both[u][:, PAIR:]
        cross = turned_once(both[u][:, :PAIR], beta_end[u])
        trans_s[block(i), cols(j)] = jnp.where(is_low, cross[:BLOCK], cross[BLOCK:]) + eye * jnp.exp(run[u][BLOCK - 1:BLOCK, :])
        cross = turned_once(jnp.concatenate([both[u][:, PAIR:], value[u]], axis=0),
                            jnp.concatenate([beta_end[u], key_end[u]], axis=0))
        added_s[block(i), cols(j)] = jnp.where(is_low, cross[:BLOCK], cross[BLOCK:])


def compose_half(base, trans_s, added_s, before_s):
    width = trans_s.shape[1]
    pairs = width // PAIR
    masks = lane_masks(bf16)
    zero = jnp.zeros((BLOCK, PAIR), f32)
    both = {}
    for c in range(GROUP):
        block = pl.ds(pl.multiple_of(base + c * BLOCK, BLOCK), BLOCK)
        for j in range(pairs):
            cols = slice(j * PAIR, (j + 1) * PAIR)
            if c == 0:
                both[j] = jnp.concatenate([trans_s[block, cols], added_s[block, cols]], axis=0)
                continue
            before_s[base // BLOCK + c, :, cols] = both[j]
            both[j] = nn(lhs3(both[j]), rhs_nn(trans_s[block, cols], masks)) + jnp.concatenate(
                [zero, added_s[block, cols]], axis=0)
    return both


def join_halves(first, second, msg, half_s):
    masks = lane_masks(bf16)
    for j in range(len(first)):
        half_s[:, j * PAIR:(j + 1) * PAIR] = first[j]
        both = nn(lhs3(first[j]), rhs_nn(second[j][:BLOCK], masks))
        change = both[:BLOCK] - unit_eye()
        added = both[BLOCK:] + second[j][BLOCK:]
        for side in range(2):
            head = 2 * j + side
            packed = pack(change, side).astype(bf16)
            for q in range(2):
                msg[2 * head + q, 0:32, :] = packed
                msg[2 * head + q, 32:48, :] = pack(added[32 * q:32 * (q + 1)], side).astype(bf16)


def read_chunks(chunks, proj, store, before_s, half_s, reads_out, fixed_out, gate_out):
    recept_s, value_s, alpha_s, pulled_s, upper_b, upper_k, trans_s, added_s = store
    width = recept_s.shape[1]
    pairs = width // PAIR
    masks = lane_masks(bf16)
    for c in chunks:
        block = slice(c * BLOCK, (c + 1) * BLOCK)
        for j in range(pairs):
            cols = slice(j * PAIR, (j + 1) * PAIR)
            upper = lhs3(upper_b[block, cols])
            both = nn(upper, jnp.concatenate(
                [rhs_nn(alpha_s[block, cols], masks), rhs_nn(pulled_s[block, cols], masks)], axis=1))
            reads = recept_s[block, cols] + both[:, :PAIR]
            fixed = both[:, PAIR:] + nn(lhs3(upper_k[block, cols]), rhs_nn(value_s[block, cols], masks))
            for earlier in ([before_s.at[c]] if c % GROUP else []) + ([half_s] if c >= GROUP else []):
                both = nt(lhs3(reads), jnp.concatenate(
                    [rhs_nt(earlier[:BLOCK, cols], masks), rhs_nt(earlier[BLOCK:, cols], masks)], axis=0))
                reads = both[:, :PAIR]
                fixed = fixed + both[:, PAIR:]
            reads_out[block, cols] = reads
            fixed_out[block, cols] = fixed
            gate_out[block, cols] = sigmoid(proj[block, 5 * width + j * PAIR:5 * width + (j + 1) * PAIR].astype(f32))


def pack(x, side):
    half = x.shape[0] // 2
    is_low = lax.broadcasted_iota(jnp.int32, (half, PAIR), 1) < HEAD
    top, bottom = x[:half], x[half:]
    if side == 0:
        return jnp.where(is_low, top, pltpu.roll(bottom, HEAD, 1))
    return jnp.where(is_low, pltpu.roll(top, HEAD, 1), bottom)


def fold(x):
    half = x.shape[0] // 2
    is_low = lax.broadcasted_iota(jnp.int32, (half, PAIR), 1) < HEAD
    return jnp.where(is_low, x[:half], x[half:])


def unfold(x):
    is_low = lax.broadcasted_iota(jnp.int32, x.shape, 1) < HEAD
    other = pltpu.roll(x, HEAD, 1)
    return jnp.concatenate([jnp.where(is_low, x, other), jnp.where(is_low, other, x)], axis=0)


def twice(change):
    change = change.astype(bf16)
    return jnp.concatenate([change, change], axis=0)


def through_map(x, change2):
    is_low = lax.broadcasted_iota(jnp.int32, x.shape, 1) < HEAD
    hi, lo = (part.astype(f32) for part in split(x))
    return settled(hi + lo + jnp.dot(jnp.where(is_low, hi, lo).astype(bf16), change2, preferred_element_type=f32))


def unit_eye():
    row = lax.broadcasted_iota(jnp.int32, (HEAD, PAIR), 0)
    col = lax.rem(lax.broadcasted_iota(jnp.int32, (HEAD, PAIR), 1), HEAD)
    return (row == col).astype(f32)


class Map:
    def __init__(self, change, added):
        self.change, self.added = change, added
        self.operand = twice(change)

    def then(self, later):
        eye = unit_eye()
        change = through_map(self.change + eye, later.operand) - eye
        return Map(change, through_map(self.added, later.operand) + later.added)

    def apply(self, state):
        return through_map(state, self.operand) + self.added

    def message(self):
        return jnp.concatenate([fold(self.change), fold(self.added)], axis=0).astype(bf16)


def map_of(piece):
    piece = piece.astype(f32)
    return Map(unfold(piece[0:32]), unfold(piece[32:48]))


def layer(tokens, gain, wr, wk, wv, wd, wa, wg, mix, decay_base, rate_base, drift, group_gain, start, w_out, out,
          own, normed, mate_rows, others, last, last_in, wbuf, proj, edge_s, before_s, half_s, half_own, msg, reads_s, fixed_s, gate_s,
          slab, slab_sum, across, pre_map, pre_add, back, entering, gated, token_rows, w_out_buf,
          own_sem, w_sem, out_sem, hop_send, hop_recv, edge_send, edge_recv,
          send1, recv1, send2, recv2, send3, recv3, send4, recv4, ready_a, ready_b, *store):
    me = here()
    y, z = me["tp"], me["z"]
    ny, nx, nc, nz = lax.axis_size("tp"), lax.axis_size("x"), lax.axis_size("c"), lax.axis_size("z")
    far = lax.rem(y + 2, ny)
    unit = me["x"] * nc + me["c"]
    units = nx * nc
    seq = z * units + unit
    total = units * nz
    rows = own.shape[0]
    half = rows // 2
    width = wbuf.shape[2]

    def at(index, tp):
        return {"z": index // units, "x": lax.rem(index // nc, nx), "c": lax.rem(index, nc), "tp": tp}

    def in_slab(index):
        return {"z": z, "x": index // nc, "c": lax.rem(index, nc), "tp": y}

    def along(index):
        return {"z": index, "x": me["x"], "c": me["c"], "tp": y}

    def remote(src, dst, send, recv, to):
        return pltpu.make_async_remote_copy(
            src_ref=src, dst_ref=dst, send_sem=send, recv_sem=recv, device_id=to, device_id_type=MESH)

    def greet(to):
        pl.semaphore_signal(barrier, inc=1, device_id=to, device_id_type=MESH)

    fetch = pltpu.make_async_copy(tokens, own, own_sem)
    fetch.start()
    w_copies = [pltpu.make_async_copy(w, wbuf.at[i], w_sem.at[i]) for i, w in enumerate((wr, wk, wv, wd, wa, wg))]
    barrier = pltpu.get_barrier_semaphore()
    odd = lax.rem(y, 2)
    mate = y + 1 - 2 * odd
    beside = lax.rem(y + 2 * odd + ny - 1, ny)
    x_up, x_down = lax.rem(me["x"] + 1, nx), lax.rem(me["x"] + nx - 1, nx)
    z_up, z_down = lax.rem(z + 1, nz), lax.rem(z + nz - 1, nz)
    near = [{"tp": mate}, {"tp": beside}, {"c": 1 - me["c"]}, {"z": z_up}, {"z": z_down}, {"x": x_up}, {"x": x_down}]
    for to in near:
        greet(to)
    for x in (x_up, x_down):
        greet({"x": x, "c": 1 - me["c"]})
    ends_stretch = jnp.logical_and(y == ny - 1, seq < total - 1)
    has_before = seq > 0

    def normalize(x):
        return (x * lax.rsqrt(jnp.mean(x * x, axis=-1, keepdims=True) + NORM_FLOOR) * gain[...]).astype(bf16)

    fetch.wait()
    for copy in w_copies:
        copy.start()
    normed[...] = normalize(own[...].astype(f32))
    last[...] = normed[rows - 16:rows, :].astype(f32)[15:16, :]
    pl.semaphore_wait(barrier, 9)
    top, low_half = pl.ds(0, half), pl.ds(half, half)

    def quarter(k):
        return others.at[pl.ds(k * half, half)]

    def hop(src, dst, sem, to):
        return remote(src, dst, hop_send.at[sem], hop_recv.at[sem], {"tp": to})

    mate_top = hop(normed.at[top], mate_rows.at[top], 0, mate)
    mate_low = hop(normed.at[low_half], mate_rows.at[low_half], 1, mate)
    beside_low = hop(normed.at[low_half], quarter(0), 2, beside)
    far_top = hop(mate_rows.at[top], quarter(1), 3, beside)
    beside_top = hop(normed.at[top], quarter(2), 4, beside)
    far_low = hop(quarter(0), quarter(3), 5, mate)
    mate_top.start()
    beside_low.start()

    for to in near:
        pl.semaphore_signal(ready_a, inc=1, device_id=to, device_id_type=MESH)

    out_copy = pltpu.make_async_copy(w_out, w_out_buf, out_sem)
    out_copy.start()

    def project(block, parts):
        for i in range(6):
            res = jnp.dot(block[...], wbuf[i], preferred_element_type=f32)
            at_row = 0
            for base, count in parts:
                area = pl.ds(pl.multiple_of(base, 16), count)
                proj[area, width * i:width * (i + 1)] = res[at_row:at_row + count].astype(bf16)
                at_row += count
            if block is mate_rows and i < 3:
                edge_s[:, width * i:width * (i + 1)] = res[rows:].astype(bf16).astype(f32)

    for copy in w_copies:
        copy.wait()
    project(normed, [(y * rows, rows)])
    pl.semaphore_wait(ready_a, 7)
    for to in near[:3] + near[5:] + [{"z": lax.rem(z + 2, nz)}, {"z": lax.rem(z + nz - 2, nz)}]:
        pl.semaphore_signal(ready_b, inc=1, device_id=to, device_id_type=MESH)

    edge = remote(last, last_in.at[0], edge_send.at[3], edge_recv.at[0], at(lax.rem(seq + 1, total), ny - 1))
    spread_edge = [remote(last_in.at[0], last_in.at[0], edge_send.at[k], edge_recv.at[0], {"tp": k}) for k in range(3)]
    inner = [remote(last, last_in.at[1], edge_send.at[4 + k], edge_recv.at[1], {"tp": 2 + k}) for k in range(2)]
    spreads = jnp.logical_and(y == ny - 1, has_before)

    @pl.when(ends_stretch)
    def _():
        edge.start()

    @pl.when(y == 1)
    def _():
        for copy in inner:
            copy.start()

    mate_top.wait_send()
    mate_low.start()
    beside_low.wait_send()
    beside_top.start()

    @pl.when(spreads)
    def _():
        edge.wait_recv()
        for copy in spread_edge:
            copy.start()

    mate_top.wait_recv()
    beside_low.wait_recv()
    beside_top.wait_send()
    far_top.start()
    mate_low.wait_send()
    far_low.start()

    @pl.when(jnp.logical_and(y < ny - 1, has_before))
    def _():
        edge.wait_recv()

    @pl.when(jnp.logical_not(has_before))
    def _():
        last_in[0] = jnp.zeros_like(last)

    @pl.when(y >= 2)
    def _():
        inner[0].wait_recv()

    @pl.when(y < 2)
    def _():
        last_in[1] = jnp.zeros_like(last)

    mate_rows[rows:, :] = jnp.concatenate(
        [jnp.broadcast_to(last_in[k], (8, own.shape[1])) for k in range(2)], axis=0).astype(bf16)
    mate_low.wait_recv()
    project(mate_rows, [(mate * rows, rows)])

    group = GROUP * BLOCK
    early = y < 2

    def columns(i, j):
        return slice(i * width + j * PAIR, i * width + (j + 1) * PAIR)

    def first_edge(i, j):
        return jnp.where(early, edge_s[0:1, columns(i, j)], edge_s[8:9, columns(i, j)])

    def second_edge(i, j):
        return jnp.where(early, proj[group - 16:group, columns(i, j)].astype(f32)[15:16], edge_s[0:1, columns(i, j)])

    own_base = jnp.where(early, 0, group)
    state_group(own_base, first_edge, proj, mix, decay_base, rate_base, drift, store)
    own_half = compose_half(own_base, store[6], store[7], before_s)
    for j, both in own_half.items():
        half_own[:, j * PAIR:(j + 1) * PAIR] = both
    pl.semaphore_wait(ready_b, 7)
    far_top.wait_recv()
    beside_top.wait_recv()
    far_low.wait_recv()
    project(others, [(beside * rows + half, half), (far * rows, half), (beside * rows, half), (far * rows + half, half)])
    state_group(group - own_base, second_edge, proj, mix, decay_base, rate_base, drift, store)
    other_half = compose_half(group - own_base, store[6], store[7], before_s)
    ours = {j: half_own[:, j * PAIR:(j + 1) * PAIR] for j in other_half}
    join_halves({j: jnp.where(early, ours[j], other_half[j]) for j in ours},
                {j: jnp.where(early, other_half[j], ours[j]) for j in ours}, msg, half_s)

    def landed(buffer, sems, k):
        return remote(buffer.at[k], buffer.at[k], send1.at[0], sems.at[k], in_slab(unit))

    first = []
    for d in (4, 3, 5, 2, 6, 1, 7):
        peer = lax.rem(unit + d, units)
        first.append(remote(msg.at[peer], slab.at[unit], send1.at[d], recv1.at[unit], in_slab(peer)))
        first[-1].start()
    slab[unit] = msg[unit]
    read_chunks((0, 1, 2, 3), proj, store, before_s, half_s, reads_s, fixed_s, gate_s)

    for k in range(8):
        @pl.when(k != unit)
        def _():
            landed(slab, recv1, k).wait_recv()

    one = [map_of(slab[k]) for k in range(8)]
    two = [one[2 * k].then(one[2 * k + 1]) for k in range(4)]
    four = [two[2 * k].then(two[2 * k + 1]) for k in range(2)]
    slab_sum[...] = four[0].then(four[1]).message()

    def onward(d):
        return remote(slab_sum, across.at[z], send2.at[d], recv2.at[z], along(lax.rem(z + d, nz)))

    for d in (4, 5, 3, 6, 2, 7, 1):
        @pl.when(z + d < nz)
        def _():
            onward(d).start()

    six = four[0].then(two[2])
    before = (one[0], two[0], two[0].then(one[2]), four[0], four[0].then(one[4]), six, six.then(one[6]))
    for k in range(7):
        pre_map[k] = before[k].operand
        pre_add[k] = before[k].added
    read_chunks((4, 5), proj, store, before_s, half_s, reads_s, fixed_s, gate_s)
    begin = start[me["x"], pl.ds(pl.multiple_of(me["c"] * 32, 32), 32), :]
    state = jnp.concatenate([begin, begin], axis=1)
    for k in range(7):
        @pl.when(k < z)
        def _():
            landed(across, recv2, k).wait_recv()

    one = [map_of(jnp.where(k < z, across[k].astype(f32), 0.0)) for k in range(7)]
    late = one[3].then(one[4]).then(one[5].then(one[6]))
    state = late.apply(one[1].then(one[2]).apply(one[0].apply(state)))
    back[0] = fold(state).astype(bf16)
    for k in range(7):
        back[k + 1] = fold(through_map(state, pre_map[k]) + pre_add[k]).astype(bf16)
    third = []
    for d in (4, 3, 5, 2, 6, 1, 7):
        peer = lax.rem(unit + d, units)
        third.append(remote(back.at[peer], entering.at[unit], send3.at[d], recv3.at[unit], in_slab(peer)))
        third[-1].start()
    entering[unit] = back[unit]
    for k in range(8):
        @pl.when(k != unit)
        def _():
            landed(entering, recv3, k).wait_recv()

    masks = lane_masks(bf16)
    is_low = lax.broadcasted_iota(jnp.int32, (16, PAIR), 1) < HEAD
    turned = []
    for j in range(width // PAIR):
        parts = []
        for q in range(2):
            a, b = entering[4 * j + q].astype(f32), entering[4 * j + 2 + q].astype(f32)
            parts.append(jnp.where(is_low, a, pltpu.roll(b, HEAD, 1)))
            parts.append(jnp.where(is_low, pltpu.roll(a, HEAD, 1), b))
        diagonal = diag_parts(jnp.concatenate(parts, axis=0), masks)[0]
        turned.append(jnp.concatenate([diagonal, diagonal], axis=1))

    def share(k):
        return pl.ds(pl.multiple_of(k * rows, 16), rows)

    def gate_rows(areas):
        units = [(at_rows, j) for at_rows in areas for j in range(width // PAIR)]

        def cols(j):
            return slice(j * PAIR, (j + 1) * PAIR)

        mixed = [fixed_s[r, cols(j)] + nt(jnp.concatenate(split(reads_s[r, cols(j)]), axis=1), turned[j]) for r, j in units]
        center = [m - head_sum(m, masks) * (1.0 / HEAD) for m in mixed]
        spread = [head_sum(m * m, masks) * (1.0 / HEAD) for m in center]
        for (r, j), m, v in zip(units, center, spread):
            scaled = m * lax.rsqrt(v + GROUP_FLOOR) * group_gain[:, cols(j)]
            gated[r, cols(j)] = (scaled * gate_s[r, cols(j)]).astype(bf16)

    fourth = {}
    for d in (2, 1, 3):
        peer = lax.rem(y + d, ny)
        fourth[d] = remote(gated.at[share(peer)], token_rows.at[d], send4.at[d], recv4.at[d], {"tp": peer})
    gate_rows([share(lax.rem(y + d, ny)) for d in (2, 1, 3)])
    for d in (2, 1, 3):
        fourth[d].start()
    gate_rows([share(y)])
    out_copy.wait()

    def product(block, owner):
        return jnp.dot(block, w_out_buf[pl.ds(pl.multiple_of(owner * width, width), width), :],
                       preferred_element_type=f32)

    result = product(gated[share(y), :], y)
    for d in (1, 3, 2):
        fourth[d].wait_recv()
        result = result + product(token_rows[d], lax.rem(y + ny - d, ny))
    out[...] = result.astype(bf16)

    for copy in (far_top, far_low, *first, *third, *fourth.values()):
        copy.wait_send()
    for d in range(1, 8):
        @pl.when(z + d < nz)
        def _():
            onward(d).wait_send()

    @pl.when(ends_stretch)
    def _():
        edge.wait_send()

    @pl.when(spreads)
    def _():
        for copy in spread_edge:
            copy.wait_send()

    @pl.when(y == 1)
    def _():
        for copy in inner:
            copy.wait_send()


def call_layer(tokens, gain, weights, mix, decay_base, rate_base, drift, group_gain, start, w_out):
    rows, depth = tokens.shape
    width = weights[0].shape[1]
    inner = w_out.shape[0]
    length = 4 * rows
    dma = pltpu.SemaphoreType.DMA
    return pl.pallas_call(
        layer,
        out_shape=jax.ShapeDtypeStruct((rows, depth), bf16),
        in_specs=[ANY_SPEC, VMEM_SPEC] + [ANY_SPEC] * 6 + [VMEM_SPEC] * 3 + [SMEM_SPEC] + [VMEM_SPEC] * 2 + [ANY_SPEC],
        out_specs=VMEM_SPEC,
        scratch_shapes=[
            pltpu.VMEM((rows, depth), bf16),
            pltpu.VMEM((rows, depth), bf16),
            pltpu.VMEM((rows + 16, depth), bf16),
            pltpu.VMEM((2 * rows, depth), bf16),
            pltpu.VMEM((1, depth), f32),
            pltpu.VMEM((2, 1, depth), f32),
            pltpu.VMEM((6, depth, width), bf16),
            pltpu.VMEM((length, 6 * width), bf16),
            pltpu.VMEM((16, 3 * width), f32),
            pltpu.VMEM((length // BLOCK, 2 * BLOCK, width), f32),
            pltpu.VMEM((2 * BLOCK, width), f32),
            pltpu.VMEM((2 * BLOCK, width), f32),
            pltpu.VMEM((8, 48, PAIR), bf16),
            pltpu.VMEM((length, width), f32),
            pltpu.VMEM((length, width), f32),
            pltpu.VMEM((length, width), f32),
            pltpu.VMEM((8, 48, PAIR), bf16),
            pltpu.VMEM((48, PAIR), bf16),
            pltpu.VMEM((8, 48, PAIR), bf16),
            pltpu.VMEM((7, PAIR, PAIR), bf16),
            pltpu.VMEM((7, 32, PAIR), f32),
            pltpu.VMEM((8, 16, PAIR), bf16),
            pltpu.VMEM((8, 16, PAIR), bf16),
            pltpu.VMEM((length, width), bf16),
            pltpu.VMEM((4, rows, width), bf16),
            pltpu.VMEM((inner, depth), bf16),
            dma(()), dma((6,)), dma(()), dma((6,)), dma((6,)), dma((6,)), dma((2,)),
            dma((8,)), dma((8,)), dma((8,)), dma((8,)), dma((8,)), dma((8,)), dma((4,)), dma((4,)),
            pltpu.SemaphoreType.REGULAR, pltpu.SemaphoreType.REGULAR,
        ] + [pltpu.VMEM((length, width), f32)] * 8,
        compiler_params=pltpu.CompilerParams(collective_id=0, has_side_effects=True),
        name="layer",
    )(tokens, gain, *weights, mix, decay_base, rate_base, drift, group_gain, start, w_out)


def per_device(tokens, norm_gain, w_recept, w_key, w_value, w_decay, w_rate, w_gate, shift_mix, decay_base, rate_base,
               decay_drift, group_gain, initial_state, w_out):
    return call_layer(
        tokens, norm_gain.reshape(1, -1), (w_recept, w_key, w_value, w_decay, w_rate, w_gate), shift_mix,
        decay_base.reshape(1, -1), rate_base.reshape(1, -1), decay_drift, group_gain.reshape(1, -1), initial_state, w_out)


def solution(mesh):
    finer = Mesh(mesh.devices.reshape(8, 4, 2, mesh.shape["tp"]), AXES)
    in_specs = (
        P(SP_TP, None),
        P(),
        P(None, "tp"),
        P(None, "tp"),
        P(None, "tp"),
        P(None, "tp"),
        P(None, "tp"),
        P(None, "tp"),
        P(None, "tp"),
        P("tp"),
        P("tp"),
        P(SP),
        P("tp"),
        P("tp", None, None),
        P(),
    )
    return jax.shard_map(
        per_device, mesh=finer, in_specs=in_specs, out_specs=P(SP_TP, None), check_vma=False
    )
```
